32 devices in a mesh: sp: 8 (over z, y), tp: 4 (over x, core).
Axes of the slice: x: 2, y: 2, z: 4, core: 2. Of those that a mesh axis runs over, the one named last changes fastest.
Arguments:
- stream_in: bfloat16 [2048, 4096], P(('sp', 'tp')), may hold values from -6 to 6
- q_first: bfloat16 [2048, 1024], P('sp', 'tp'), may hold values from -110 to 110
- q_second: bfloat16 [2048, 1024], P('sp', 'tp'), may hold values from -110 to 110
- k_first: bfloat16 [2048, 512], P('sp', 'tp'), may hold values from -7 to 7
- k_second: bfloat16 [2048, 512], P('sp', 'tp'), may hold values from -7 to 7
- values: bfloat16 [2048, 1024], P('sp', 'tp'), may hold values from -6 to 6
- head_lambda: float32 [8], P('tp'), may hold values from 0.3 to 0.8
- w_out: bfloat16 [2048, 4096], P('tp'), may hold values from -0.125 to 0.125
- norm_gain: float32 [4096], replicated, may hold values from 0.1 to 1.9
- routes: int32 [2048, 4], P(('sp', 'tp')), may hold values from 0 to 7, all different within a row; in each aligned block of 64 rows (0 to 63, 64 to 127, ...) at most 48 rows name the same one
- route_w: float32 [2048, 4], P(('sp', 'tp')), may hold values from 0.2 to 1
- w_gate: bfloat16 [8, 4096, 128], P('sp'), may hold values from -0.09375 to 0.09375
- w_up: bfloat16 [8, 4096, 128], P('sp'), may hold values from -0.09375 to 0.09375
- w_down: bfloat16 [8, 128, 4096], P('sp'), may hold values from -0.5 to 0.5
- s_gate: bfloat16 [4096, 512], P(None, 'tp'), may hold values from -0.09375 to 0.09375
- s_up: bfloat16 [4096, 512], P(None, 'tp'), may hold values from -0.09375 to 0.09375
- s_down: bfloat16 [512, 4096], P('tp'), may hold values from -0.25 to 0.25
Outputs:
- layer_out: bfloat16 [2048, 4096], P(('sp', 'tp'))
The draws below stay inside these ranges and needn't reach their ends.
Inputs may be any that keep to these rules, and one draw needn't show every extreme that they name: `routes`: each row names 4 different experts. Within the rows of one device (aligned blocks of 64 rows) no expert is named more than 48 times, and in some blocks one expert is named exactly 48 times.
All inputs are finite; a program needn't handle non-finite values.
Results may differ from the reference program's by a relative error of at most 0.017.
Values may be sent and summed in bfloat16 or wider, within the bound.
A program may use at most 128 MiB of HBM per device.

```python
import math
import jax
import jax.numpy as jnp
import numpy as np
from jax import lax

D = 4096
HEAD = 128
HEADS = 8
KV_HEADS = 4
VD = 256
F = 128
SF = 512
TOPK = 4
ROWS = 64
TOKENS = 2048
EXP = 8
CAP = 48
N_SP = 8
N_TP = 4


def key_table(key, which):
    raw = jnp.clip(jax.random.normal(jax.random.fold_in(key, 100 + which), (TOKENS, KV_HEADS * HEAD), jnp.float32), -4.5, 4.5) * 1.3
    return raw


def query_table(key, which):
    raw = jnp.clip(jax.random.normal(jax.random.fold_in(key, 300 + which), (TOKENS, HEADS * HEAD), jnp.float32), -4.5, 4.5) * 1.3
    return raw


def draw_q_first(key, part):
    return query_table(key, 1).astype(jnp.bfloat16)


def draw_q_second(key, part):
    return query_table(key, 2).astype(jnp.bfloat16)


def draw_k_first(key, part):
    return key_table(key, 1).astype(jnp.bfloat16)


def draw_k_second(key, part):
    return key_table(key, 2).astype(jnp.bfloat16)


def level_of(rng, shape, split, smallest, largest):
    factor_of = 1.0
    for axis_at, blocks in split:
        draws = jax.random.uniform(jax.random.fold_in(jax.random.fold_in(rng, 6), axis_at), (blocks,), jnp.float32, smallest / len(split), largest / len(split))
        factor_of = factor_of * jnp.repeat(jnp.exp(draws), shape[axis_at] // blocks).reshape((-1,) + (1,) * (len(shape) - 1 - axis_at))
    return factor_of


def routed_block(own_key, own, number, rows, amount, top, bound, lean):
    ranking = jax.random.permutation(own_key, amount)
    packed, common = shares(amount, rows * top, bound, lean, True), shares(amount, rows * top, bound, lean, False)
    places = jnp.arange(amount)

    def named(tallies, rotation):
        used = int((tallies > 0).sum())
        fixed = max(1, used // 4)
        shifted = fixed + (places - fixed + rotation * (used - fixed)) % max(1, amount - fixed)
        return jnp.zeros((amount,), jnp.int32).at[ranking[jnp.where(places < fixed, places, shifted)]].set(jnp.asarray(tallies, jnp.int32))

    tallies = jnp.where(number % 4 == 0, named(packed, number // 4), named(common, number - number // 4 - 1))
    mixed = jax.random.permutation(jax.random.fold_in(own, 3), amount)
    source_of, sink = mixed[0:amount // 2 * 2:2], mixed[1:amount // 2 * 2:2]
    margin = jnp.minimum(tallies[source_of] - 1, bound - tallies[sink]) // 2
    margin = jnp.where((source_of == ranking[0]) | (sink == ranking[0]) | (tallies[sink] == 0), 0, jnp.maximum(margin, 0))
    shifted = jax.random.randint(jax.random.fold_in(own, 4), (amount // 2,), 0, 1 << 20) % (margin + 1)
    tallies = tallies.at[source_of].add(-shifted).at[sink].add(shifted)
    labels = jnp.searchsorted(jnp.cumsum(tallies), jnp.arange(rows * top), side="right").astype(jnp.int32)
    grid = labels.reshape(top, rows).T
    grid = grid[jax.random.permutation(jax.random.fold_in(own, 1), rows)]
    rotation = jax.random.randint(jax.random.fold_in(own, 2), (rows, 1), 0, top)
    return jnp.take_along_axis(grid, (jnp.arange(top)[None, :] + rotation) % top, axis=1)


def shares(amount, total, limit, skew, full):
    loads = [(1 << 20) // math.isqrt(standing ** skew) + 1 for standing in range(1, amount + 1)]
    largest = limit if full else min(limit, max(-(-total // amount), total * loads[0] // sum(loads)))
    least = 1 if total - largest >= amount - 1 else 0
    holding, spare = [largest] + [least] * (amount - 1), total - largest - least * (amount - 1)
    while spare > 0:
        candidates = [i for i in range(1, amount) if holding[i] < largest] or [i for i in range(1, amount) if holding[i] < limit]
        mass, left = sum([loads[i] for i in candidates]), spare
        for i in candidates:
            addition = min(limit - holding[i], max(1, left * loads[i] // mass), spare)
            holding[i] = holding[i] + addition
            spare = spare - addition
    return np.array(holding)


def normal_values(key, extent, deviation, most, shards=(), held_as=jnp.bfloat16):
    loudness = level_of(key, extent, shards, -0.22, 0.18) if shards else 1.0
    drawn = jax.random.normal(key, extent, jnp.float32) * deviation * loudness
    return jnp.minimum(jnp.maximum(drawn, -most), most).astype(held_as)


def setup_inputs(seed: int = 0) -> dict:
    keys = jax.random.split(jax.random.key(seed), 18)
    stream_in = normal_values(keys[0], (TOKENS, D), 1.0, 6.0, ((0, 32),))
    q_first = draw_q_first(jax.random.fold_in(keys[17], 71), 0)
    q_second = draw_q_second(jax.random.fold_in(keys[17], 71), 0)
    k_first = draw_k_first(jax.random.fold_in(keys[17], 71), 0)
    k_second = draw_k_second(jax.random.fold_in(keys[17], 71), 0)
    values = normal_values(keys[5], (TOKENS, KV_HEADS * VD), 1.0, 6.0, ((0, 8), (1, 4)))
    head_lambda = jnp.clip(0.3 + 0.5 * jax.random.uniform(keys[6], (HEADS,), jnp.float32) ** level_of(keys[6], (HEADS,), ((0, 4),), -0.2, 0.2), 0.3, 0.8)
    w_out = normal_values(keys[7], (HEADS * VD, D), (HEADS * VD) ** -0.5, 0.125, ((0, 4),))
    norm_gain = jnp.clip(1.0 + 0.18 * jax.random.normal(keys[8], (D,), jnp.float32), 0.1, 1.9)
    routes_keys = jax.random.split(jax.random.fold_in(keys[9], 1), TOKENS // ROWS)
    routes_turns = jax.random.permutation(jax.random.fold_in(keys[9], 3), TOKENS // ROWS)
    routes = jax.vmap(lambda own, number: routed_block(jax.random.fold_in(keys[9], 2), own, number, ROWS, EXP, TOPK, CAP, 1))(routes_keys, routes_turns).reshape((TOKENS, TOPK))
    route_w = jnp.clip(0.2 + 0.8 * jax.random.uniform(keys[10], (TOKENS, TOPK), jnp.float32) ** level_of(keys[10], (TOKENS, TOPK), ((0, 32),), -0.2, 0.2), 0.2, 1.0)
    w_gate = normal_values(keys[11], (EXP, D, F), D ** -0.5, 0.09375, ((0, 8),))
    w_up = normal_values(keys[12], (EXP, D, F), D ** -0.5, 0.09375, ((0, 8),))
    w_down = normal_values(keys[13], (EXP, F, D), F ** -0.5, 0.5, ((0, 8),))
    s_gate = normal_values(keys[14], (D, SF), D ** -0.5, 0.09375, ((1, 4),))
    s_up = normal_values(keys[15], (D, SF), D ** -0.5, 0.09375, ((1, 4),))
    s_down = normal_values(keys[16], (SF, D), SF ** -0.5, 0.25, ((0, 4),))
    return {"stream_in": stream_in, "q_first": q_first, "q_second": q_second, "k_first": k_first, "k_second": k_second, "values": values, "head_lambda": head_lambda, "w_out": w_out, "norm_gain": norm_gain, "routes": routes, "route_w": route_w, "w_gate": w_gate, "w_up": w_up, "w_down": w_down, "s_gate": s_gate, "s_up": s_up, "s_down": s_down}


FLOOR = -1e+30

def absorb(state, first_q, second_q, first_k, second_k, value_rows, query_pos, key_pos):
    allowed = key_pos[None, :] <= query_pos[:, None]
    scale = first_q.shape[-1] ** (-0.5)
    result = []
    pairs = ((first_q, first_k), (second_q, second_k))
    for index in range(2):
        query_rows, key_rows = pairs[index]
        peak, total, accum = (state[3 * index], state[3 * index + 1], state[3 * index + 2])
        scores = jnp.dot(query_rows, key_rows.T, preferred_element_type=jnp.float32) * scale
        scores = jnp.where(allowed, scores, FLOOR)
        raised = jnp.maximum(peak, scores.max(-1))
        weights = jnp.where(allowed, jnp.exp(scores - raised[:, None]), 0.0)
        fade = jnp.exp(peak - raised)
        total = total * fade + weights.sum(-1)
        accum = accum * fade[:, None] + jnp.dot(weights.astype(jnp.bfloat16), value_rows, preferred_element_type=jnp.float32)
        result += [raised, total, accum]
    return tuple(result)

def one_head(first_q, second_q, first_k, second_k, value_rows, weight, span, blocks):

    def per_block(block):
        begin = block * span
        query_one = lax.dynamic_slice_in_dim(first_q, begin, span, 0)
        query_two = lax.dynamic_slice_in_dim(second_q, begin, span, 0)
        query_pos = begin + jnp.arange(span, dtype=jnp.int32)
        peaks = jnp.full((span,), FLOOR, jnp.float32)
        sums = jnp.zeros((span,), jnp.float32)
        accums = jnp.zeros((span, VD), jnp.float32)
        start_state = (peaks, sums, accums, peaks, sums, accums)

        def visit(inner, state):
            key_begin = inner * span
            key_one = lax.dynamic_slice_in_dim(first_k, key_begin, span, 0)
            key_two = lax.dynamic_slice_in_dim(second_k, key_begin, span, 0)
            value_part = lax.dynamic_slice_in_dim(value_rows, key_begin, span, 0)
            key_pos = key_begin + jnp.arange(span, dtype=jnp.int32)
            return absorb(state, query_one, query_two, key_one, key_two, value_part, query_pos, key_pos)
        final = lax.fori_loop(jnp.int32(0), block + 1, visit, start_state)
        head_out = final[2] / final[1][:, None] - weight * final[5] / final[4][:, None]
        head_out = head_out * lax.rsqrt(lax.optimization_barrier(jnp.mean(head_out * head_out, axis=-1, keepdims=True)) + 1e-05)
        return head_out.astype(jnp.bfloat16)
    outputs = lax.map(per_block, jnp.arange(blocks, dtype=jnp.int32))
    return outputs.reshape(TOKENS, VD)

def reference(stream_in, q_first, q_second, k_first, k_second, values, head_lambda, w_out, norm_gain, routes, route_w, w_gate, w_up, w_down, s_gate, s_up, s_down):
    group = HEADS // KV_HEADS
    span = math.gcd(TOKENS, 512)
    blocks = TOKENS // span
    parts = []
    for head in range(HEADS):
        key_head = head // group
        parts.append(one_head(q_first[:, head * HEAD:(head + 1) * HEAD], q_second[:, head * HEAD:(head + 1) * HEAD], k_first[:, key_head * HEAD:(key_head + 1) * HEAD], k_second[:, key_head * HEAD:(key_head + 1) * HEAD], values[:, key_head * VD:(key_head + 1) * VD], head_lambda[head], span, blocks))
    attn_rows = jnp.concatenate(parts, axis=1)
    attn = jnp.dot(attn_rows, w_out, preferred_element_type=jnp.float32)
    resid = (stream_in.astype(jnp.float32) + attn).astype(jnp.bfloat16)
    stream = lax.optimization_barrier(resid).astype(jnp.float32)
    normed = (stream * lax.rsqrt(lax.optimization_barrier(jnp.mean(stream * stream, axis=-1, keepdims=True)) + 1e-06) * norm_gain).astype(jnp.bfloat16)
    shared_hidden = (jax.nn.silu(jnp.dot(normed, s_gate, preferred_element_type=jnp.float32)) * jnp.dot(normed, s_up, preferred_element_type=jnp.float32)).astype(jnp.bfloat16)
    shared = jnp.dot(shared_hidden, s_down, preferred_element_type=jnp.float32)
    flat_ids = routes.reshape(-1).astype(jnp.int32)
    count_all = TOKENS * TOPK
    token_of = jnp.arange(count_all, dtype=jnp.int32) // TOPK
    order = jnp.argsort(flat_ids, stable=True).astype(jnp.int32)
    counts = lax.optimization_barrier(jnp.sum((flat_ids[None, :] == jnp.arange(EXP, dtype=jnp.int32)[:, None]).astype(jnp.int32), axis=1)).astype(jnp.int32)
    starts = (jnp.cumsum(counts) - counts).astype(jnp.int32)
    window = N_SP * N_TP * CAP
    padded = jnp.concatenate([order, jnp.zeros((window,), jnp.int32)])
    flat_weights = route_w.reshape(-1)

    def serve(routed, inputs):
        gate_e, up_e, down_e, begin, count = inputs
        picks = lax.dynamic_slice_in_dim(padded, begin, window, 0)
        live = jnp.arange(window, dtype=jnp.int32) < count
        tokens_here = token_of[picks]
        rows_here = normed[tokens_here]
        hidden = (jax.nn.silu(jnp.dot(rows_here, gate_e, preferred_element_type=jnp.float32)) * jnp.dot(rows_here, up_e, preferred_element_type=jnp.float32)).astype(jnp.bfloat16)
        result = jnp.dot(hidden, down_e, preferred_element_type=jnp.float32).astype(jnp.bfloat16)
        scaled = result.astype(jnp.float32) * jnp.where(live, flat_weights[picks], 0.0)[:, None]
        return (routed.at[tokens_here].add(scaled), None)
    routed, _ = lax.scan(serve, jnp.zeros((TOKENS, D), jnp.float32), (w_gate, w_up, w_down, starts, counts))
    return (stream + routed + shared).astype(jnp.bfloat16)
```

```python
import functools
import math

import jax
import jax.numpy as jnp
from jax import lax
from jax.experimental import pallas as pl
from jax.experimental.pallas import tpu as pltpu
from jax.sharding import PartitionSpec as P

HEAD = 128


FLOOR = -1e30


def absorb(state, first_q, second_q, first_k, second_k, value_rows, query_pos, key_pos):
    allowed = key_pos[None, :] <= query_pos[:, None]
    scale = first_q.shape[-1] ** (-0.5)
    result = []
    pairs = ((first_q, first_k), (second_q, second_k))
    for index in range(2):
        query_rows, key_rows = pairs[index]
        peak, total, accum = (state[3 * index], state[3 * index + 1], state[3 * index + 2])
        scores = (
            jnp.einsum("qagd,kad->agqk", query_rows, key_rows, preferred_element_type=jnp.float32)
            * scale
        )
        scores = jnp.where(allowed, scores, FLOOR)
        raised = jnp.maximum(peak, scores.max(-1))
        weights = jnp.where(allowed, jnp.exp(scores - raised[..., None]), 0.0)
        fade = jnp.exp(peak - raised)
        total = total * fade + weights.sum(-1)
        accum = accum * fade[..., None] + jnp.einsum(
            "agqk,kad->agqd",
            weights.astype(jnp.bfloat16),
            value_rows,
            preferred_element_type=jnp.float32,
        )
        result += [raised, total, accum]
    return tuple(result)


def empty_state(kv_local, group, count, value_dim):
    peaks = jnp.full((kv_local, group, count), FLOOR, jnp.float32)
    sums = jnp.zeros((kv_local, group, count), jnp.float32)
    accums = jnp.zeros((kv_local, group, count, value_dim), jnp.float32)
    return (peaks, sums, accums, peaks, sums, accums)


def fold_rows(state, first_q, second_q, query_pos, last_row, pieces, start):
    first_k, second_k, value_rows = pieces
    length = first_k.shape[0]
    kv_local = first_q.shape[1]
    value_dim = value_rows.shape[1] // kv_local
    span = math.gcd(length, 2048)

    def sweep(current):

        def visit(block, inner):
            begin = block * span
            key_one = lax.dynamic_slice_in_dim(first_k, begin, span, 0).reshape(
                span, kv_local, HEAD
            )
            key_two = lax.dynamic_slice_in_dim(second_k, begin, span, 0).reshape(
                span, kv_local, HEAD
            )
            value_part = lax.dynamic_slice_in_dim(value_rows, begin, span, 0).reshape(
                span, kv_local, value_dim
            )
            key_pos = begin + jnp.arange(span, dtype=jnp.int32)
            return absorb(
                inner, first_q, second_q, key_one, key_two, value_part, query_pos, key_pos
            )

        return lax.fori_loop(0, length // span, visit, current)

    def unchanged(current):
        return current

    return lax.cond(start <= last_row, sweep, unchanged, state)


def finish_heads(final, head_lambda):
    kv_local, group, count, value_dim = final[2].shape
    weight = head_lambda.reshape(kv_local, group, 1, 1)
    head_out = final[2] / final[1][..., None] - weight * final[5] / final[4][..., None]
    head_out = head_out * lax.rsqrt(jnp.mean(head_out * head_out, axis=-1, keepdims=True) + 1e-05)
    return (
        head_out.transpose(2, 0, 1, 3)
        .reshape(count, kv_local * group * value_dim)
        .astype(jnp.bfloat16)
    )


def shared_part(normed, s_gate, s_up, s_down):
    piece = lax.all_gather(normed, "tp", axis=0, tiled=True)
    gate_part = jnp.dot(piece, s_gate, preferred_element_type=jnp.float32)
    up_part = jnp.dot(piece, s_up, preferred_element_type=jnp.float32)
    hidden = (jax.nn.silu(gate_part) * up_part).astype(jnp.bfloat16)
    terms = jnp.dot(hidden, s_down, preferred_element_type=jnp.float32)
    return lax.psum_scatter(
        terms.astype(jnp.bfloat16), "tp", scatter_dimension=0, tiled=True
    ).astype(jnp.float32)


def routed_part(normed, routes, route_w, w_gate, w_up, w_down):
    rows, topk = routes.shape
    local_experts = w_gate.shape[0]
    experts = local_experts * lax.axis_size("sp")
    slots = max(2, 3 * rows * topk // (2 * experts))
    flat_ids = routes.reshape(-1)
    hits = (flat_ids[:, None] == jnp.arange(experts, dtype=jnp.int32)[None, :]).astype(jnp.int32)
    slot_of = jnp.sum(jnp.cumsum(hits, axis=0) * hits, axis=1) - 1
    target = flat_ids * slots + slot_of
    placing = jnp.any(
        jnp.arange(experts * slots, dtype=jnp.int32)[:, None, None]
        == target.reshape(rows, topk)[None, :, :],
        axis=-1,
    ).astype(jnp.bfloat16)
    outgoing = (
        jnp.dot(placing, normed, preferred_element_type=jnp.float32)
        .astype(jnp.bfloat16)
        .reshape(experts, slots, normed.shape[1])
    )
    arrived = lax.all_to_all(outgoing, "sp", split_axis=0, concat_axis=0, tiled=True)
    sources = arrived.shape[0] // local_experts
    grouped = arrived.reshape(sources, local_experts, arrived.shape[1], arrived.shape[2])
    gate_part = jnp.einsum("sjcd,jdf->sjcf", grouped, w_gate, preferred_element_type=jnp.float32)
    up_part = jnp.einsum("sjcd,jdf->sjcf", grouped, w_up, preferred_element_type=jnp.float32)
    hidden = (jax.nn.silu(gate_part) * up_part).astype(jnp.bfloat16)
    result = jnp.einsum(
        "sjcf,jfd->sjcd", hidden, w_down, preferred_element_type=jnp.float32
    ).astype(jnp.bfloat16)
    returned = lax.all_to_all(
        result.reshape(arrived.shape), "sp", split_axis=0, concat_axis=0, tiled=True
    )
    picked = (
        returned.reshape(experts * slots, normed.shape[1])[target]
        .reshape(rows, topk, normed.shape[1])
        .astype(jnp.float32)
    )
    return jnp.sum(picked * route_w[..., None], axis=1)


def local(
    stream_in,
    q_first,
    q_second,
    k_first,
    k_second,
    values,
    head_lambda,
    w_out,
    norm_gain,
    routes,
    route_w,
    w_gate,
    w_up,
    w_down,
    s_gate,
    s_up,
    s_down,
):
    seq_rows = q_first.shape[0]
    kv_local = k_first.shape[1] // HEAD
    heads_local = q_first.shape[1] // HEAD
    group = heads_local // kv_local
    value_dim = values.shape[1] // kv_local
    offset = lax.axis_index("sp") * seq_rows
    query_pos = offset + jnp.arange(seq_rows, dtype=jnp.int32)
    last_row = offset + seq_rows - 1
    first_q = q_first.reshape(seq_rows, kv_local, group, HEAD)
    second_q = q_second.reshape(seq_rows, kv_local, group, HEAD)
    start_state = empty_state(kv_local, group, seq_rows, value_dim)
    folded_state = fold_rows(
        start_state,
        first_q,
        second_q,
        query_pos,
        last_row,
        (
            lax.all_gather(k_first, "sp", axis=0, tiled=True),
            lax.all_gather(k_second, "sp", axis=0, tiled=True),
            lax.all_gather(values, "sp", axis=0, tiled=True),
        ),
        jnp.int32(0),
    )
    attn_rows = finish_heads(folded_state, head_lambda)
    attn = lax.psum_scatter(
        jnp.dot(attn_rows, w_out, preferred_element_type=jnp.float32).astype(jnp.bfloat16),
        "tp",
        scatter_dimension=0,
        tiled=True,
    ).astype(jnp.float32)
    resid = (stream_in.astype(jnp.float32) + attn).astype(jnp.bfloat16)
    stream = lax.optimization_barrier(resid).astype(jnp.float32)
    normed = (
        stream * lax.rsqrt(jnp.mean(stream * stream, axis=-1, keepdims=True) + 1e-06) * norm_gain
    ).astype(jnp.bfloat16)
    routed = routed_part(normed, routes, route_w, w_gate, w_up, w_down)
    shared = shared_part(normed, s_gate, s_up, s_down)
    return (stream + routed + shared).astype(jnp.bfloat16)


def mesh_copy(src, dst, send_sem, recv_sem, axis, target):
    return pltpu.make_async_remote_copy(
        src_ref=src,
        dst_ref=dst,
        send_sem=send_sem,
        recv_sem=recv_sem,
        device_id={axis: target},
        device_id_type=pl.DeviceIdType.MESH,
    )


def greet(axis, target):
    pl.semaphore_signal(
        pltpu.get_barrier_semaphore(),
        inc=1,
        device_id={axis: target},
        device_id_type=pl.DeviceIdType.MESH,
    )


def near_kernel(
    n, nt, group, pieces,
    q_one, q_two, k_one, k_two, val, lam, w_out_h, stream, gain, mix,
    gate_h, up_h, s_gate_h, s_up_h, down_h, s_down_h,
    out,
    stacked, keys_one, keys_two, vals, peak, total, accum, rows_in,
    w, order, out_one, in_one, out_two, in_two, resid,
    gates, ups, s_gate, s_up, wall, gathered, beside, stat, stat_b,
    out_hid, in_hid, out_sh, in_sh, units, out_fin, in_fin, result,
    load, send_kv, recv_kv, send_one, recv_one, send_two, recv_two,
    send_g, recv_g, send_d, recv_d, send_sd, recv_sd,
    send_x, recv_x, send_b, recv_b, send_h, recv_h, send_s, recv_s,
    send_u, recv_u, send_f, recv_f, save,
):
    me, mine = lax.axis_index("sp"), lax.axis_index("tp")
    place, side = me // 2, me % 2
    far, core = mine // 2, mine % 2
    depth = n // 2
    pair, partner, across = me + 1 - 2 * side, mine + 1 - 2 * core, 2 * (1 - far) + core
    above, below = place < depth - 1, place > 0
    seq = q_one.shape[0]
    rows, width = stream.shape
    hid, wide = down_h.shape[0], s_down_h.shape[0]
    scale = HEAD ** (-0.5)
    half = width // 2

    def column(o):
        return 2 * ((place + o) % depth) + side

    def cols_of(f):
        return pl.ds(pl.multiple_of(f * half, half), half)

    loads = [
        pltpu.make_async_copy(source, target, load.at[i])
        for i, (source, target) in enumerate(
            (
                (w_out_h, w),
                (gate_h, gates.at[0]),
                (up_h, ups.at[0]),
                (s_gate_h, s_gate),
                (s_up_h, s_up),
                (
                    down_h.at[:, cols_of(far)],
                    wall.at[pl.ds(pl.multiple_of(me * hid, hid), hid)],
                ),
                (
                    s_down_h.at[:, cols_of(far)],
                    wall.at[pl.ds(pl.multiple_of(n * hid + mine * wide, wide), wide)],
                ),
            )
        )
    ]
    for o in range(1, depth):
        greet("sp", column(o))
    greet("sp", pair)
    greet("tp", across)
    greet("tp", partner)
    pl.semaphore_wait(pltpu.get_barrier_semaphore(), depth + 2)

    sources = (k_one, k_two, val)
    held = (keys_one, keys_two, vals)

    def copies(block, way, target, own):
        return [
            mesh_copy(
                sources[a] if own else held[a].at[block],
                held[a].at[block],
                send_kv.at[way, a, block],
                recv_kv.at[a, block],
                "sp",
                target,
            )
            for a in range(3)
        ]

    def start(block, way, target, own=False):
        for one in copies(block, way, target, own):
            one.start()

    def arrive(block):
        for one in copies(block, 0, pair, False):
            one.wait_recv()

    share = width // 2
    share_at = pl.ds(pl.multiple_of(core * share, share), share)
    other_at = pl.ds(pl.multiple_of((1 - core) * share, share), share)

    def pair_weights():
        return [
            mesh_copy(
                h.at[share_at], v.at[1, share_at], send_g.at[0, i], recv_g.at[0, i], "sp", pair
            )
            for i, (h, v) in enumerate(((gate_h, gates), (up_h, ups)))
        ]

    def pair_weights_on(at):
        return [
            mesh_copy(
                v.at[1, at], v.at[1, at], send_g.at[1, i], recv_g.at[1, i], "tp", partner
            )
            for i, v in enumerate((gates, ups))
        ]

    part = hid // 2

    def down_at(block, c):
        return wall.at[pl.ds(pl.multiple_of(block * hid + c * part, part), part)]

    def down_own(way, target):
        return mesh_copy(
            down_h.at[pl.ds(pl.multiple_of(core * part, part), part), cols_of(far)],
            down_at(me, core),
            send_d.at[way],
            recv_d.at[0, me],
            "sp",
            target,
        )

    def down_pair(block):
        return mesh_copy(
            down_at(block, core),
            down_at(block, core),
            send_d.at[depth + block],
            recv_d.at[0, block],
            "sp",
            pair,
        )

    def down_core(block, c):
        return mesh_copy(
            down_at(block, c),
            down_at(block, c),
            send_d.at[depth + n + block],
            recv_d.at[1, block],
            "tp",
            partner,
        )

    def sd_at(u):
        return wall.at[pl.ds(pl.multiple_of(n * hid + u * wide, wide), wide)]

    def sd_own(way, f, target):
        return mesh_copy(
            s_down_h.at[:, cols_of(f)], sd_at(mine), send_sd.at[way], recv_sd.at[mine], "tp", target
        )

    def sd_on(u):
        return mesh_copy(sd_at(u), sd_at(u), send_sd.at[2], recv_sd.at[u], "tp", partner)

    @pl.when(above)
    def _():
        start(me, 0, me + 2, True)

    @pl.when(side == 0)
    def _():
        start(me, 1, pair, True)

    for one in loads:
        one.start()
    late = place >= depth // 2

    @pl.when(late)
    def _():
        sd_own(1, 1 - far, across).start()

    sd_own(0, far, partner).start()
    for o in range(1, depth):

        @pl.when(place + o >= depth)
        def _():
            down_own(o, column(o)).start()

    for index, q in enumerate((q_one, q_two)):
        for h in range(group):
            stacked[index, h * seq : (h + 1) * seq, :] = q[:, h * HEAD : (h + 1) * HEAD]

    def scores_of(index, keys):
        return (
            lax.dot_general(
                stacked[index], keys, (((1,), (1,)), ((), ())), preferred_element_type=jnp.float32
            )
            * scale
        )

    spread = (group * seq, seq)
    row_of = lax.broadcasted_iota(jnp.int32, spread, 0) % seq
    allowed = lax.broadcasted_iota(jnp.int32, spread, 1) <= row_of
    for index, keys in enumerate((k_one, k_two)):
        scores = jnp.where(allowed, scores_of(index, keys[...]), FLOOR)
        top = jnp.max(scores, axis=-1, keepdims=True)
        weights = jnp.exp(scores - top)
        peak[index] = top
        total[index] = jnp.sum(weights, axis=-1, keepdims=True)
        accum[index] = jnp.dot(
            weights.astype(jnp.bfloat16), val[...], preferred_element_type=jnp.float32
        )

    def fold(block):
        for index in range(2):
            scores = scores_of(index, held[index][block])
            old = peak[index]
            top = jnp.maximum(old, jnp.max(scores, axis=-1, keepdims=True))
            weights = jnp.exp(scores - top)
            fade = jnp.exp(old - top)
            peak[index] = top
            total[index] = total[index] * fade + jnp.sum(weights, axis=-1, keepdims=True)
            accum[index] = accum[index] * fade + jnp.dot(
                weights.astype(jnp.bfloat16), vals[block], preferred_element_type=jnp.float32
            )

    def weights_out():
        for one in pair_weights():
            one.start()
        down_own(0, pair).start()

    pl.when(place == 0)(weights_out)

    def visit(e, carry):
        @pl.when(place >= e)
        def _():
            block = me - 2 * e
            for up, over in zip(copies(block, 0, me + 2, False), copies(block, 1, pair, False)):
                over.wait_recv()
                pl.when(above)(up.start)
                over.start()
            pl.when(e == place)(weights_out)
            fold(block)

        @pl.when((place >= e - 1) & ((e > 1) | (side == 1)))
        def _():
            block = pair - 2 * (e - 1)
            arrive(block)
            fold(block)

        return carry

    lax.fori_loop(1, depth + 1, visit, 0)

    @pl.when(above)
    def _():
        down_own(1, me + 2).start()

    def down_up(block):
        return mesh_copy(
            down_at(block, core),
            down_at(block, core),
            send_d.at[depth + 2 * n + block],
            recv_d.at[0, block],
            "sp",
            me + 2,
        )

    def lift(d):
        @pl.when((place >= d) & above)
        def _():
            down_up(me - 2 * d).wait_recv()
            down_up(me - 2 * d).start()

    for h in range(group):
        cut = slice(h * seq, (h + 1) * seq)
        head = accum[0, cut, :] / total[0, cut, :] - lam[h] * (
            accum[1, cut, :] / total[1, cut, :]
        )
        head = head * lax.rsqrt(jnp.mean(head * head, axis=-1, keepdims=True) + 1e-05)
        size = head.shape[1]
        rows_in[:, h * size : (h + 1) * size] = head.astype(jnp.bfloat16)

    for o in range(2):
        base = 2 * ((far + o) % 2)
        for which, parity in enumerate((1 - core, core)):
            begin = pl.multiple_of((base + parity) * rows, rows)
            order[which, o * rows : (o + 1) * rows, :] = rows_in[pl.ds(begin, rows), :]

    first = [
        mesh_copy(out_one.at[i], in_one.at[i], send_one.at[i], recv_one.at[i], "tp", partner)
        for i in range(pieces)
    ]
    second = [
        mesh_copy(out_two.at[i], in_two.at[i], send_two.at[i], recv_two.at[i], "tp", across)
        for i in range(pieces)
    ]
    span = width // pieces
    lift(1)
    loads[0].wait()
    for i in range(pieces):
        out_one[i] = jnp.dot(
            order[0], w[:, i * span : (i + 1) * span], preferred_element_type=jnp.float32
        ).astype(jnp.bfloat16)
        first[i].start()
    kept = []
    for i in range(pieces):
        sums = jnp.dot(
            order[1], w[:, i * span : (i + 1) * span], preferred_element_type=jnp.float32
        )
        first[i].wait_recv()
        sums = sums + in_one[i].astype(jnp.float32)
        out_two[i] = sums[rows:].astype(jnp.bfloat16)
        second[i].start()
        kept.append(sums[:rows])

    @pl.when(jnp.logical_not(late))
    def _():
        sd_own(1, 1 - far, across).start()

    for d in range(2, depth):
        lift(d)

    def row_part(block, extra, spot, i):
        return block.at[spot, i] if i < pieces else extra.at[spot]

    def row_copy(spot, way, target, i):
        some = row_part(gathered, stat, spot, i)
        return mesh_copy(
            some,
            some,
            send_x.at[way, i, spot],
            recv_x.at[i, spot],
            "sp",
            target,
        )

    def beside_own(way, target, i):
        return mesh_copy(
            row_part(gathered, stat, place, i),
            row_part(beside, stat_b, mine, i),
            send_b.at[way, i],
            recv_b.at[i, mine],
            "tp",
            target,
        )

    def beside_on(u, i):
        some = row_part(beside, stat_b, u, i)
        return mesh_copy(some, some, send_b.at[2, i], recv_b.at[i, u], "tp", partner)

    def raise_row(e, i):
        row_copy(place - e, 0, pair, i).wait_recv()
        row_copy(place - e, 0, me + 2, i).start()

    def lower_row(e, i):
        row_copy(place + e, 0, pair, i).wait_recv()
        row_copy(place + e, 1, me - 2, i).start()

    def rows_out(i):
        pl.when(above)(lambda: row_copy(place, 0, me + 2, i).start())
        pl.when(below)(lambda: row_copy(place, 1, me - 2, i).start())
        beside_own(1, across, i).start()
        beside_own(0, partner, i).start()

    fine = resid.shape[2]
    per = span // fine
    squares = jnp.zeros((rows, 1), jnp.float32)
    for i in range(pieces):
        cut = slice(i * span, (i + 1) * span)
        second[i].wait_recv()
        sums = kept[i] + in_two[i].astype(jnp.float32)
        sums = (stream[:, cut].astype(jnp.float32) + sums).astype(jnp.bfloat16)
        for j in range(per):
            resid[i * per + j] = sums[:, j * fine : (j + 1) * fine]
        sums = sums.astype(jnp.float32)
        squares = squares + jnp.sum(sums * sums, axis=-1, keepdims=True)
        gathered[place, i] = (sums * gain[:, cut]).astype(jnp.bfloat16)
        rows_out(i)
    shrink = lax.rsqrt(squares / width + 1e-06)
    stat[place] = jnp.broadcast_to(shrink, stat.shape[1:])
    rows_out(pieces)
    for e in range(1, depth - 1):
        for i in range(pieces + 1):
            pl.when(above & (place >= e))(lambda: raise_row(e, i))
            if e == depth - 2:
                pl.when(above & below)(lambda: lower_row(1, i))


    def pass_down(e):
        def one(block, fresh):
            pl.when(fresh)(lambda: down_pair(block).wait_recv())
            down_pair(block).start()
            down_core(block, core).start()

        pl.when(place >= e)(lambda: one(me - 2 * e, jnp.logical_not(above)))
        pl.when(place + e < depth)(lambda: one(me + 2 * e, place >= 0))

    def collect(e):
        def one(block):
            down_pair(block).wait_recv()
            down_core(block, core).start()

        pl.when(place >= e)(lambda: one(pair - 2 * e))
        pl.when(place + e < depth)(lambda: one(pair + 2 * e))

    def hidden_of(block, spot, scales, g, u):
        def project(m):
            parts = [
                jnp.dot(
                    block[spot, i],
                    m[i * span : (i + 1) * span, :],
                    preferred_element_type=jnp.float32,
                )
                for i in range(pieces)
            ]
            return sum(parts[1:], parts[0]) * scales[spot][:, :1]

        gate_part, up_part = project(g), project(u)
        return (gate_part / (1.0 + jnp.exp(-gate_part)) * up_part).astype(jnp.bfloat16)

    for i in range(1, 5):
        loads[i].wait()

    def hid_copy(spot):
        return mesh_copy(
            out_hid.at[spot], in_hid.at[place], send_h.at[spot], recv_h.at[place], "sp",
            2 * spot + side,
        )

    def serve(spot):
        out_hid[spot, side] = hidden_of(gathered, spot, stat, gates.at[0], ups.at[0])
        out_hid[spot, 1 - side] = hidden_of(gathered, spot, stat, gates.at[1], ups.at[1])
        hid_copy(spot).start()

    def sh_copy(u):
        return mesh_copy(
            out_sh.at[u], in_sh.at[mine], send_s.at[u], recv_s.at[mine], "tp", u
        )

    def answer(u):
        out_sh[u] = hidden_of(beside, u, stat_b, s_gate, s_up)
        sh_copy(u).start()

    def turn(e, carry):
        low, high = place >= e, place + e < depth

        @pl.when(low & jnp.logical_not(above))
        def _():
            for i in range(pieces + 1):
                row_copy(place - e, 0, pair, i).wait_recv()

        @pl.when(high)
        def _():
            for i in range(pieces + 1):
                pl.when(below & (e > 1))(lambda: lower_row(e, i))
                pl.when(jnp.logical_not(below))(
                    lambda: row_copy(place + e, 0, pair, i).wait_recv()
                )

        @pl.when(e == 1)
        def _():
            for one, onward in zip(pair_weights(), pair_weights_on(share_at)):
                one.wait_recv()
                onward.start()
            pass_down(1)
            in_sh[mine] = hidden_of(gathered, place, stat, s_gate, s_up)
            in_hid[place, side] = hidden_of(gathered, place, stat, gates.at[0], ups.at[0])
            for one in pair_weights_on(other_at):
                one.wait_recv()

        @pl.when(low)
        def _():
            serve(place - e)

        @pl.when(high)
        def _():
            serve(place + e)

        pass_down(e + 1)

        @pl.when(e == 1)
        def _():
            down_pair(pair).wait_recv()
            down_core(pair, core).start()
            in_hid[place, 1 - side] = hidden_of(gathered, place, stat, gates.at[1], ups.at[1])
            u = across
            for i in range(pieces + 1):
                beside_on(u, i).wait_recv()
                beside_on(u, i).start()
            answer(u)
            sd_on(u).wait_recv()
            sd_on(u).start()
            for o in range(2):
                u = 2 * ((far + o) % 2) + 1 - core
                for i in range(pieces + 1):
                    beside_on(u, i).wait_recv()
                answer(u)

        return carry

    lax.fori_loop(1, depth, turn, 0)

    segments = units.shape[1]

    def unit_copy(s):
        return mesh_copy(
            units.at[0, s], units.at[1, s], send_u.at[s], recv_u.at[s], "tp", across
        )

    for o in range(1, nt):
        u = (mine + o) % nt
        mesh_copy(
            out_sh.at[u], in_sh.at[u], send_s.at[u], recv_s.at[u], "tp", u
        ).wait_recv()
    seg = units.shape[3]
    for j in range(nt):
        at = j * wide
        units[0, depth + at // seg, :, at % seg : at % seg + wide] = in_sh[j]
    for s in range(depth, segments):
        unit_copy(s).start()

    for e in range(1, depth - 1):
        collect(e)
    for spot in range(depth):

        @pl.when(place != spot)
        def _():
            mesh_copy(
                out_hid.at[spot], in_hid.at[spot], send_h.at[spot], recv_h.at[spot], "sp",
                2 * spot + side,
            ).wait_recv()

        for k in range(2):
            j = 2 * spot + k
            units[0, spot, :, k * hid : (k + 1) * hid] = (
                in_hid[spot, k].astype(jnp.float32) * mix[:, j : j + 1]
            ).astype(jnp.bfloat16)
        unit_copy(spot).start()
    collect(depth - 1)

    loads[5].wait()
    loads[6].wait()
    for o in range(2):
        sd_on(2 * ((far + o) % 2) + 1 - core).wait_recv()

    def receive_down(block, carry):
        @pl.when(block != me)
        def _():
            down_core(block, 1 - core).wait_recv()

        return carry

    lax.fori_loop(0, n, receive_down, 0)
    for s in range(segments):
        unit_copy(s).wait_recv()

    def fin_copy(i):
        return mesh_copy(out_fin.at[i], in_fin.at[i], send_f.at[i], recv_f.at[i], "tp", across)

    def put(spot):
        return pltpu.make_async_copy(
            result.at[spot],
            out.at[:, pl.ds(pl.multiple_of(spot * fine, fine), fine)],
            save.at[spot],
        )

    count = half // fine
    for i in range(count):
        cut = slice(i * fine, (i + 1) * fine)
        terms = [
            jnp.dot(
                units[:, s].reshape(2 * rows, seg),
                wall[s * seg : (s + 1) * seg, cut],
                preferred_element_type=jnp.float32,
            )
            for s in range(segments)
        ]
        both = sum(terms[1:], terms[0])
        out_fin[i] = both[rows:].astype(jnp.bfloat16)
        fin_copy(i).start()
        spot = far * count + i
        result[spot] = (resid[spot].astype(jnp.float32) + both[:rows]).astype(jnp.bfloat16)
        put(spot).start()
    for i in range(count):
        spot = (1 - far) * count + i
        fin_copy(i).wait_recv()
        result[spot] = (
            resid[spot].astype(jnp.float32) + in_fin[i].astype(jnp.float32)
        ).astype(jnp.bfloat16)
        put(spot).start()

    def settle(e, carry):
        @pl.when(place >= e)
        def _():
            block = me - 2 * e

            @pl.when(above)
            def _():
                for one in copies(block, 0, me + 2, False):
                    one.wait_send()

                @pl.when(e > 0)
                def _():
                    down_up(block).wait_send()

            @pl.when((e > 0) | (side == 0))
            def _():
                for one in copies(block, 1, pair, False):
                    one.wait_send()

        @pl.when((place + e < depth) & below)
        def _():
            for i in range(pieces + 1):
                row_copy(place + e, 1, me - 2, i).wait_send()

        @pl.when((place >= e) & above)
        def _():
            for i in range(pieces + 1):
                row_copy(place - e, 0, me + 2, i).wait_send()

        @pl.when(e != place)
        def _():
            hid_copy(e).wait_send()
            down_pair(2 * e + side).wait_send()

        return carry

    lax.fori_loop(0, depth, settle, 0)

    def settle_down(block, carry):
        @pl.when(block != me)
        def _():
            down_core(block, core).wait_send()

        return carry

    lax.fori_loop(0, n, settle_down, 0)
    for one in first + second + pair_weights() + pair_weights_on(share_at):
        one.wait_send()
    for o in range(1, depth):
        pl.when((place + o >= depth) | (o == 1))(lambda: down_own(o, column(o)).wait_send())
    down_own(0, pair).wait_send()
    sd_own(0, far, partner).wait_send()
    sd_own(1, 1 - far, across).wait_send()
    sd_on(across).wait_send()
    for i in range(pieces + 1):
        beside_own(0, partner, i).wait_send()
        beside_own(1, across, i).wait_send()
        beside_on(across, i).wait_send()
    for o in range(1, nt):
        sh_copy((mine + o) % nt).wait_send()
    for s in range(segments):
        unit_copy(s).wait_send()
    for i in range(count):
        fin_copy(i).wait_send()
    for i in range(2 * count):
        put(i).wait()


def near(
    stream_in,
    q_first,
    q_second,
    k_first,
    k_second,
    values,
    head_lambda,
    w_out,
    norm_gain,
    routes,
    route_w,
    w_gate,
    w_up,
    w_down,
    s_gate,
    s_up,
    s_down,
):
    n, nt = lax.axis_size("sp"), lax.axis_size("tp")
    depth = n // 2
    seq, rows, width = q_first.shape[0], stream_in.shape[0], stream_in.shape[1]
    group, value_dim = q_first.shape[1] // HEAD, values.shape[1]
    hid, wide = w_down.shape[1], s_down.shape[0]
    tall, features = group * seq, group * value_dim
    pieces = 4
    span = width // pieces
    half, fine = width // 2, width // 8
    seg = 2 * hid
    segments = depth + nt * wide // seg
    chosen = routes[:, :, None] == jnp.arange(n, dtype=jnp.int32)[None, None, :]
    mix = jnp.sum(jnp.where(chosen, route_w[:, :, None], 0.0), axis=1)
    vmem = pl.BlockSpec(memory_space=pltpu.VMEM)
    smem = pl.BlockSpec(memory_space=pltpu.SMEM)
    hbm = pl.BlockSpec(memory_space=pl.ANY)
    low, high = jnp.bfloat16, jnp.float32
    dma = pltpu.SemaphoreType.DMA
    return pl.pallas_call(
        functools.partial(near_kernel, n, nt, group, pieces),
        out_shape=jax.ShapeDtypeStruct((rows, width), low),
        in_specs=[vmem] * 5 + [smem, hbm] + [vmem] * 3 + [hbm] * 6,
        out_specs=hbm,
        scratch_shapes=[
            pltpu.VMEM((2, tall, HEAD), low),
            pltpu.VMEM((n, seq, HEAD), low),
            pltpu.VMEM((n, seq, HEAD), low),
            pltpu.VMEM((n, seq, value_dim), low),
            pltpu.VMEM((2, tall, 1), high),
            pltpu.VMEM((2, tall, 1), high),
            pltpu.VMEM((2, tall, value_dim), high),
            pltpu.VMEM((seq, features), low),
            pltpu.VMEM((features, width), low),
            pltpu.VMEM((2, 2 * rows, features), low),
            pltpu.VMEM((pieces, 2 * rows, span), low),
            pltpu.VMEM((pieces, 2 * rows, span), low),
            pltpu.VMEM((pieces, rows, span), low),
            pltpu.VMEM((pieces, rows, span), low),
            pltpu.VMEM((width // fine, rows, fine), low),
            pltpu.VMEM((2, width, hid), low),
            pltpu.VMEM((2, width, hid), low),
            pltpu.VMEM((width, wide), low),
            pltpu.VMEM((width, wide), low),
            pltpu.VMEM((n * hid + nt * wide, half), low),
            pltpu.VMEM((depth, pieces, rows, span), low),
            pltpu.VMEM((nt, pieces, rows, span), low),
            pltpu.VMEM((depth, rows, HEAD), high),
            pltpu.VMEM((nt, rows, HEAD), high),
            pltpu.VMEM((depth, 2, rows, hid), low),
            pltpu.VMEM((depth, 2, rows, hid), low),
            pltpu.VMEM((nt, rows, wide), low),
            pltpu.VMEM((nt, rows, wide), low),
            pltpu.VMEM((2, segments, rows, seg), low),
            pltpu.VMEM((half // fine, rows, fine), low),
            pltpu.VMEM((half // fine, rows, fine), low),
            pltpu.VMEM((width // fine, rows, fine), low),
            dma((7,)),
            dma((2, 3, n)),
            dma((3, n)),
            dma((pieces,)),
            dma((pieces,)),
            dma((pieces,)),
            dma((pieces,)),
            dma((2, 2)),
            dma((2, 2)),
            dma((depth + 3 * n,)),
            dma((2, n)),
            dma((3,)),
            dma((nt,)),
            dma((2, pieces + 1, depth)),
            dma((pieces + 1, depth)),
            dma((3, pieces + 1)),
            dma((pieces + 1, nt)),
            dma((depth,)),
            dma((depth,)),
            dma((nt,)),
            dma((nt,)),
            dma((segments,)),
            dma((segments,)),
            dma((half // fine,)),
            dma((half // fine,)),
            dma((width // fine,)),
        ],
        compiler_params=pltpu.CompilerParams(
            collective_id=0, has_side_effects=True, vmem_limit_bytes=60 << 20
        ),
        name="layer",
    )(
        q_first, q_second, k_first, k_second, values, head_lambda, w_out, stream_in,
        norm_gain.reshape(1, width), mix, w_gate[0], w_up[0], s_gate, s_up, w_down[0], s_down,
    )


def layer(*arrays):
    n, nt = lax.axis_size("sp"), lax.axis_size("tp")
    k_first, values, w_gate, w_down, s_down = (arrays[i] for i in (3, 5, 11, 13, 16))
    fits = (
        4 <= n <= 16
        and n % 2 == 0
        and nt == 4
        and k_first.shape[1] == HEAD
        and w_gate.shape[0] == 1
        and w_down.shape[1] % (16 * nt) == 0
        and s_down.shape[0] % (16 * n) == 0
        and w_down.shape[1] % HEAD == 0
        and (2 * w_down.shape[1]) % s_down.shape[0] == 0
        and (nt * s_down.shape[0]) % (2 * w_down.shape[1]) == 0
        and w_down.shape[2] % (16 * HEAD) == 0
    )
    return near(*arrays) if fits else local(*arrays)


def solution(mesh):
    return jax.shard_map(
        layer,
        mesh=mesh,
        in_specs=(
            P(("sp", "tp"), None),
            P("sp", "tp"),
            P("sp", "tp"),
            P("sp", "tp"),
            P("sp", "tp"),
            P("sp", "tp"),
            P("tp"),
            P("tp", None),
            P(),
            P(("sp", "tp"), None),
            P(("sp", "tp"), None),
            P("sp", None, None),
            P("sp", None, None),
            P("sp", None, None),
            P(None, "tp"),
            P(None, "tp"),
            P("tp", None),
        ),
        out_specs=P(("sp", "tp"), None),
        check_vma=False,
    )
```

```python
import functools
import math

import jax
import jax.numpy as jnp
from jax import lax
from jax.experimental import pallas as pl
from jax.experimental.pallas import tpu as pltpu
from jax.sharding import PartitionSpec as P

HEAD = 128


FLOOR = -1e30


def absorb(state, first_q, second_q, first_k, second_k, value_rows, query_pos, key_pos):
    allowed = key_pos[None, :] <= query_pos[:, None]
    scale = first_q.shape[-1] ** (-0.5)
    result = []
    pairs = ((first_q, first_k), (second_q, second_k))
    for index in range(2):
        query_rows, key_rows = pairs[index]
        peak, total, accum = (state[3 * index], state[3 * index + 1], state[3 * index + 2])
        scores = (
            jnp.einsum("qagd,kad->agqk", query_rows, key_rows, preferred_element_type=jnp.float32)
            * scale
        )
        scores = jnp.where(allowed, scores, FLOOR)
        raised = jnp.maximum(peak, scores.max(-1))
        weights = jnp.where(allowed, jnp.exp(scores - raised[..., None]), 0.0)
        fade = jnp.exp(peak - raised)
        total = total * fade + weights.sum(-1)
        accum = accum * fade[..., None] + jnp.einsum(
            "agqk,kad->agqd",
            weights.astype(jnp.bfloat16),
            value_rows,
            preferred_element_type=jnp.float32,
        )
        result += [raised, total, accum]
    return tuple(result)


def empty_state(kv_local, group, count, value_dim):
    peaks = jnp.full((kv_local, group, count), FLOOR, jnp.float32)
    sums = jnp.zeros((kv_local, group, count), jnp.float32)
    accums = jnp.zeros((kv_local, group, count, value_dim), jnp.float32)
    return (peaks, sums, accums, peaks, sums, accums)


def fold_rows(state, first_q, second_q, query_pos, last_row, pieces, start):
    first_k, second_k, value_rows = pieces
    length = first_k.shape[0]
    kv_local = first_q.shape[1]
    value_dim = value_rows.shape[1] // kv_local
    span = math.gcd(length, 2048)

    def sweep(current):

        def visit(block, inner):
            begin = block * span
            key_one = lax.dynamic_slice_in_dim(first_k, begin, span, 0).reshape(
                span, kv_local, HEAD
            )
            key_two = lax.dynamic_slice_in_dim(second_k, begin, span, 0).reshape(
                span, kv_local, HEAD
            )
            value_part = lax.dynamic_slice_in_dim(value_rows, begin, span, 0).reshape(
                span, kv_local, value_dim
            )
            key_pos = begin + jnp.arange(span, dtype=jnp.int32)
            return absorb(
                inner, first_q, second_q, key_one, key_two, value_part, query_pos, key_pos
            )

        return lax.fori_loop(0, length // span, visit, current)

    def unchanged(current):
        return current

    return lax.cond(start <= last_row, sweep, unchanged, state)


def finish_heads(final, head_lambda):
    kv_local, group, count, value_dim = final[2].shape
    weight = head_lambda.reshape(kv_local, group, 1, 1)
    head_out = final[2] / final[1][..., None] - weight * final[5] / final[4][..., None]
    head_out = head_out * lax.rsqrt(jnp.mean(head_out * head_out, axis=-1, keepdims=True) + 1e-05)
    return (
        head_out.transpose(2, 0, 1, 3)
        .reshape(count, kv_local * group * value_dim)
        .astype(jnp.bfloat16)
    )


def shared_part(normed, s_gate, s_up, s_down):
    piece = lax.all_gather(normed, "tp", axis=0, tiled=True)
    gate_part = jnp.dot(piece, s_gate, preferred_element_type=jnp.float32)
    up_part = jnp.dot(piece, s_up, preferred_element_type=jnp.float32)
    hidden = (jax.nn.silu(gate_part) * up_part).astype(jnp.bfloat16)
    terms = jnp.dot(hidden, s_down, preferred_element_type=jnp.float32)
    return lax.psum_scatter(
        terms.astype(jnp.bfloat16), "tp", scatter_dimension=0, tiled=True
    ).astype(jnp.float32)


def routed_part(normed, routes, route_w, w_gate, w_up, w_down):
    rows, topk = routes.shape
    local_experts = w_gate.shape[0]
    experts = local_experts * lax.axis_size("sp")
    slots = max(2, 3 * rows * topk // (2 * experts))
    flat_ids = routes.reshape(-1)
    hits = (flat_ids[:, None] == jnp.arange(experts, dtype=jnp.int32)[None, :]).astype(jnp.int32)
    slot_of = jnp.sum(jnp.cumsum(hits, axis=0) * hits, axis=1) - 1
    target = flat_ids * slots + slot_of
    placing = jnp.any(
        jnp.arange(experts * slots, dtype=jnp.int32)[:, None, None]
        == target.reshape(rows, topk)[None, :, :],
        axis=-1,
    ).astype(jnp.bfloat16)
    outgoing = (
        jnp.dot(placing, normed, preferred_element_type=jnp.float32)
        .astype(jnp.bfloat16)
        .reshape(experts, slots, normed.shape[1])
    )
    arrived = lax.all_to_all(outgoing, "sp", split_axis=0, concat_axis=0, tiled=True)
    sources = arrived.shape[0] // local_experts
    grouped = arrived.reshape(sources, local_experts, arrived.shape[1], arrived.shape[2])
    gate_part = jnp.einsum("sjcd,jdf->sjcf", grouped, w_gate, preferred_element_type=jnp.float32)
    up_part = jnp.einsum("sjcd,jdf->sjcf", grouped, w_up, preferred_element_type=jnp.float32)
    hidden = (jax.nn.silu(gate_part) * up_part).astype(jnp.bfloat16)
    result = jnp.einsum(
        "sjcf,jfd->sjcd", hidden, w_down, preferred_element_type=jnp.float32
    ).astype(jnp.bfloat16)
    returned = lax.all_to_all(
        result.reshape(arrived.shape), "sp", split_axis=0, concat_axis=0, tiled=True
    )
    picked = (
        returned.reshape(experts * slots, normed.shape[1])[target]
        .reshape(rows, topk, normed.shape[1])
        .astype(jnp.float32)
    )
    return jnp.sum(picked * route_w[..., None], axis=1)


def local(
    stream_in,
    q_first,
    q_second,
    k_first,
    k_second,
    values,
    head_lambda,
    w_out,
    norm_gain,
    routes,
    route_w,
    w_gate,
    w_up,
    w_down,
    s_gate,
    s_up,
    s_down,
):
    seq_rows = q_first.shape[0]
    kv_local = k_first.shape[1] // HEAD
    heads_local = q_first.shape[1] // HEAD
    group = heads_local // kv_local
    value_dim = values.shape[1] // kv_local
    offset = lax.axis_index("sp") * seq_rows
    query_pos = offset + jnp.arange(seq_rows, dtype=jnp.int32)
    last_row = offset + seq_rows - 1
    first_q = q_first.reshape(seq_rows, kv_local, group, HEAD)
    second_q = q_second.reshape(seq_rows, kv_local, group, HEAD)
    start_state = empty_state(kv_local, group, seq_rows, value_dim)
    folded_state = fold_rows(
        start_state,
        first_q,
        second_q,
        query_pos,
        last_row,
        (
            lax.all_gather(k_first, "sp", axis=0, tiled=True),
            lax.all_gather(k_second, "sp", axis=0, tiled=True),
            lax.all_gather(values, "sp", axis=0, tiled=True),
        ),
        jnp.int32(0),
    )
    attn_rows = finish_heads(folded_state, head_lambda)
    attn = lax.psum_scatter(
        jnp.dot(attn_rows, w_out, preferred_element_type=jnp.float32).astype(jnp.bfloat16),
        "tp",
        scatter_dimension=0,
        tiled=True,
    ).astype(jnp.float32)
    resid = (stream_in.astype(jnp.float32) + attn).astype(jnp.bfloat16)
    stream = lax.optimization_barrier(resid).astype(jnp.float32)
    normed = (
        stream * lax.rsqrt(jnp.mean(stream * stream, axis=-1, keepdims=True) + 1e-06) * norm_gain
    ).astype(jnp.bfloat16)
    routed = routed_part(normed, routes, route_w, w_gate, w_up, w_down)
    shared = shared_part(normed, s_gate, s_up, s_down)
    return (stream + routed + shared).astype(jnp.bfloat16)


def mesh_copy(src, dst, send_sem, recv_sem, axis, target):
    return pltpu.make_async_remote_copy(
        src_ref=src,
        dst_ref=dst,
        send_sem=send_sem,
        recv_sem=recv_sem,
        device_id={axis: target},
        device_id_type=pl.DeviceIdType.MESH,
    )


def greet(axis, target):
    pl.semaphore_signal(
        pltpu.get_barrier_semaphore(),
        inc=1,
        device_id={axis: target},
        device_id_type=pl.DeviceIdType.MESH,
    )


def near_kernel(
    n, nt, group, pieces,
    q_one_h, q_two_h, k_one_h, k_two_h, val_h, lam, w_out_h, stream_h, gain_h, mix_h,
    gate_h, up_h, s_gate_h, s_up_h, down_h, s_down_h,
    out,
    q_one, q_two, k_one, k_two, val, stream, gain, mix_t,
    stacked, keys_one, keys_two, vals, peak, total, accum, rows_in,
    w, order, out_one, in_one, out_two, in_two, resid,
    gates, ups, s_gate, s_up, wall, gathered, beside, stat, stat_b,
    out_hid, in_hid, out_sh, in_sh, units, out_fin, in_fin, result, mix, square, extra, partial,
    load, send_kv, recv_kv, send_one, recv_one, send_two, recv_two,
    send_g, recv_g, send_d, recv_d, send_sd, recv_sd,
    send_x, recv_x, send_b, recv_b, send_h, recv_h, send_s, recv_s,
    send_u, recv_u, send_f, recv_f, save, send_e, recv_e,
):
    me, mine = lax.axis_index("sp"), lax.axis_index("tp")
    place, side = me // 2, me % 2
    far, core = mine // 2, mine % 2
    depth = n // 2
    pair, partner, across = me + 1 - 2 * side, mine + 1 - 2 * core, 2 * (1 - far) + core
    above, below = place < depth - 1, place > 0
    seq = q_one.shape[0]
    rows, width = stream.shape
    hid, wide = down_h.shape[0], s_down_h.shape[0]
    scale = HEAD ** (-0.5)
    half = width // 2

    def column(o):
        return 2 * ((place + o) % depth) + side

    def cols_of(f):
        return pl.ds(pl.multiple_of(f * half, half), half)

    loads = [
        pltpu.make_async_copy(source, target, load.at[i])
        for i, (source, target) in enumerate(
            (
                (w_out_h, w),
                (gate_h, gates.at[0]),
                (up_h, ups.at[0]),
                (s_gate_h, s_gate),
                (s_up_h, s_up),
                (
                    down_h.at[:, cols_of(far)],
                    wall.at[pl.ds(pl.multiple_of(me * hid, hid), hid)],
                ),
                (
                    s_down_h.at[:, cols_of(far)],
                    wall.at[pl.ds(pl.multiple_of(n * hid + mine * wide, wide), wide)],
                ),
            )
        )
    ]
    for o in range(1, depth):
        greet("sp", column(o))
    greet("sp", pair)
    greet("tp", across)
    greet("tp", partner)
    inputs = [
        pltpu.make_async_copy(source, target, load.at[7 + i])
        for i, (source, target) in enumerate(
            (
                (k_one_h, k_one),
                (k_two_h, k_two),
                (val_h, val),
                (q_one_h, q_one),
                (q_two_h, q_two),
                (stream_h, stream),
                (gain_h, gain),
                (mix_h, mix_t),
            )
        )
    ]
    for one in inputs:
        one.start()
    for one in inputs[:3]:
        one.wait()
    pl.semaphore_wait(pltpu.get_barrier_semaphore(), depth + 2)

    sources = (k_one, k_two, val)
    held = (keys_one, keys_two, vals)

    def copies(block, way, target, own):
        return [
            mesh_copy(
                sources[a] if own else held[a].at[block],
                held[a].at[block],
                send_kv.at[way, a, block // 2],
                recv_kv.at[a, block],
                "sp",
                target,
            )
            for a in range(3)
        ]

    def start(block, way, target, own=False):
        for one in copies(block, way, target, own):
            one.start()

    def arrive(block):
        for one in copies(block, 0, pair, False):
            one.wait_recv()

    share = width // 2
    share_at = pl.ds(pl.multiple_of(core * share, share), share)
    other_at = pl.ds(pl.multiple_of((1 - core) * share, share), share)

    def pair_weights():
        return [
            mesh_copy(
                h.at[share_at], v.at[1, share_at], send_g.at[0, i], recv_g.at[0, i], "sp", pair
            )
            for i, (h, v) in enumerate(((gate_h, gates), (up_h, ups)))
        ]

    def pair_weights_on(at):
        return [
            mesh_copy(
                v.at[1, at], v.at[1, at], send_g.at[1, i], recv_g.at[1, i], "tp", partner
            )
            for i, v in enumerate((gates, ups))
        ]

    part = hid // 2

    def down_at(block, c):
        return wall.at[pl.ds(pl.multiple_of(block * hid + c * part, part), part)]

    def down_own(way, target):
        return mesh_copy(
            down_h.at[pl.ds(pl.multiple_of(core * part, part), part), cols_of(far)],
            down_at(me, core),
            send_d.at[way],
            recv_d.at[0, me],
            "sp",
            target,
        )

    def down_pair(block):
        return mesh_copy(
            down_at(block, core),
            down_at(block, core),
            send_d.at[depth + block // 2],
            recv_d.at[0, block],
            "sp",
            pair,
        )

    def down_core(block, c):
        return mesh_copy(
            down_at(block, c),
            down_at(block, c),
            send_d.at[3 * depth + block],
            recv_d.at[1, block],
            "tp",
            partner,
        )

    def extra_at(s, c):
        return extra.at[pl.ds(pl.multiple_of(s * hid + c * part, part), part)]

    def extra_own():
        return mesh_copy(
            down_h.at[pl.ds(pl.multiple_of(core * part, part), part), cols_of(1 - far)],
            extra_at(side, core),
            send_e.at[0],
            recv_e.at[0, side],
            "sp",
            side,
        )

    def extra_pair(s):
        return mesh_copy(
            extra_at(s, core), extra_at(s, core), send_e.at[1], recv_e.at[0, s], "sp", pair
        )

    def extra_core(s, c):
        return mesh_copy(
            extra_at(s, c), extra_at(s, c), send_e.at[2 + s], recv_e.at[1, s], "tp", partner
        )

    def sd_at(u):
        return wall.at[pl.ds(pl.multiple_of(n * hid + u * wide, wide), wide)]

    def sd_own(way, f, target):
        return mesh_copy(
            s_down_h.at[:, cols_of(f)], sd_at(mine), send_sd.at[way], recv_sd.at[mine], "tp", target
        )

    def sd_on(u):
        return mesh_copy(sd_at(u), sd_at(u), send_sd.at[2], recv_sd.at[u], "tp", partner)

    @pl.when(above)
    def _():
        start(me, 0, me + 2, True)

    @pl.when(side == 0)
    def _():
        start(me, 1, pair, True)

    for one in loads:
        one.start()
    late = place >= depth // 2

    @pl.when(late)
    def _():
        sd_own(1, 1 - far, across).start()

    sd_own(0, far, partner).start()
    for o in range(1, depth):

        @pl.when(place + o >= depth)
        def _():
            down_own(o, column(o)).start()

    top_place = place == depth - 1
    pl.when(top_place)(lambda: extra_own().start())

    for one in inputs[3:]:
        one.wait()
    for index, q in enumerate((q_one, q_two)):
        for h in range(group):
            stacked[index, h * seq : (h + 1) * seq, :] = q[:, h * HEAD : (h + 1) * HEAD]

    def scores_of(index, keys):
        return (
            lax.dot_general(
                stacked[index], keys, (((1,), (1,)), ((), ())), preferred_element_type=jnp.float32
            )
            * scale
        )

    spread = (group * seq, seq)
    row_of = lax.broadcasted_iota(jnp.int32, spread, 0) % seq
    allowed = lax.broadcasted_iota(jnp.int32, spread, 1) <= row_of
    for index, keys in enumerate((k_one, k_two)):
        scores = jnp.where(allowed, scores_of(index, keys[...]), FLOOR)
        top = jnp.max(scores, axis=-1, keepdims=True)
        weights = jnp.exp(scores - top)
        peak[index] = top
        total[index] = jnp.sum(weights, axis=-1, keepdims=True)
        accum[index] = jnp.dot(
            weights.astype(jnp.bfloat16), val[...], preferred_element_type=jnp.float32
        )

    def fold(block):
        for index in range(2):
            scores = scores_of(index, held[index][block])
            old = peak[index]
            top = jnp.maximum(old, jnp.max(scores, axis=-1, keepdims=True))
            weights = jnp.exp(scores - top)
            fade = jnp.exp(old - top)
            peak[index] = top
            total[index] = total[index] * fade + jnp.sum(weights, axis=-1, keepdims=True)
            accum[index] = accum[index] * fade + jnp.dot(
                weights.astype(jnp.bfloat16), vals[block], preferred_element_type=jnp.float32
            )

    def down_up(block):
        return mesh_copy(
            down_at(block, core),
            down_at(block, core),
            send_d.at[2 * depth + block // 2],
            recv_d.at[0, block],
            "sp",
            me + 2,
        )

    def lift(d):
        @pl.when((place >= d) & above)
        def _():
            down_up(me - 2 * d).wait_recv()
            down_up(me - 2 * d).start()

    def weights_out():
        pl.when(above)(lambda: down_own(1, me + 2).start())
        for one in pair_weights():
            one.start()
        down_own(0, pair).start()
        lift(1)

    pl.when(place == 0)(weights_out)

    def visit(e, carry):
        @pl.when(place >= e)
        def _():
            block = me - 2 * e
            for up, over in zip(copies(block, 0, me + 2, False), copies(block, 1, pair, False)):
                over.wait_recv()
                pl.when(above)(up.start)
                over.start()
            pl.when(e == place)(weights_out)
            fold(block)

        @pl.when((place >= e - 1) & ((e > 1) | (side == 1)))
        def _():
            block = pair - 2 * (e - 1)
            arrive(block)
            fold(block)

        return carry

    lax.fori_loop(1, depth + 1, visit, 0)

    for d in range(2, depth):
        lift(d)

    for h in range(group):
        cut = slice(h * seq, (h + 1) * seq)
        head = accum[0, cut, :] / total[0, cut, :] - lam[h] * (
            accum[1, cut, :] / total[1, cut, :]
        )
        head = head * lax.rsqrt(jnp.mean(head * head, axis=-1, keepdims=True) + 1e-05)
        size = head.shape[1]
        rows_in[:, h * size : (h + 1) * size] = head.astype(jnp.bfloat16)

    for o in range(2):
        base = 2 * ((far + o) % 2)
        for which, parity in enumerate((1 - core, core)):
            begin = pl.multiple_of((base + parity) * rows, rows)
            order[which, o * rows : (o + 1) * rows, :] = rows_in[pl.ds(begin, rows), :]

    first = [
        mesh_copy(out_one.at[i], in_one.at[i], send_one.at[0], recv_one.at[i], "tp", partner)
        for i in range(pieces)
    ]
    second = [
        mesh_copy(out_two.at[i], in_two.at[i], send_two.at[0], recv_two.at[i], "tp", across)
        for i in range(pieces)
    ]
    span = width // pieces
    loads[0].wait()
    for i in range(pieces):
        out_one[i] = jnp.dot(
            order[0], w[:, i * span : (i + 1) * span], preferred_element_type=jnp.float32
        ).astype(jnp.bfloat16)
        first[i].start()
    kept = []
    for i in range(pieces):
        sums = jnp.dot(
            order[1], w[:, i * span : (i + 1) * span], preferred_element_type=jnp.float32
        )
        first[i].wait_recv()
        sums = sums + in_one[i].astype(jnp.float32)
        out_two[i] = sums[rows:].astype(jnp.bfloat16)
        second[i].start()
        kept.append(sums[:rows])

    @pl.when(jnp.logical_not(late))
    def _():
        sd_own(1, 1 - far, across).start()

    def row_part(block, extra, spot, i):
        return block.at[spot, i] if i < pieces else extra.at[spot]

    def row_copy(spot, way, target, i):
        some = row_part(gathered, stat, spot, i)
        return mesh_copy(
            some,
            some,
            send_x.at[way, i // pieces, spot],
            recv_x.at[i, spot],
            "sp",
            target,
        )

    def rows_sent(spot, way):
        for some, kind in ((gathered.at[spot], 0), (stat.at[spot], 1)):
            mesh_copy(
                some, some, send_x.at[way, kind, spot], recv_x.at[0, spot], "sp", pair
            ).wait_send()

    def beside_own(way, target, i):
        return mesh_copy(
            row_part(gathered, stat, place, i),
            row_part(beside, stat_b, mine, i),
            send_b.at[way, i // pieces],
            recv_b.at[i // pieces, mine],
            "tp",
            target,
        )

    def beside_on(u, kind, way=2):
        some = (beside, stat_b)[kind].at[u]
        return mesh_copy(some, some, send_b.at[way, kind], recv_b.at[kind, u], "tp", partner)

    def raise_row(e, i):
        row_copy(place - e, 0, pair, i).wait_recv()
        row_copy(place - e, 0, me + 2, i).start()

    def lower_row(e, i):
        row_copy(place + e, 0, pair, i).wait_recv()
        row_copy(place + e, 1, me - 2, i).start()

    def rows_out(i):
        pl.when(above)(lambda: row_copy(place, 0, me + 2, i).start())
        pl.when(below)(lambda: row_copy(place, 1, me - 2, i).start())
        beside_own(1, across, i).start()
        beside_own(0, partner, i).start()

    fine = resid.shape[2]
    per = span // fine
    squares = jnp.zeros((rows, 1), jnp.float32)
    for i in range(pieces):
        cut = slice(i * span, (i + 1) * span)
        second[i].wait_recv()
        sums = kept[i] + in_two[i].astype(jnp.float32)
        sums = (stream[:, cut].astype(jnp.float32) + sums).astype(jnp.bfloat16)
        for j in range(per):
            resid[i * per + j] = sums[:, j * fine : (j + 1) * fine]
        sums = sums.astype(jnp.float32)
        squares = squares + jnp.sum(sums * sums, axis=-1, keepdims=True)
        gathered[place, i] = (sums * gain[:, cut]).astype(jnp.bfloat16)
        rows_out(i)
    shrink = lax.rsqrt(squares / width + 1e-06)
    stat[place] = jnp.broadcast_to(shrink, stat.shape[1:])
    rows_out(pieces)
    for e in range(1, depth - 1):
        for i in range(pieces + 1):
            pl.when(above & (place >= e))(lambda: raise_row(e, i))
            if e == depth - 2:
                pl.when(above & below)(lambda: lower_row(1, i))


    def pass_down(e):
        def one(block, fresh):
            pl.when(fresh)(lambda: down_pair(block).wait_recv())
            down_pair(block).start()
            down_core(block, core).start()

        pl.when(place >= e)(lambda: one(me - 2 * e, jnp.logical_not(above)))
        pl.when(place + e < depth)(lambda: one(me + 2 * e, place >= 0))

    def collect(e):
        def one(block):
            down_pair(block).wait_recv()
            down_core(block, core).start()

        pl.when(place >= e)(lambda: one(pair - 2 * e))
        pl.when(place + e < depth)(lambda: one(pair + 2 * e))

    def hidden_of(block, spot, scales, g, u):
        def project(m):
            parts = [
                jnp.dot(
                    block[spot, i],
                    m[i * span : (i + 1) * span, :],
                    preferred_element_type=jnp.float32,
                )
                for i in range(pieces)
            ]
            return sum(parts[1:], parts[0]) * scales[spot][:, :1]

        gate_part, up_part = project(g), project(u)
        return (gate_part / (1.0 + jnp.exp(-gate_part)) * up_part).astype(jnp.bfloat16)

    square[...] = jnp.zeros_like(square)
    square[0:n, 0:rows] = mix_t[...]
    turned = square[...].T
    for j in range(n):
        mix[j] = jnp.broadcast_to(turned[0:rows, j : j + 1], mix.shape[1:])
    for i in range(1, 5):
        loads[i].wait()

    def hid_copy(spot):
        return mesh_copy(
            out_hid.at[spot], in_hid.at[place], send_h.at[spot], recv_h.at[place], "sp",
            2 * spot + side,
        )

    def serve(spot):
        out_hid[spot, side] = hidden_of(gathered, spot, stat, gates.at[0], ups.at[0])
        out_hid[spot, 1 - side] = hidden_of(gathered, spot, stat, gates.at[1], ups.at[1])
        hid_copy(spot).start()

    def sh_copy(u):
        return mesh_copy(
            out_sh.at[u], in_sh.at[mine], send_s.at[u], recv_s.at[mine], "tp", u
        )

    def answer(u):
        out_sh[u] = hidden_of(beside, u, stat_b, s_gate, s_up)
        sh_copy(u).start()

    def turn(e, carry):
        low, high = place >= e, place + e < depth

        @pl.when(low & jnp.logical_not(above))
        def _():
            for i in range(pieces + 1):
                row_copy(place - e, 0, pair, i).wait_recv()

        @pl.when(high)
        def _():
            for i in range(pieces + 1):
                pl.when(below & (e > 1))(lambda: lower_row(e, i))
                pl.when(jnp.logical_not(below))(
                    lambda: row_copy(place + e, 0, pair, i).wait_recv()
                )

        @pl.when(e == 1)
        def _():
            for one, onward in zip(pair_weights(), pair_weights_on(share_at)):
                one.wait_recv()
                onward.start()
            pass_down(1)
            in_sh[mine] = hidden_of(gathered, place, stat, s_gate, s_up)
            in_hid[place, side] = hidden_of(gathered, place, stat, gates.at[0], ups.at[0])
            for one in pair_weights_on(other_at):
                one.wait_recv()

        @pl.when(low)
        def _():
            serve(place - e)

        @pl.when(high)
        def _():
            serve(place + e)

        pass_down(e + 1)

        @pl.when(e == 2)
        def _():
            down_pair(pair).wait_recv()
            down_core(pair, core).start()
            in_hid[place, 1 - side] = hidden_of(gathered, place, stat, gates.at[1], ups.at[1])
            u = across
            for kind in range(2):
                beside_on(u, kind).wait_recv()
                beside_on(u, kind).start()
            answer(u)
            sd_on(u).wait_recv()
            sd_on(u).start()
            for o in range(2):
                u = 2 * ((far + o) % 2) + 1 - core
                for kind in range(2):
                    beside_on(u, kind).wait_recv()
                answer(u)

        return carry

    @pl.when(place == 0)
    def _():
        extra_pair(side).wait_recv()
        extra_pair(side).start()
        extra_core(side, core).start()

    lax.fori_loop(1, depth - 1, turn, 0)
    last = depth - 1

    @pl.when(place == 0)
    def _():
        for i in range(pieces + 1):
            row_copy(last, 0, pair, i).wait_recv()
        serve(last)

    segments = units.shape[1]

    def unit_copy(s):
        return mesh_copy(
            units.at[0, s], units.at[1, s], send_u.at[s], recv_u.at[s], "tp", across
        )

    for o in range(1, nt):
        u = (mine + o) % nt
        mesh_copy(
            out_sh.at[u], in_sh.at[u], send_s.at[u], recv_s.at[u], "tp", u
        ).wait_recv()
    seg = units.shape[3]
    for j in range(nt):
        at = j * wide
        units[0, depth + at // seg, :, at % seg : at % seg + wide] = in_sh[j]
    for s in range(depth, segments):
        unit_copy(s).start()

    for e in range(1, depth - 1):
        collect(e)

    def place_unit(spot):
        @pl.when(place != spot)
        def _():
            mesh_copy(
                out_hid.at[spot], in_hid.at[spot], send_h.at[spot], recv_h.at[spot], "sp",
                2 * spot + side,
            ).wait_recv()

        for k in range(2):
            j = 2 * spot + k
            units[0, spot, :, k * hid : (k + 1) * hid] = (
                in_hid[spot, k].astype(jnp.float32) * mix[j][:, :1]
            ).astype(jnp.bfloat16)

    for spot in range(last - 1, -1, -1):
        place_unit(spot)
        unit_copy(spot).start()

    @pl.when(place != 0)
    def _():
        place_unit(last)
        unit_copy(last).start()

    @pl.when(top_place)
    def _():
        for i in range(pieces + 1):
            row_copy(0, 0, pair, i).wait_recv()
        serve(0)

    @pl.when(place == 0)
    def _():
        extra_pair(1 - side).wait_recv()
        extra_core(1 - side, core).start()

    collect(last)

    loads[5].wait()
    loads[6].wait()
    for o in range(2):
        sd_on(2 * ((far + o) % 2) + 1 - core).wait_recv()

    def receive_down(block, carry):
        @pl.when(block != me)
        def _():
            down_core(block, 1 - core).wait_recv()

        return carry

    lax.fori_loop(0, n, receive_down, 0)
    early = [s for s in range(segments) if s != last]
    for s in early:
        unit_copy(s).wait_recv()

    def fin_copy(i):
        return mesh_copy(out_fin.at[i], in_fin.at[i], send_f.at[0], recv_f.at[i], "tp", across)

    def put(spot):
        return pltpu.make_async_copy(
            result.at[spot],
            out.at[:, pl.ds(pl.multiple_of(spot * fine, fine), fine)],
            save.at[spot],
        )

    count = half // fine
    mine_at, other_of = far * count, (1 - far) * count
    for i in range(count):
        cut = slice(i * fine, (i + 1) * fine)
        terms = [
            jnp.dot(
                units[:, s].reshape(2 * rows, seg),
                wall[s * seg : (s + 1) * seg, cut],
                preferred_element_type=jnp.float32,
            )
            for s in early
        ]
        both = sum(terms[1:], terms[0])
        partial[i] = both

        @pl.when(place == 0)
        def _():
            out_fin[i] = both[rows:].astype(jnp.bfloat16)
            fin_copy(i).start()

    def close(spot, terms):
        result[spot] = (resid[spot].astype(jnp.float32) + terms).astype(jnp.bfloat16)
        put(spot).start()

    @pl.when(place == 0)
    def _():
        extra_core(0, 1 - core).wait_recv()
        extra_core(1, 1 - core).wait_recv()
        for i in range(count):
            fin_copy(i).wait_recv()
        place_unit(last)
        rest = units[0, last]
        for i in range(count):
            cut = slice(i * fine, (i + 1) * fine)
            terms = jnp.dot(
                rest, wall[last * seg : (last + 1) * seg, cut], preferred_element_type=jnp.float32
            )
            close(mine_at + i, partial[i, :rows] + terms)
            terms = jnp.dot(rest, extra[:, cut], preferred_element_type=jnp.float32)
            close(other_of + i, in_fin[i].astype(jnp.float32) + terms)

    @pl.when(place != 0)
    def _():
        unit_copy(last).wait_recv()
        for i in range(count):
            cut = slice(i * fine, (i + 1) * fine)
            both = partial[i] + jnp.dot(
                units[:, last].reshape(2 * rows, seg),
                wall[last * seg : (last + 1) * seg, cut],
                preferred_element_type=jnp.float32,
            )
            out_fin[i] = both[rows:].astype(jnp.bfloat16)
            fin_copy(i).start()
            close(mine_at + i, both[:rows])
        for i in range(count):
            fin_copy(i).wait_recv()
            close(other_of + i, in_fin[i].astype(jnp.float32))

    def settle(e, carry):
        @pl.when(place >= e)
        def _():
            block = me - 2 * e

            @pl.when(above)
            def _():
                for one in copies(block, 0, me + 2, False):
                    one.wait_send()

                @pl.when(e > 0)
                def _():
                    down_up(block).wait_send()

            @pl.when((e > 0) | (side == 0))
            def _():
                for one in copies(block, 1, pair, False):
                    one.wait_send()

        pl.when((place + e < depth) & below)(lambda: rows_sent(place + e, 1))
        pl.when((place >= e) & above)(lambda: rows_sent(place - e, 0))

        @pl.when(e != place)
        def _():
            hid_copy(e).wait_send()
            down_pair(2 * e + side).wait_send()

        return carry

    lax.fori_loop(0, depth, settle, 0)

    def settle_down(block, carry):
        @pl.when(block != me)
        def _():
            down_core(block, core).wait_send()

        return carry

    lax.fori_loop(0, n, settle_down, 0)
    for one in pair_weights() + pair_weights_on(share_at):
        one.wait_send()
    for some, sem, rec in (
        (out_one, send_one.at[0], recv_one.at[0]),
        (out_two, send_two.at[0], recv_two.at[0]),
        (out_fin, send_f.at[0], recv_f.at[0]),
    ):
        mesh_copy(some, some, sem, rec, "tp", partner).wait_send()
    for o in range(1, depth):
        pl.when((place + o >= depth) | (o == 1))(lambda: down_own(o, column(o)).wait_send())
    down_own(0, pair).wait_send()
    sd_own(0, far, partner).wait_send()
    sd_own(1, 1 - far, across).wait_send()
    sd_on(across).wait_send()
    for kind in range(2):
        for way in range(3):
            beside_on(across, kind, way).wait_send()
    for o in range(1, nt):
        sh_copy((mine + o) % nt).wait_send()
    for s in early:
        unit_copy(s).wait_send()
    pl.when(place != 0)(lambda: unit_copy(last).wait_send())
    pl.when(top_place)(lambda: extra_own().wait_send())

    @pl.when(place == 0)
    def _():
        extra_pair(side).wait_send()
        extra_core(0, core).wait_send()
        extra_core(1, core).wait_send()

    for i in range(2 * count):
        put(i).wait()


def near(
    stream_in,
    q_first,
    q_second,
    k_first,
    k_second,
    values,
    head_lambda,
    w_out,
    norm_gain,
    routes,
    route_w,
    w_gate,
    w_up,
    w_down,
    s_gate,
    s_up,
    s_down,
):
    n, nt = lax.axis_size("sp"), lax.axis_size("tp")
    depth = n // 2
    seq, rows, width = q_first.shape[0], stream_in.shape[0], stream_in.shape[1]
    group, value_dim = q_first.shape[1] // HEAD, values.shape[1]
    hid, wide = w_down.shape[1], s_down.shape[0]
    tall, features = group * seq, group * value_dim
    pieces = 4
    span = width // pieces
    half, fine = width // 2, width // 8
    seg = 2 * hid
    segments = depth + nt * wide // seg
    chosen = routes.T[None, :, :] == jnp.arange(n, dtype=jnp.int32)[:, None, None]
    mix_t = jnp.sum(jnp.where(chosen, route_w.T[None, :, :], 0.0), axis=1)
    smem = pl.BlockSpec(memory_space=pltpu.SMEM)
    hbm = pl.BlockSpec(memory_space=pl.ANY)
    low, high = jnp.bfloat16, jnp.float32
    dma = pltpu.SemaphoreType.DMA
    return pl.pallas_call(
        functools.partial(near_kernel, n, nt, group, pieces),
        out_shape=jax.ShapeDtypeStruct((rows, width), low),
        in_specs=[hbm] * 5 + [smem] + [hbm] * 10,
        out_specs=hbm,
        scratch_shapes=[
            pltpu.VMEM((seq, group * HEAD), low),
            pltpu.VMEM((seq, group * HEAD), low),
            pltpu.VMEM((seq, HEAD), low),
            pltpu.VMEM((seq, HEAD), low),
            pltpu.VMEM((seq, value_dim), low),
            pltpu.VMEM((rows, width), low),
            pltpu.VMEM((1, width), high),
            pltpu.VMEM((n, rows), high),
            pltpu.VMEM((2, tall, HEAD), low),
            pltpu.VMEM((n, seq, HEAD), low),
            pltpu.VMEM((n, seq, HEAD), low),
            pltpu.VMEM((n, seq, value_dim), low),
            pltpu.VMEM((2, tall, 1), high),
            pltpu.VMEM((2, tall, 1), high),
            pltpu.VMEM((2, tall, value_dim), high),
            pltpu.VMEM((seq, features), low),
            pltpu.VMEM((features, width), low),
            pltpu.VMEM((2, 2 * rows, features), low),
            pltpu.VMEM((pieces, 2 * rows, span), low),
            pltpu.VMEM((pieces, 2 * rows, span), low),
            pltpu.VMEM((pieces, rows, span), low),
            pltpu.VMEM((pieces, rows, span), low),
            pltpu.VMEM((width // fine, rows, fine), low),
            pltpu.VMEM((2, width, hid), low),
            pltpu.VMEM((2, width, hid), low),
            pltpu.VMEM((width, wide), low),
            pltpu.VMEM((width, wide), low),
            pltpu.VMEM((n * hid + nt * wide, half), low),
            pltpu.VMEM((depth, pieces, rows, span), low),
            pltpu.VMEM((nt, pieces, rows, span), low),
            pltpu.VMEM((depth, rows, HEAD), high),
            pltpu.VMEM((nt, rows, HEAD), high),
            pltpu.VMEM((depth, 2, rows, hid), low),
            pltpu.VMEM((depth, 2, rows, hid), low),
            pltpu.VMEM((nt, rows, wide), low),
            pltpu.VMEM((nt, rows, wide), low),
            pltpu.VMEM((2, segments, rows, seg), low),
            pltpu.VMEM((half // fine, rows, fine), low),
            pltpu.VMEM((half // fine, rows, fine), low),
            pltpu.VMEM((width // fine, rows, fine), low),
            pltpu.VMEM((n, rows, HEAD), high),
            pltpu.VMEM((HEAD, HEAD), high),
            pltpu.VMEM((2 * hid, half), low),
            pltpu.VMEM((half // fine, 2 * rows, fine), high),
            dma((15,)),
            dma((2, 3, depth)),
            dma((3, n)),
            dma((1,)),
            dma((pieces,)),
            dma((1,)),
            dma((pieces,)),
            dma((2, 2)),
            dma((2, 2)),
            dma((3 * depth + n,)),
            dma((2, n)),
            dma((3,)),
            dma((nt,)),
            dma((2, 2, depth)),
            dma((pieces + 1, depth)),
            dma((3, 2)),
            dma((2, nt)),
            dma((depth,)),
            dma((depth,)),
            dma((nt,)),
            dma((nt,)),
            dma((segments,)),
            dma((segments,)),
            dma((1,)),
            dma((half // fine,)),
            dma((width // fine,)),
            dma((4,)),
            dma((2, 2)),
        ],
        compiler_params=pltpu.CompilerParams(
            collective_id=0, has_side_effects=True, vmem_limit_bytes=60 << 20
        ),
        name="layer",
    )(
        q_first, q_second, k_first, k_second, values, head_lambda, w_out, stream_in,
        norm_gain.reshape(1, width), mix_t, w_gate[0], w_up[0], s_gate, s_up, w_down[0], s_down,
    )


def layer(*arrays):
    n, nt = lax.axis_size("sp"), lax.axis_size("tp")
    k_first, values, w_gate, w_down, s_down = (arrays[i] for i in (3, 5, 11, 13, 16))
    fits = (
        4 <= n <= 16
        and n % 2 == 0
        and nt == 4
        and k_first.shape[1] == HEAD
        and arrays[0].shape[0] <= HEAD
        and w_gate.shape[0] == 1
        and w_down.shape[1] % (16 * nt) == 0
        and s_down.shape[0] % (16 * n) == 0
        and w_down.shape[1] % HEAD == 0
        and (2 * w_down.shape[1]) % s_down.shape[0] == 0
        and (nt * s_down.shape[0]) % (2 * w_down.shape[1]) == 0
        and w_down.shape[2] % (16 * HEAD) == 0
    )
    return near(*arrays) if fits else local(*arrays)


def solution(mesh):
    return jax.shard_map(
        layer,
        mesh=mesh,
        in_specs=(
            P(("sp", "tp"), None),
            P("sp", "tp"),
            P("sp", "tp"),
            P("sp", "tp"),
            P("sp", "tp"),
            P("sp", "tp"),
            P("tp"),
            P("tp", None),
            P(),
            P(("sp", "tp"), None),
            P(("sp", "tp"), None),
            P("sp", None, None),
            P("sp", None, None),
            P("sp", None, None),
            P(None, "tp"),
            P(None, "tp"),
            P("tp", None),
        ),
        out_specs=P(("sp", "tp"), None),
        check_vma=False,
    )
```

```python
import functools
import math

import jax
import jax.numpy as jnp
from jax import lax
from jax.experimental import pallas as pl
from jax.experimental.pallas import tpu as pltpu
from jax.sharding import PartitionSpec as P

HEAD = 128


FLOOR = -1e30


def absorb(state, first_q, second_q, first_k, second_k, value_rows, query_pos, key_pos):
    allowed = key_pos[None, :] <= query_pos[:, None]
    scale = first_q.shape[-1] ** (-0.5)
    result = []
    pairs = ((first_q, first_k), (second_q, second_k))
    for index in range(2):
        query_rows, key_rows = pairs[index]
        peak, total, accum = (state[3 * index], state[3 * index + 1], state[3 * index + 2])
        scores = (
            jnp.einsum("qagd,kad->agqk", query_rows, key_rows, preferred_element_type=jnp.float32)
            * scale
        )
        scores = jnp.where(allowed, scores, FLOOR)
        raised = jnp.maximum(peak, scores.max(-1))
        weights = jnp.where(allowed, jnp.exp(scores - raised[..., None]), 0.0)
        fade = jnp.exp(peak - raised)
        total = total * fade + weights.sum(-1)
        accum = accum * fade[..., None] + jnp.einsum(
            "agqk,kad->agqd",
            weights.astype(jnp.bfloat16),
            value_rows,
            preferred_element_type=jnp.float32,
        )
        result += [raised, total, accum]
    return tuple(result)


def empty_state(kv_local, group, count, value_dim):
    peaks = jnp.full((kv_local, group, count), FLOOR, jnp.float32)
    sums = jnp.zeros((kv_local, group, count), jnp.float32)
    accums = jnp.zeros((kv_local, group, count, value_dim), jnp.float32)
    return (peaks, sums, accums, peaks, sums, accums)


def fold_rows(state, first_q, second_q, query_pos, last_row, pieces, start):
    first_k, second_k, value_rows = pieces
    length = first_k.shape[0]
    kv_local = first_q.shape[1]
    value_dim = value_rows.shape[1] // kv_local
    span = math.gcd(length, 2048)

    def sweep(current):

        def visit(block, inner):
            begin = block * span
            key_one = lax.dynamic_slice_in_dim(first_k, begin, span, 0).reshape(
                span, kv_local, HEAD
            )
            key_two = lax.dynamic_slice_in_dim(second_k, begin, span, 0).reshape(
                span, kv_local, HEAD
            )
            value_part = lax.dynamic_slice_in_dim(value_rows, begin, span, 0).reshape(
                span, kv_local, value_dim
            )
            key_pos = begin + jnp.arange(span, dtype=jnp.int32)
            return absorb(
                inner, first_q, second_q, key_one, key_two, value_part, query_pos, key_pos
            )

        return lax.fori_loop(0, length // span, visit, current)

    def unchanged(current):
        return current

    return lax.cond(start <= last_row, sweep, unchanged, state)


def finish_heads(final, head_lambda):
    kv_local, group, count, value_dim = final[2].shape
    weight = head_lambda.reshape(kv_local, group, 1, 1)
    head_out = final[2] / final[1][..., None] - weight * final[5] / final[4][..., None]
    head_out = head_out * lax.rsqrt(jnp.mean(head_out * head_out, axis=-1, keepdims=True) + 1e-05)
    return (
        head_out.transpose(2, 0, 1, 3)
        .reshape(count, kv_local * group * value_dim)
        .astype(jnp.bfloat16)
    )


def shared_part(normed, s_gate, s_up, s_down):
    piece = lax.all_gather(normed, "tp", axis=0, tiled=True)
    gate_part = jnp.dot(piece, s_gate, preferred_element_type=jnp.float32)
    up_part = jnp.dot(piece, s_up, preferred_element_type=jnp.float32)
    hidden = (jax.nn.silu(gate_part) * up_part).astype(jnp.bfloat16)
    terms = jnp.dot(hidden, s_down, preferred_element_type=jnp.float32)
    return lax.psum_scatter(
        terms.astype(jnp.bfloat16), "tp", scatter_dimension=0, tiled=True
    ).astype(jnp.float32)


def routed_part(normed, routes, route_w, w_gate, w_up, w_down):
    rows, topk = routes.shape
    local_experts = w_gate.shape[0]
    experts = local_experts * lax.axis_size("sp")
    slots = max(2, 3 * rows * topk // (2 * experts))
    flat_ids = routes.reshape(-1)
    hits = (flat_ids[:, None] == jnp.arange(experts, dtype=jnp.int32)[None, :]).astype(jnp.int32)
    slot_of = jnp.sum(jnp.cumsum(hits, axis=0) * hits, axis=1) - 1
    target = flat_ids * slots + slot_of
    placing = jnp.any(
        jnp.arange(experts * slots, dtype=jnp.int32)[:, None, None]
        == target.reshape(rows, topk)[None, :, :],
        axis=-1,
    ).astype(jnp.bfloat16)
    outgoing = (
        jnp.dot(placing, normed, preferred_element_type=jnp.float32)
        .astype(jnp.bfloat16)
        .reshape(experts, slots, normed.shape[1])
    )
    arrived = lax.all_to_all(outgoing, "sp", split_axis=0, concat_axis=0, tiled=True)
    sources = arrived.shape[0] // local_experts
    grouped = arrived.reshape(sources, local_experts, arrived.shape[1], arrived.shape[2])
    gate_part = jnp.einsum("sjcd,jdf->sjcf", grouped, w_gate, preferred_element_type=jnp.float32)
    up_part = jnp.einsum("sjcd,jdf->sjcf", grouped, w_up, preferred_element_type=jnp.float32)
    hidden = (jax.nn.silu(gate_part) * up_part).astype(jnp.bfloat16)
    result = jnp.einsum(
        "sjcf,jfd->sjcd", hidden, w_down, preferred_element_type=jnp.float32
    ).astype(jnp.bfloat16)
    returned = lax.all_to_all(
        result.reshape(arrived.shape), "sp", split_axis=0, concat_axis=0, tiled=True
    )
    picked = (
        returned.reshape(experts * slots, normed.shape[1])[target]
        .reshape(rows, topk, normed.shape[1])
        .astype(jnp.float32)
    )
    return jnp.sum(picked * route_w[..., None], axis=1)


def local(
    stream_in,
    q_first,
    q_second,
    k_first,
    k_second,
    values,
    head_lambda,
    w_out,
    norm_gain,
    routes,
    route_w,
    w_gate,
    w_up,
    w_down,
    s_gate,
    s_up,
    s_down,
):
    seq_rows = q_first.shape[0]
    kv_local = k_first.shape[1] // HEAD
    heads_local = q_first.shape[1] // HEAD
    group = heads_local // kv_local
    value_dim = values.shape[1] // kv_local
    offset = lax.axis_index("sp") * seq_rows
    query_pos = offset + jnp.arange(seq_rows, dtype=jnp.int32)
    last_row = offset + seq_rows - 1
    first_q = q_first.reshape(seq_rows, kv_local, group, HEAD)
    second_q = q_second.reshape(seq_rows, kv_local, group, HEAD)
    start_state = empty_state(kv_local, group, seq_rows, value_dim)
    folded_state = fold_rows(
        start_state,
        first_q,
        second_q,
        query_pos,
        last_row,
        (
            lax.all_gather(k_first, "sp", axis=0, tiled=True),
            lax.all_gather(k_second, "sp", axis=0, tiled=True),
            lax.all_gather(values, "sp", axis=0, tiled=True),
        ),
        jnp.int32(0),
    )
    attn_rows = finish_heads(folded_state, head_lambda)
    attn = lax.psum_scatter(
        jnp.dot(attn_rows, w_out, preferred_element_type=jnp.float32).astype(jnp.bfloat16),
        "tp",
        scatter_dimension=0,
        tiled=True,
    ).astype(jnp.float32)
    resid = (stream_in.astype(jnp.float32) + attn).astype(jnp.bfloat16)
    stream = lax.optimization_barrier(resid).astype(jnp.float32)
    normed = (
        stream * lax.rsqrt(jnp.mean(stream * stream, axis=-1, keepdims=True) + 1e-06) * norm_gain
    ).astype(jnp.bfloat16)
    routed = routed_part(normed, routes, route_w, w_gate, w_up, w_down)
    shared = shared_part(normed, s_gate, s_up, s_down)
    return (stream + routed + shared).astype(jnp.bfloat16)


def mesh_copy(src, dst, send_sem, recv_sem, axis, target):
    return pltpu.make_async_remote_copy(
        src_ref=src,
        dst_ref=dst,
        send_sem=send_sem,
        recv_sem=recv_sem,
        device_id={axis: target},
        device_id_type=pl.DeviceIdType.MESH,
    )


def greet(axis, target):
    pl.semaphore_signal(
        pltpu.get_barrier_semaphore(),
        inc=1,
        device_id={axis: target},
        device_id_type=pl.DeviceIdType.MESH,
    )


def near_kernel(
    n, nt, group, pieces,
    q_one_h, q_two_h, k_one_h, k_two_h, val_h, lam, w_out_h, stream_h, gain_h, route_h, share_h,
    gate_h, up_h, s_gate_h, s_up_h, down_h, s_down_h,
    out,
    q_one, q_two, k_one, k_two, val, stream, gain, route_t, share_t,
    stacked, keys_one, keys_two, vals, peak, total, accum, rows_in,
    w, order, out_one, in_one, out_two, in_two, resid,
    gates, ups, s_gate, s_up, wall, gathered, beside, stat, stat_b,
    out_hid, in_hid, out_sh, in_sh, units, out_fin, in_fin, result, mix, square, extra, partial,
    load, send_kv, recv_kv, send_one, recv_one, send_two, recv_two,
    send_g, recv_g, send_d, recv_d, send_sd, recv_sd,
    send_x, recv_x, send_b, recv_b, send_h, recv_h, send_s, recv_s,
    send_u, recv_u, send_f, recv_f, save, send_e, recv_e,
):
    me, mine = lax.axis_index("sp"), lax.axis_index("tp")
    place, side = me // 2, me % 2
    far, core = mine // 2, mine % 2
    depth = n // 2
    pair, partner, across = me + 1 - 2 * side, mine + 1 - 2 * core, 2 * (1 - far) + core
    above, below = place < depth - 1, place > 0
    seq = q_one.shape[0]
    rows, width = stream.shape
    hid, wide = down_h.shape[0], s_down_h.shape[0]
    scale = HEAD ** (-0.5)
    half = width // 2

    def column(o):
        return 2 * ((place + o) % depth) + side

    def cols_of(f):
        return pl.ds(pl.multiple_of(f * half, half), half)

    loads = [
        pltpu.make_async_copy(source, target, load.at[i])
        for i, (source, target) in enumerate(
            (
                (w_out_h, w),
                (gate_h, gates.at[0]),
                (up_h, ups.at[0]),
                (s_gate_h, s_gate),
                (s_up_h, s_up),
                (
                    down_h.at[:, cols_of(far)],
                    wall.at[pl.ds(pl.multiple_of(me * hid, hid), hid)],
                ),
                (
                    s_down_h.at[:, cols_of(far)],
                    wall.at[pl.ds(pl.multiple_of(n * hid + mine * wide, wide), wide)],
                ),
            )
        )
    ]
    for o in range(1, depth):
        greet("sp", column(o))
    greet("sp", pair)
    greet("tp", across)
    greet("tp", partner)
    inputs = [
        pltpu.make_async_copy(source, target, load.at[7 + i])
        for i, (source, target) in enumerate(
            (
                (k_one_h, k_one),
                (k_two_h, k_two),
                (val_h, val),
                (q_one_h, q_one),
                (q_two_h, q_two),
                (stream_h, stream),
                (gain_h, gain),
                (route_h, route_t),
                (share_h, share_t),
            )
        )
    ]
    for one in inputs:
        one.start()
    for one in inputs[:3]:
        one.wait()
    pl.semaphore_wait(pltpu.get_barrier_semaphore(), depth + 2)

    sources = (k_one, k_two, val)
    held = (keys_one, keys_two, vals)

    def copies(block, way, target, own):
        return [
            mesh_copy(
                sources[a] if own else held[a].at[block],
                held[a].at[block],
                send_kv.at[way, a, block // 2],
                recv_kv.at[a, block],
                "sp",
                target,
            )
            for a in range(3)
        ]

    def start(block, way, target, own=False):
        for one in copies(block, way, target, own):
            one.start()

    def arrive(block):
        for one in copies(block, 0, pair, False):
            one.wait_recv()

    share = width // 2
    share_at = pl.ds(pl.multiple_of(core * share, share), share)
    other_at = pl.ds(pl.multiple_of((1 - core) * share, share), share)

    def pair_weights():
        return [
            mesh_copy(
                h.at[share_at], v.at[1, share_at], send_g.at[0, i], recv_g.at[0, i], "sp", pair
            )
            for i, (h, v) in enumerate(((gate_h, gates), (up_h, ups)))
        ]

    def pair_weights_on(at):
        return [
            mesh_copy(
                v.at[1, at], v.at[1, at], send_g.at[1, i], recv_g.at[1, i], "tp", partner
            )
            for i, v in enumerate((gates, ups))
        ]

    part = hid // 2

    def down_at(block, c):
        return wall.at[pl.ds(pl.multiple_of(block * hid + c * part, part), part)]

    def down_own(way, target):
        return mesh_copy(
            down_h.at[pl.ds(pl.multiple_of(core * part, part), part), cols_of(far)],
            down_at(me, core),
            send_d.at[way],
            recv_d.at[0, me],
            "sp",
            target,
        )

    def down_pair(block):
        return mesh_copy(
            down_at(block, core),
            down_at(block, core),
            send_d.at[depth + block // 2],
            recv_d.at[0, block],
            "sp",
            pair,
        )

    def down_core(block, c):
        return mesh_copy(
            down_at(block, c),
            down_at(block, c),
            send_d.at[3 * depth + block],
            recv_d.at[1, block],
            "tp",
            partner,
        )

    def extra_at(s, c):
        return extra.at[pl.ds(pl.multiple_of(s * hid + c * part, part), part)]

    def extra_own():
        return mesh_copy(
            down_h.at[pl.ds(pl.multiple_of(core * part, part), part), cols_of(1 - far)],
            extra_at(side, core),
            send_e.at[0],
            recv_e.at[0, side],
            "sp",
            side,
        )

    def extra_pair(s):
        return mesh_copy(
            extra_at(s, core), extra_at(s, core), send_e.at[1], recv_e.at[0, s], "sp", pair
        )

    def extra_core(s, c):
        return mesh_copy(
            extra_at(s, c), extra_at(s, c), send_e.at[2 + s], recv_e.at[1, s], "tp", partner
        )

    def sd_at(u):
        return wall.at[pl.ds(pl.multiple_of(n * hid + u * wide, wide), wide)]

    def sd_own(way, f, target):
        return mesh_copy(
            s_down_h.at[:, cols_of(f)], sd_at(mine), send_sd.at[way], recv_sd.at[mine], "tp", target
        )

    def sd_on(u):
        return mesh_copy(sd_at(u), sd_at(u), send_sd.at[2], recv_sd.at[u], "tp", partner)

    @pl.when(above)
    def _():
        start(me, 0, me + 2, True)

    @pl.when(side == 0)
    def _():
        start(me, 1, pair, True)

    for one in loads:
        one.start()
    late = place >= depth // 2

    @pl.when(late)
    def _():
        sd_own(1, 1 - far, across).start()

    sd_own(0, far, partner).start()
    for o in range(1, depth):

        @pl.when(place + o >= depth)
        def _():
            down_own(o, column(o)).start()

    top_place = place == depth - 1
    pl.when(top_place)(lambda: extra_own().start())

    for one in inputs[3:]:
        one.wait()
    for index, q in enumerate((q_one, q_two)):
        for h in range(group):
            stacked[index, h * seq : (h + 1) * seq, :] = q[:, h * HEAD : (h + 1) * HEAD]

    def scores_of(index, keys):
        return (
            lax.dot_general(
                stacked[index], keys, (((1,), (1,)), ((), ())), preferred_element_type=jnp.float32
            )
            * scale
        )

    spread = (group * seq, seq)
    row_of = lax.broadcasted_iota(jnp.int32, spread, 0) % seq
    allowed = lax.broadcasted_iota(jnp.int32, spread, 1) <= row_of
    for index, keys in enumerate((k_one, k_two)):
        scores = jnp.where(allowed, scores_of(index, keys[...]), FLOOR)
        top = jnp.max(scores, axis=-1, keepdims=True)
        weights = jnp.exp(scores - top)
        peak[index] = top
        total[index] = jnp.sum(weights, axis=-1, keepdims=True)
        accum[index] = jnp.dot(
            weights.astype(jnp.bfloat16), val[...], preferred_element_type=jnp.float32
        )

    def fold(block):
        for index in range(2):
            scores = scores_of(index, held[index][block])
            old = peak[index]
            top = jnp.maximum(old, jnp.max(scores, axis=-1, keepdims=True))
            weights = jnp.exp(scores - top)
            fade = jnp.exp(old - top)
            peak[index] = top
            total[index] = total[index] * fade + jnp.sum(weights, axis=-1, keepdims=True)
            accum[index] = accum[index] * fade + jnp.dot(
                weights.astype(jnp.bfloat16), vals[block], preferred_element_type=jnp.float32
            )

    def down_up(block):
        return mesh_copy(
            down_at(block, core),
            down_at(block, core),
            send_d.at[2 * depth + block // 2],
            recv_d.at[0, block],
            "sp",
            me + 2,
        )

    def lift(d):
        @pl.when((place >= d) & above)
        def _():
            down_up(me - 2 * d).wait_recv()
            down_up(me - 2 * d).start()

    def weights_out():
        pl.when(above)(lambda: down_own(1, me + 2).start())
        for one in pair_weights():
            one.start()
        down_own(0, pair).start()
        lift(1)

    pl.when(place == 0)(weights_out)

    def visit(e, carry):
        @pl.when(place >= e)
        def _():
            block = me - 2 * e
            for up, over in zip(copies(block, 0, me + 2, False), copies(block, 1, pair, False)):
                over.wait_recv()
                pl.when(above)(up.start)
                over.start()
            pl.when(e == place)(weights_out)
            fold(block)

        @pl.when((place >= e - 1) & ((e > 1) | (side == 1)))
        def _():
            block = pair - 2 * (e - 1)
            arrive(block)
            fold(block)

        return carry

    lax.fori_loop(1, depth + 1, visit, 0)

    for d in range(2, depth):
        lift(d)

    for h in range(group):
        cut = slice(h * seq, (h + 1) * seq)
        head = accum[0, cut, :] / total[0, cut, :] - lam[h] * (
            accum[1, cut, :] / total[1, cut, :]
        )
        head = head * lax.rsqrt(jnp.mean(head * head, axis=-1, keepdims=True) + 1e-05)
        size = head.shape[1]
        rows_in[:, h * size : (h + 1) * size] = head.astype(jnp.bfloat16)

    for o in range(2):
        base = 2 * ((far + o) % 2)
        for which, parity in enumerate((1 - core, core)):
            begin = pl.multiple_of((base + parity) * rows, rows)
            order[which, o * rows : (o + 1) * rows, :] = rows_in[pl.ds(begin, rows), :]

    first = [
        mesh_copy(out_one.at[i], in_one.at[i], send_one.at[0], recv_one.at[i], "tp", partner)
        for i in range(pieces)
    ]
    second = [
        mesh_copy(out_two.at[i], in_two.at[i], send_two.at[0], recv_two.at[i], "tp", across)
        for i in range(pieces)
    ]
    span = width // pieces
    loads[0].wait()
    for i in range(pieces):
        out_one[i] = jnp.dot(
            order[0], w[:, i * span : (i + 1) * span], preferred_element_type=jnp.float32
        ).astype(jnp.bfloat16)
        first[i].start()
    kept = []
    for i in range(pieces):
        sums = jnp.dot(
            order[1], w[:, i * span : (i + 1) * span], preferred_element_type=jnp.float32
        )
        first[i].wait_recv()
        sums = sums + in_one[i].astype(jnp.float32)
        out_two[i] = sums[rows:].astype(jnp.bfloat16)
        second[i].start()
        kept.append(sums[:rows])

    @pl.when(jnp.logical_not(late))
    def _():
        sd_own(1, 1 - far, across).start()

    def row_part(block, extra, spot, i):
        return block.at[spot, i] if i < pieces else extra.at[spot]

    def row_copy(spot, way, target, i):
        some = row_part(gathered, stat, spot, i)
        return mesh_copy(
            some,
            some,
            send_x.at[way, i // pieces, spot],
            recv_x.at[i, spot],
            "sp",
            target,
        )

    def rows_sent(spot, way):
        for some, kind in ((gathered.at[spot], 0), (stat.at[spot], 1)):
            mesh_copy(
                some, some, send_x.at[way, kind, spot], recv_x.at[0, spot], "sp", pair
            ).wait_send()

    def beside_own(way, target, i):
        return mesh_copy(
            row_part(gathered, stat, place, i),
            row_part(beside, stat_b, mine, i),
            send_b.at[way, i // pieces],
            recv_b.at[i // pieces, mine],
            "tp",
            target,
        )

    def beside_on(u, kind, way=2):
        some = (beside, stat_b)[kind].at[u]
        return mesh_copy(some, some, send_b.at[way, kind], recv_b.at[kind, u], "tp", partner)

    def raise_row(e, i):
        row_copy(place - e, 0, pair, i).wait_recv()
        row_copy(place - e, 0, me + 2, i).start()

    def lower_row(e, i):
        row_copy(place + e, 0, pair, i).wait_recv()
        row_copy(place + e, 1, me - 2, i).start()

    def rows_out(i):
        pl.when(above)(lambda: row_copy(place, 0, me + 2, i).start())
        pl.when(below)(lambda: row_copy(place, 1, me - 2, i).start())
        beside_own(1, across, i).start()
        beside_own(0, partner, i).start()

    fine = resid.shape[2]
    per = span // fine
    squares = jnp.zeros((rows, 1), jnp.float32)
    for i in range(pieces):
        cut = slice(i * span, (i + 1) * span)
        second[i].wait_recv()
        sums = kept[i] + in_two[i].astype(jnp.float32)
        sums = (stream[:, cut].astype(jnp.float32) + sums).astype(jnp.bfloat16)
        for j in range(per):
            resid[i * per + j] = sums[:, j * fine : (j + 1) * fine]
        sums = sums.astype(jnp.float32)
        squares = squares + jnp.sum(sums * sums, axis=-1, keepdims=True)
        gathered[place, i] = (sums * gain[:, cut]).astype(jnp.bfloat16)
        rows_out(i)
    shrink = lax.rsqrt(squares / width + 1e-06)
    square[0:rows, :] = jnp.broadcast_to(shrink, (rows, HEAD))
    stat[place] = square[...].T[0 : stat.shape[1], :]
    rows_out(pieces)
    for e in range(1, depth - 1):
        for i in range(pieces + 1):
            pl.when(above & (place >= e))(lambda: raise_row(e, i))
            if e == depth - 2:
                pl.when(above & below)(lambda: lower_row(1, i))


    def pass_down(e):
        def one(block, fresh):
            pl.when(fresh)(lambda: down_pair(block).wait_recv())
            down_pair(block).start()
            down_core(block, core).start()

        pl.when(place >= e)(lambda: one(me - 2 * e, jnp.logical_not(above)))
        pl.when(place + e < depth)(lambda: one(me + 2 * e, place >= 0))

    def collect(e):
        def one(block):
            down_pair(block).wait_recv()
            down_core(block, core).start()

        pl.when(place >= e)(lambda: one(pair - 2 * e))
        pl.when(place + e < depth)(lambda: one(pair + 2 * e))

    def factors(scales, spot):
        square[0 : scales.shape[1], :] = scales[spot]
        return square[...].T[0:rows, :1]

    def hidden_of(block, spot, factor, g, u):
        def project(m):
            parts = [
                jnp.dot(
                    block[spot, i],
                    m[i * span : (i + 1) * span, :],
                    preferred_element_type=jnp.float32,
                )
                for i in range(pieces)
            ]
            return sum(parts[1:], parts[0]) * factor

        gate_part, up_part = project(g), project(u)
        return (gate_part / (1.0 + jnp.exp(-gate_part)) * up_part).astype(jnp.bfloat16)

    square[...] = jnp.zeros_like(square)
    for j in range(n):
        chosen = jnp.where(route_t[...] == j, share_t[...], 0.0)
        square[j : j + 1, 0:rows] = jnp.sum(chosen, axis=0, keepdims=True)
    turned = square[...].T
    for j in range(n):
        mix[j] = jnp.broadcast_to(turned[0:rows, j : j + 1], mix.shape[1:])
    for i in range(1, 5):
        loads[i].wait()

    def hid_copy(spot):
        return mesh_copy(
            out_hid.at[spot], in_hid.at[place], send_h.at[spot], recv_h.at[place], "sp",
            2 * spot + side,
        )

    def serve(spot):
        factor = factors(stat, spot)
        out_hid[spot, side] = hidden_of(gathered, spot, factor, gates.at[0], ups.at[0])
        out_hid[spot, 1 - side] = hidden_of(gathered, spot, factor, gates.at[1], ups.at[1])
        hid_copy(spot).start()

    def sh_copy(u):
        return mesh_copy(
            out_sh.at[u], in_sh.at[mine], send_s.at[u], recv_s.at[mine], "tp", u
        )

    def answer(u):
        out_sh[u] = hidden_of(beside, u, factors(stat_b, u), s_gate, s_up)
        sh_copy(u).start()

    def turn(e, carry):
        low, high = place >= e, place + e < depth

        @pl.when(low & jnp.logical_not(above))
        def _():
            for i in range(pieces + 1):
                row_copy(place - e, 0, pair, i).wait_recv()

        @pl.when(high)
        def _():
            for i in range(pieces + 1):
                pl.when(below & (e > 1))(lambda: lower_row(e, i))
                pl.when(jnp.logical_not(below))(
                    lambda: row_copy(place + e, 0, pair, i).wait_recv()
                )

        @pl.when(e == 1)
        def _():
            for one, onward in zip(pair_weights(), pair_weights_on(share_at)):
                one.wait_recv()
                onward.start()
            pass_down(1)
            factor = factors(stat, place)
            in_sh[mine] = hidden_of(gathered, place, factor, s_gate, s_up)
            in_hid[place, side] = hidden_of(gathered, place, factor, gates.at[0], ups.at[0])
            for one in pair_weights_on(other_at):
                one.wait_recv()

        @pl.when(low)
        def _():
            serve(place - e)

        @pl.when(high)
        def _():
            serve(place + e)

        pass_down(e + 1)

        @pl.when(e == 2)
        def _():
            down_pair(pair).wait_recv()
            down_core(pair, core).start()
            in_hid[place, 1 - side] = hidden_of(
                gathered, place, factors(stat, place), gates.at[1], ups.at[1]
            )
            u = across
            for kind in range(2):
                beside_on(u, kind).wait_recv()
                beside_on(u, kind).start()
            answer(u)
            sd_on(u).wait_recv()
            sd_on(u).start()
            for o in range(2):
                u = 2 * ((far + o) % 2) + 1 - core
                for kind in range(2):
                    beside_on(u, kind).wait_recv()
                answer(u)

        return carry

    @pl.when(place == 0)
    def _():
        extra_pair(side).wait_recv()
        extra_pair(side).start()
        extra_core(side, core).start()

    lax.fori_loop(1, depth - 1, turn, 0)
    last = depth - 1

    @pl.when(place == 0)
    def _():
        for i in range(pieces + 1):
            row_copy(last, 0, pair, i).wait_recv()
        serve(last)

    segments = units.shape[1]

    def unit_copy(s):
        return mesh_copy(
            units.at[0, s], units.at[1, s], send_u.at[s], recv_u.at[s], "tp", across
        )

    for o in range(1, nt):
        u = (mine + o) % nt
        mesh_copy(
            out_sh.at[u], in_sh.at[u], send_s.at[u], recv_s.at[u], "tp", u
        ).wait_recv()
    seg = units.shape[3]
    for j in range(nt):
        at = j * wide
        units[0, depth + at // seg, :, at % seg : at % seg + wide] = in_sh[j]
    for s in range(depth, segments):
        unit_copy(s).start()

    for e in range(1, depth - 1):
        collect(e)

    def place_unit(spot):
        @pl.when(place != spot)
        def _():
            mesh_copy(
                out_hid.at[spot], in_hid.at[spot], send_h.at[spot], recv_h.at[spot], "sp",
                2 * spot + side,
            ).wait_recv()

        for k in range(2):
            j = 2 * spot + k
            units[0, spot, :, k * hid : (k + 1) * hid] = (
                in_hid[spot, k].astype(jnp.float32) * mix[j][:, :1]
            ).astype(jnp.bfloat16)

    for spot in range(last - 1, -1, -1):
        place_unit(spot)
        unit_copy(spot).start()

    @pl.when(place != 0)
    def _():
        place_unit(last)
        unit_copy(last).start()

    @pl.when(top_place)
    def _():
        for i in range(pieces + 1):
            row_copy(0, 0, pair, i).wait_recv()
        serve(0)

    @pl.when(place == 0)
    def _():
        extra_pair(1 - side).wait_recv()
        extra_core(1 - side, core).start()

    collect(last)

    loads[5].wait()
    loads[6].wait()
    for o in range(2):
        sd_on(2 * ((far + o) % 2) + 1 - core).wait_recv()

    def receive_down(block, carry):
        @pl.when(block != me)
        def _():
            down_core(block, 1 - core).wait_recv()

        return carry

    lax.fori_loop(0, n, receive_down, 0)
    early = [s for s in range(segments) if s != last]
    for s in early:
        unit_copy(s).wait_recv()
    pl.when(place != 0)(lambda: unit_copy(last).wait_recv())

    def fin_copy(i):
        return mesh_copy(out_fin.at[i], in_fin.at[i], send_f.at[0], recv_f.at[i], "tp", across)

    def put(spot):
        return pltpu.make_async_copy(
            result.at[spot],
            out.at[:, pl.ds(pl.multiple_of(spot * fine, fine), fine)],
            save.at[spot],
        )

    def close(spot, terms):
        result[spot] = (resid[spot].astype(jnp.float32) + terms).astype(jnp.bfloat16)
        put(spot).start()

    count = half // fine
    mine_at, other_of = far * count, (1 - far) * count
    for i in range(count):
        cut = slice(i * fine, (i + 1) * fine)
        terms = [
            jnp.dot(
                units[:, s].reshape(2 * rows, seg),
                wall[s * seg : (s + 1) * seg, cut],
                preferred_element_type=jnp.float32,
            )
            for s in early
        ]
        both = sum(terms[1:], terms[0])

        @pl.when(place == 0)
        def _():
            partial[i] = both[:rows]
            out_fin[i] = both[rows:].astype(jnp.bfloat16)
            fin_copy(i).start()

        @pl.when(place != 0)
        def _():
            full = both + jnp.dot(
                units[:, last].reshape(2 * rows, seg),
                wall[last * seg : (last + 1) * seg, cut],
                preferred_element_type=jnp.float32,
            )
            out_fin[i] = full[rows:].astype(jnp.bfloat16)
            fin_copy(i).start()
            close(mine_at + i, full[:rows])

    @pl.when(place == 0)
    def _():
        extra_core(0, 1 - core).wait_recv()
        extra_core(1, 1 - core).wait_recv()
        for i in range(count):
            fin_copy(i).wait_recv()
        place_unit(last)
        rest = units[0, last]
        for i in range(count):
            cut = slice(i * fine, (i + 1) * fine)
            terms = jnp.dot(
                rest, wall[last * seg : (last + 1) * seg, cut], preferred_element_type=jnp.float32
            )
            close(mine_at + i, partial[i] + terms)
            terms = jnp.dot(rest, extra[:, cut], preferred_element_type=jnp.float32)
            close(other_of + i, in_fin[i].astype(jnp.float32) + terms)

    @pl.when(place != 0)
    def _():
        for i in range(count):
            fin_copy(i).wait_recv()
            close(other_of + i, in_fin[i].astype(jnp.float32))

    def settle(e, carry):
        @pl.when(place >= e)
        def _():
            block = me - 2 * e

            @pl.when(above)
            def _():
                for one in copies(block, 0, me + 2, False):
                    one.wait_send()

                @pl.when(e > 0)
                def _():
                    down_up(block).wait_send()

            @pl.when((e > 0) | (side == 0))
            def _():
                for one in copies(block, 1, pair, False):
                    one.wait_send()

        pl.when((place + e < depth) & below)(lambda: rows_sent(place + e, 1))
        pl.when((place >= e) & above)(lambda: rows_sent(place - e, 0))

        @pl.when(e != place)
        def _():
            hid_copy(e).wait_send()
            down_pair(2 * e + side).wait_send()

        return carry

    lax.fori_loop(0, depth, settle, 0)

    def settle_down(block, carry):
        @pl.when(block != me)
        def _():
            down_core(block, core).wait_send()

        return carry

    lax.fori_loop(0, n, settle_down, 0)
    for one in pair_weights() + pair_weights_on(share_at):
        one.wait_send()
    for some, sem, rec in (
        (out_one, send_one.at[0], recv_one.at[0]),
        (out_two, send_two.at[0], recv_two.at[0]),
        (out_fin, send_f.at[0], recv_f.at[0]),
    ):
        mesh_copy(some, some, sem, rec, "tp", partner).wait_send()
    for o in range(1, depth):
        pl.when((place + o >= depth) | (o == 1))(lambda: down_own(o, column(o)).wait_send())
    down_own(0, pair).wait_send()
    sd_own(0, far, partner).wait_send()
    sd_own(1, 1 - far, across).wait_send()
    sd_on(across).wait_send()
    for kind in range(2):
        for way in range(3):
            beside_on(across, kind, way).wait_send()
    for o in range(1, nt):
        sh_copy((mine + o) % nt).wait_send()
    for s in early:
        unit_copy(s).wait_send()
    pl.when(place != 0)(lambda: unit_copy(last).wait_send())
    pl.when(top_place)(lambda: extra_own().wait_send())

    @pl.when(place == 0)
    def _():
        extra_pair(side).wait_send()
        extra_core(0, core).wait_send()
        extra_core(1, core).wait_send()

    for i in range(2 * count):
        put(i).wait()


def near(
    stream_in,
    q_first,
    q_second,
    k_first,
    k_second,
    values,
    head_lambda,
    w_out,
    norm_gain,
    routes,
    route_w,
    w_gate,
    w_up,
    w_down,
    s_gate,
    s_up,
    s_down,
):
    n, nt = lax.axis_size("sp"), lax.axis_size("tp")
    depth = n // 2
    seq, rows, width = q_first.shape[0], stream_in.shape[0], stream_in.shape[1]
    group, value_dim = q_first.shape[1] // HEAD, values.shape[1]
    hid, wide = w_down.shape[1], s_down.shape[0]
    tall, features = group * seq, group * value_dim
    pieces = 4
    span = width // pieces
    half, fine = width // 2, width // 8
    seg = 2 * hid
    segments = depth + nt * wide // seg
    topk = routes.shape[1]
    smem = pl.BlockSpec(memory_space=pltpu.SMEM)
    hbm = pl.BlockSpec(memory_space=pl.ANY)
    low, high = jnp.bfloat16, jnp.float32
    dma = pltpu.SemaphoreType.DMA
    return pl.pallas_call(
        functools.partial(near_kernel, n, nt, group, pieces),
        out_shape=jax.ShapeDtypeStruct((rows, width), low),
        in_specs=[hbm] * 5 + [smem] + [hbm] * 11,
        out_specs=hbm,
        scratch_shapes=[
            pltpu.VMEM((seq, group * HEAD), low),
            pltpu.VMEM((seq, group * HEAD), low),
            pltpu.VMEM((seq, HEAD), low),
            pltpu.VMEM((seq, HEAD), low),
            pltpu.VMEM((seq, value_dim), low),
            pltpu.VMEM((rows, width), low),
            pltpu.VMEM((1, width), high),
            pltpu.VMEM((topk, rows), jnp.int32),
            pltpu.VMEM((topk, rows), high),
            pltpu.VMEM((2, tall, HEAD), low),
            pltpu.VMEM((n, seq, HEAD), low),
            pltpu.VMEM((n, seq, HEAD), low),
            pltpu.VMEM((n, seq, value_dim), low),
            pltpu.VMEM((2, tall, 1), high),
            pltpu.VMEM((2, tall, 1), high),
            pltpu.VMEM((2, tall, value_dim), high),
            pltpu.VMEM((seq, features), low),
            pltpu.VMEM((features, width), low),
            pltpu.VMEM((2, 2 * rows, features), low),
            pltpu.VMEM((pieces, 2 * rows, span), low),
            pltpu.VMEM((pieces, 2 * rows, span), low),
            pltpu.VMEM((pieces, rows, span), low),
            pltpu.VMEM((pieces, rows, span), low),
            pltpu.VMEM((width // fine, rows, fine), low),
            pltpu.VMEM((2, width, hid), low),
            pltpu.VMEM((2, width, hid), low),
            pltpu.VMEM((width, wide), low),
            pltpu.VMEM((width, wide), low),
            pltpu.VMEM((n * hid + nt * wide, half), low),
            pltpu.VMEM((depth, pieces, rows, span), low),
            pltpu.VMEM((nt, pieces, rows, span), low),
            pltpu.VMEM((depth, 8, HEAD), high),
            pltpu.VMEM((nt, 8, HEAD), high),
            pltpu.VMEM((depth, 2, rows, hid), low),
            pltpu.VMEM((depth, 2, rows, hid), low),
            pltpu.VMEM((nt, rows, wide), low),
            pltpu.VMEM((nt, rows, wide), low),
            pltpu.VMEM((2, segments, rows, seg), low),
            pltpu.VMEM((half // fine, rows, fine), low),
            pltpu.VMEM((half // fine, rows, fine), low),
            pltpu.VMEM((width // fine, rows, fine), low),
            pltpu.VMEM((n, rows, HEAD), high),
            pltpu.VMEM((HEAD, HEAD), high),
            pltpu.VMEM((2 * hid, half), low),
            pltpu.VMEM((half // fine, rows, fine), high),
            dma((16,)),
            dma((2, 3, depth)),
            dma((3, n)),
            dma((1,)),
            dma((pieces,)),
            dma((1,)),
            dma((pieces,)),
            dma((2, 2)),
            dma((2, 2)),
            dma((3 * depth + n,)),
            dma((2, n)),
            dma((3,)),
            dma((nt,)),
            dma((2, 2, depth)),
            dma((pieces + 1, depth)),
            dma((3, 2)),
            dma((2, nt)),
            dma((depth,)),
            dma((depth,)),
            dma((nt,)),
            dma((nt,)),
            dma((segments,)),
            dma((segments,)),
            dma((1,)),
            dma((half // fine,)),
            dma((width // fine,)),
            dma((4,)),
            dma((2, 2)),
        ],
        compiler_params=pltpu.CompilerParams(
            collective_id=0, has_side_effects=True, vmem_limit_bytes=60 << 20
        ),
        name="layer",
    )(
        q_first, q_second, k_first, k_second, values, head_lambda, w_out, stream_in,
        norm_gain.reshape(1, width), routes.T, route_w.T, w_gate[0], w_up[0], s_gate, s_up, w_down[0], s_down,
    )


def layer(*arrays):
    n, nt = lax.axis_size("sp"), lax.axis_size("tp")
    k_first, values, w_gate, w_down, s_down = (arrays[i] for i in (3, 5, 11, 13, 16))
    fits = (
        4 <= n <= 16
        and n % 2 == 0
        and nt == 4
        and k_first.shape[1] == HEAD
        and arrays[0].shape[0] <= HEAD
        and w_gate.shape[0] == 1
        and w_down.shape[1] % (16 * nt) == 0
        and s_down.shape[0] % (16 * n) == 0
        and w_down.shape[1] % HEAD == 0
        and (2 * w_down.shape[1]) % s_down.shape[0] == 0
        and (nt * s_down.shape[0]) % (2 * w_down.shape[1]) == 0
        and w_down.shape[2] % (16 * HEAD) == 0
    )
    return near(*arrays) if fits else local(*arrays)


def solution(mesh):
    return jax.shard_map(
        layer,
        mesh=mesh,
        in_specs=(
            P(("sp", "tp"), None),
            P("sp", "tp"),
            P("sp", "tp"),
            P("sp", "tp"),
            P("sp", "tp"),
            P("sp", "tp"),
            P("tp"),
            P("tp", None),
            P(),
            P(("sp", "tp"), None),
            P(("sp", "tp"), None),
            P("sp", None, None),
            P("sp", None, None),
            P("sp", None, None),
            P(None, "tp"),
            P(None, "tp"),
            P("tp", None),
        ),
        out_specs=P(("sp", "tp"), None),
        check_vma=False,
    )
```

```python
import functools
import math

import jax
import jax.numpy as jnp
from jax import lax
from jax.experimental import pallas as pl
from jax.experimental.pallas import tpu as pltpu
from jax.sharding import PartitionSpec as P

HEAD = 128


FLOOR = -1e30


def absorb(state, first_q, second_q, first_k, second_k, value_rows, query_pos, key_pos):
    allowed = key_pos[None, :] <= query_pos[:, None]
    scale = first_q.shape[-1] ** (-0.5)
    result = []
    pairs = ((first_q, first_k), (second_q, second_k))
    for index in range(2):
        query_rows, key_rows = pairs[index]
        peak, total, accum = (state[3 * index], state[3 * index + 1], state[3 * index + 2])
        scores = (
            jnp.einsum("qagd,kad->agqk", query_rows, key_rows, preferred_element_type=jnp.float32)
            * scale
        )
        scores = jnp.where(allowed, scores, FLOOR)
        raised = jnp.maximum(peak, scores.max(-1))
        weights = jnp.where(allowed, jnp.exp(scores - raised[..., None]), 0.0)
        fade = jnp.exp(peak - raised)
        total = total * fade + weights.sum(-1)
        accum = accum * fade[..., None] + jnp.einsum(
            "agqk,kad->agqd",
            weights.astype(jnp.bfloat16),
            value_rows,
            preferred_element_type=jnp.float32,
        )
        result += [raised, total, accum]
    return tuple(result)


def empty_state(kv_local, group, count, value_dim):
    peaks = jnp.full((kv_local, group, count), FLOOR, jnp.float32)
    sums = jnp.zeros((kv_local, group, count), jnp.float32)
    accums = jnp.zeros((kv_local, group, count, value_dim), jnp.float32)
    return (peaks, sums, accums, peaks, sums, accums)


def fold_rows(state, first_q, second_q, query_pos, last_row, pieces, start):
    first_k, second_k, value_rows = pieces
    length = first_k.shape[0]
    kv_local = first_q.shape[1]
    value_dim = value_rows.shape[1] // kv_local
    span = math.gcd(length, 2048)

    def sweep(current):

        def visit(block, inner):
            begin = block * span
            key_one = lax.dynamic_slice_in_dim(first_k, begin, span, 0).reshape(
                span, kv_local, HEAD
            )
            key_two = lax.dynamic_slice_in_dim(second_k, begin, span, 0).reshape(
                span, kv_local, HEAD
            )
            value_part = lax.dynamic_slice_in_dim(value_rows, begin, span, 0).reshape(
                span, kv_local, value_dim
            )
            key_pos = begin + jnp.arange(span, dtype=jnp.int32)
            return absorb(
                inner, first_q, second_q, key_one, key_two, value_part, query_pos, key_pos
            )

        return lax.fori_loop(0, length // span, visit, current)

    def unchanged(current):
        return current

    return lax.cond(start <= last_row, sweep, unchanged, state)


def finish_heads(final, head_lambda):
    kv_local, group, count, value_dim = final[2].shape
    weight = head_lambda.reshape(kv_local, group, 1, 1)
    head_out = final[2] / final[1][..., None] - weight * final[5] / final[4][..., None]
    head_out = head_out * lax.rsqrt(jnp.mean(head_out * head_out, axis=-1, keepdims=True) + 1e-05)
    return (
        head_out.transpose(2, 0, 1, 3)
        .reshape(count, kv_local * group * value_dim)
        .astype(jnp.bfloat16)
    )


def shared_part(normed, s_gate, s_up, s_down):
    piece = lax.all_gather(normed, "tp", axis=0, tiled=True)
    gate_part = jnp.dot(piece, s_gate, preferred_element_type=jnp.float32)
    up_part = jnp.dot(piece, s_up, preferred_element_type=jnp.float32)
    hidden = (jax.nn.silu(gate_part) * up_part).astype(jnp.bfloat16)
    terms = jnp.dot(hidden, s_down, preferred_element_type=jnp.float32)
    return lax.psum_scatter(
        terms.astype(jnp.bfloat16), "tp", scatter_dimension=0, tiled=True
    ).astype(jnp.float32)


def routed_part(normed, routes, route_w, w_gate, w_up, w_down):
    rows, topk = routes.shape
    local_experts = w_gate.shape[0]
    experts = local_experts * lax.axis_size("sp")
    slots = max(2, 3 * rows * topk // (2 * experts))
    flat_ids = routes.reshape(-1)
    hits = (flat_ids[:, None] == jnp.arange(experts, dtype=jnp.int32)[None, :]).astype(jnp.int32)
    slot_of = jnp.sum(jnp.cumsum(hits, axis=0) * hits, axis=1) - 1
    target = flat_ids * slots + slot_of
    placing = jnp.any(
        jnp.arange(experts * slots, dtype=jnp.int32)[:, None, None]
        == target.reshape(rows, topk)[None, :, :],
        axis=-1,
    ).astype(jnp.bfloat16)
    outgoing = (
        jnp.dot(placing, normed, preferred_element_type=jnp.float32)
        .astype(jnp.bfloat16)
        .reshape(experts, slots, normed.shape[1])
    )
    arrived = lax.all_to_all(outgoing, "sp", split_axis=0, concat_axis=0, tiled=True)
    sources = arrived.shape[0] // local_experts
    grouped = arrived.reshape(sources, local_experts, arrived.shape[1], arrived.shape[2])
    gate_part = jnp.einsum("sjcd,jdf->sjcf", grouped, w_gate, preferred_element_type=jnp.float32)
    up_part = jnp.einsum("sjcd,jdf->sjcf", grouped, w_up, preferred_element_type=jnp.float32)
    hidden = (jax.nn.silu(gate_part) * up_part).astype(jnp.bfloat16)
    result = jnp.einsum(
        "sjcf,jfd->sjcd", hidden, w_down, preferred_element_type=jnp.float32
    ).astype(jnp.bfloat16)
    returned = lax.all_to_all(
        result.reshape(arrived.shape), "sp", split_axis=0, concat_axis=0, tiled=True
    )
    picked = (
        returned.reshape(experts * slots, normed.shape[1])[target]
        .reshape(rows, topk, normed.shape[1])
        .astype(jnp.float32)
    )
    return jnp.sum(picked * route_w[..., None], axis=1)


def local(
    stream_in,
    q_first,
    q_second,
    k_first,
    k_second,
    values,
    head_lambda,
    w_out,
    norm_gain,
    routes,
    route_w,
    w_gate,
    w_up,
    w_down,
    s_gate,
    s_up,
    s_down,
):
    seq_rows = q_first.shape[0]
    kv_local = k_first.shape[1] // HEAD
    heads_local = q_first.shape[1] // HEAD
    group = heads_local // kv_local
    value_dim = values.shape[1] // kv_local
    offset = lax.axis_index("sp") * seq_rows
    query_pos = offset + jnp.arange(seq_rows, dtype=jnp.int32)
    last_row = offset + seq_rows - 1
    first_q = q_first.reshape(seq_rows, kv_local, group, HEAD)
    second_q = q_second.reshape(seq_rows, kv_local, group, HEAD)
    start_state = empty_state(kv_local, group, seq_rows, value_dim)
    folded_state = fold_rows(
        start_state,
        first_q,
        second_q,
        query_pos,
        last_row,
        (
            lax.all_gather(k_first, "sp", axis=0, tiled=True),
            lax.all_gather(k_second, "sp", axis=0, tiled=True),
            lax.all_gather(values, "sp", axis=0, tiled=True),
        ),
        jnp.int32(0),
    )
    attn_rows = finish_heads(folded_state, head_lambda)
    attn = lax.psum_scatter(
        jnp.dot(attn_rows, w_out, preferred_element_type=jnp.float32).astype(jnp.bfloat16),
        "tp",
        scatter_dimension=0,
        tiled=True,
    ).astype(jnp.float32)
    resid = (stream_in.astype(jnp.float32) + attn).astype(jnp.bfloat16)
    stream = lax.optimization_barrier(resid).astype(jnp.float32)
    normed = (
        stream * lax.rsqrt(jnp.mean(stream * stream, axis=-1, keepdims=True) + 1e-06) * norm_gain
    ).astype(jnp.bfloat16)
    routed = routed_part(normed, routes, route_w, w_gate, w_up, w_down)
    shared = shared_part(normed, s_gate, s_up, s_down)
    return (stream + routed + shared).astype(jnp.bfloat16)


def mesh_copy(src, dst, send_sem, recv_sem, axis, target):
    return pltpu.make_async_remote_copy(
        src_ref=src,
        dst_ref=dst,
        send_sem=send_sem,
        recv_sem=recv_sem,
        device_id={axis: target},
        device_id_type=pl.DeviceIdType.MESH,
    )


def greet(axis, target):
    pl.semaphore_signal(
        pltpu.get_barrier_semaphore(),
        inc=1,
        device_id={axis: target},
        device_id_type=pl.DeviceIdType.MESH,
    )


def near_kernel(
    n, nt, group, pieces,
    q_one_h, q_two_h, k_one_h, k_two_h, val_h, lam, w_out_h, stream_h, gain_h, route_h, share_h,
    gate_h, up_h, s_gate_h, s_up_h, down_h, s_down_h,
    out,
    q_one, q_two, k_own, val, stream, gain, route_t, share_t,
    stacked, keys, vals, peak, total, accum, rows_in,
    w, order, out_one, in_one, out_two, in_two, resid,
    gates, ups, s_gate, s_up, wall, gathered, beside, stat, stat_b,
    out_hid, in_hid, out_sh, in_sh, units, out_fin, in_fin, result, mix, square, extra, partial,
    load, send_kv, recv_kv, send_one, recv_one, send_two, recv_two,
    send_g, recv_g, send_d, recv_d, send_sd, recv_sd,
    send_x, recv_x, send_b, recv_b, send_h, recv_h, send_s, recv_s,
    send_u, recv_u, send_f, recv_f, save, send_e, recv_e,
):
    me, mine = lax.axis_index("sp"), lax.axis_index("tp")
    place, side = me // 2, me % 2
    far, core = mine // 2, mine % 2
    depth = n // 2
    pair, partner, across = me + 1 - 2 * side, mine + 1 - 2 * core, 2 * (1 - far) + core
    above, below = place < depth - 1, place > 0
    seq = q_one.shape[0]
    rows, width = stream.shape
    hid, wide = down_h.shape[0], s_down_h.shape[0]
    scale = HEAD ** (-0.5)
    half = width // 2

    def column(o):
        return 2 * ((place + o) % depth) + side

    def cols_of(f):
        return pl.ds(pl.multiple_of(f * half, half), half)

    loads = [
        pltpu.make_async_copy(source, target, load.at[i])
        for i, (source, target) in enumerate(
            (
                (w_out_h, w),
                (gate_h, gates.at[0]),
                (up_h, ups.at[0]),
                (s_gate_h, s_gate),
                (s_up_h, s_up),
                (
                    down_h.at[:, cols_of(far)],
                    wall.at[pl.ds(pl.multiple_of(me * hid, hid), hid)],
                ),
                (
                    s_down_h.at[:, cols_of(far)],
                    wall.at[pl.ds(pl.multiple_of(n * hid + mine * wide, wide), wide)],
                ),
            )
        )
    ]
    for o in range(1, depth):
        greet("sp", column(o))
    greet("sp", pair)
    greet("tp", across)
    greet("tp", partner)
    inputs = [
        pltpu.make_async_copy(source, target, load.at[7 + i])
        for i, (source, target) in enumerate(
            (
                (k_one_h, k_own.at[0]),
                (k_two_h, k_own.at[1]),
                (val_h, val),
                (q_one_h, q_one),
                (q_two_h, q_two),
                (stream_h, stream),
                (gain_h, gain),
                (route_h, route_t),
                (share_h, share_t),
            )
        )
    ]
    for one in inputs:
        one.start()
    for one in inputs[:3]:
        one.wait()
    pl.semaphore_wait(pltpu.get_barrier_semaphore(), depth + 2)

    mid = seq // 2

    def stuff(block):
        return keys.at[block], vals.at[block, :mid], vals.at[block, mid:]

    def copies(block, way, target, own):
        return [
            mesh_copy(
                (k_own, val.at[:mid], val.at[mid:])[a] if own else stuff(block)[a],
                stuff(block)[a],
                send_kv.at[way, a, block // 2],
                recv_kv.at[a, block],
                "sp",
                target,
            )
            for a in range(3)
        ]

    def start(block, way, target, own=False):
        for one in copies(block, way, target, own):
            one.start()

    def arrive(block):
        for one in copies(block, 0, pair, False):
            one.wait_recv()

    share = width // 2
    share_at = pl.ds(pl.multiple_of(core * share, share), share)
    other_at = pl.ds(pl.multiple_of((1 - core) * share, share), share)

    def pair_weights():
        return [
            mesh_copy(
                h.at[share_at], v.at[1, share_at], send_g.at[0, i], recv_g.at[0, i], "sp", pair
            )
            for i, (h, v) in enumerate(((gate_h, gates), (up_h, ups)))
        ]

    def pair_weights_on(at):
        return [
            mesh_copy(
                v.at[1, at], v.at[1, at], send_g.at[1, i], recv_g.at[1, i], "tp", partner
            )
            for i, v in enumerate((gates, ups))
        ]

    part = hid // 2

    def down_at(block, c):
        return wall.at[pl.ds(pl.multiple_of(block * hid + c * part, part), part)]

    def down_own(way, target):
        return mesh_copy(
            down_h.at[pl.ds(pl.multiple_of(core * part, part), part), cols_of(far)],
            down_at(me, core),
            send_d.at[way],
            recv_d.at[me],
            "sp",
            target,
        )

    def down_pair(block):
        return mesh_copy(
            down_at(block, core),
            down_at(block, core),
            send_d.at[depth + block // 2],
            recv_d.at[block],
            "sp",
            pair,
        )

    def down_core(block, c):
        return mesh_copy(
            down_at(block, c),
            down_at(block, c),
            send_d.at[3 * depth],
            recv_d.at[n],
            "tp",
            partner,
        )

    def extra_at(s, c):
        return extra.at[pl.ds(pl.multiple_of(s * hid + c * part, part), part)]

    def extra_own():
        return mesh_copy(
            down_h.at[pl.ds(pl.multiple_of(core * part, part), part), cols_of(1 - far)],
            extra_at(side, core),
            send_e.at[0],
            recv_e.at[0, side],
            "sp",
            side,
        )

    def extra_pair(s):
        return mesh_copy(
            extra_at(s, core), extra_at(s, core), send_e.at[1], recv_e.at[0, s], "sp", pair
        )

    def extra_core(s, c):
        return mesh_copy(
            extra_at(s, c), extra_at(s, c), send_e.at[2 + s], recv_e.at[1, s], "tp", partner
        )

    def sd_at(u):
        return wall.at[pl.ds(pl.multiple_of(n * hid + u * wide, wide), wide)]

    def sd_own(way, f, target):
        return mesh_copy(
            s_down_h.at[:, cols_of(f)], sd_at(mine), send_sd.at[way], recv_sd.at[mine], "tp", target
        )

    def sd_on(u):
        return mesh_copy(sd_at(u), sd_at(u), send_sd.at[2], recv_sd.at[u], "tp", partner)

    @pl.when(above)
    def _():
        start(me, 0, me + 2, True)

    @pl.when(side == 0)
    def _():
        start(me, 1, pair, True)

    for one in loads:
        one.start()
    late = place >= depth // 2

    @pl.when(late)
    def _():
        sd_own(1, 1 - far, across).start()

    sd_own(0, far, partner).start()
    for o in range(1, depth):

        @pl.when(place + o >= depth)
        def _():
            down_own(o, column(o)).start()

    top_place = place == depth - 1
    pl.when(top_place)(lambda: extra_own().start())

    for one in inputs[3:]:
        one.wait()
    for index, q in enumerate((q_one, q_two)):
        for h in range(group):
            stacked[index, h * seq : (h + 1) * seq, :] = q[:, h * HEAD : (h + 1) * HEAD]

    def scores_of(index, some):
        return (
            lax.dot_general(
                stacked[index], some, (((1,), (1,)), ((), ())), preferred_element_type=jnp.float32
            )
            * scale
        )

    spread = (group * seq, seq)
    row_of = lax.broadcasted_iota(jnp.int32, spread, 0) % seq
    allowed = lax.broadcasted_iota(jnp.int32, spread, 1) <= row_of
    for index in range(2):
        scores = jnp.where(allowed, scores_of(index, k_own[index]), FLOOR)
        top = jnp.max(scores, axis=-1, keepdims=True)
        weights = jnp.exp(scores - top)
        peak[index] = top
        total[index] = jnp.sum(weights, axis=-1, keepdims=True)
        accum[index] = jnp.dot(
            weights.astype(jnp.bfloat16), val[...], preferred_element_type=jnp.float32
        )

    def fold(block):
        for index in range(2):
            scores = scores_of(index, keys[block, index])
            old = peak[index]
            top = jnp.maximum(old, jnp.max(scores, axis=-1, keepdims=True))
            weights = jnp.exp(scores - top)
            fade = jnp.exp(old - top)
            peak[index] = top
            total[index] = total[index] * fade + jnp.sum(weights, axis=-1, keepdims=True)
            accum[index] = accum[index] * fade + jnp.dot(
                weights.astype(jnp.bfloat16), vals[block], preferred_element_type=jnp.float32
            )

    def down_up(block):
        return mesh_copy(
            down_at(block, core),
            down_at(block, core),
            send_d.at[2 * depth + block // 2],
            recv_d.at[block],
            "sp",
            me + 2,
        )

    def lift(d):
        @pl.when((place >= d) & above)
        def _():
            down_up(me - 2 * d).wait_recv()
            down_up(me - 2 * d).start()

    def weights_out():
        pl.when(above)(lambda: down_own(1, me + 2).start())
        for one in pair_weights():
            one.start()
        down_own(0, pair).start()
        lift(1)

    pl.when(place == 0)(weights_out)

    def visit(e, carry):
        @pl.when(place >= e)
        def _():
            block = me - 2 * e
            for up, over in zip(copies(block, 0, me + 2, False), copies(block, 1, pair, False)):
                over.wait_recv()
                pl.when(above)(up.start)
                over.start()
            pl.when(e == place)(weights_out)
            fold(block)

        @pl.when((place >= e - 1) & ((e > 1) | (side == 1)))
        def _():
            block = pair - 2 * (e - 1)
            arrive(block)
            fold(block)

        return carry

    lax.fori_loop(1, depth + 1, visit, 0)

    for d in range(2, depth):
        lift(d)

    for h in range(group):
        cut = slice(h * seq, (h + 1) * seq)
        head = accum[0, cut, :] / total[0, cut, :] - lam[h] * (
            accum[1, cut, :] / total[1, cut, :]
        )
        head = head * lax.rsqrt(jnp.mean(head * head, axis=-1, keepdims=True) + 1e-05)
        size = head.shape[1]
        rows_in[:, h * size : (h + 1) * size] = head.astype(jnp.bfloat16)

    for o in range(2):
        base = 2 * ((far + o) % 2)
        for which, parity in enumerate((1 - core, core)):
            begin = pl.multiple_of((base + parity) * rows, rows)
            order[which, o * rows : (o + 1) * rows, :] = rows_in[pl.ds(begin, rows), :]

    first = [
        mesh_copy(out_one.at[i], in_one.at[i], send_one.at[0], recv_one.at[i], "tp", partner)
        for i in range(pieces)
    ]
    second = [
        mesh_copy(out_two.at[i], in_two.at[i], send_two.at[0], recv_two.at[i], "tp", across)
        for i in range(pieces)
    ]
    span = width // pieces
    loads[0].wait()
    for i in range(pieces):
        out_one[i] = jnp.dot(
            order[0], w[:, i * span : (i + 1) * span], preferred_element_type=jnp.float32
        ).astype(jnp.bfloat16)
        first[i].start()
    kept = []
    for i in range(pieces):
        sums = jnp.dot(
            order[1], w[:, i * span : (i + 1) * span], preferred_element_type=jnp.float32
        )
        first[i].wait_recv()
        sums = sums + in_one[i].astype(jnp.float32)
        out_two[i] = sums[rows:].astype(jnp.bfloat16)
        second[i].start()
        kept.append(sums[:rows])

    @pl.when(jnp.logical_not(late))
    def _():
        sd_own(1, 1 - far, across).start()

    def row_part(block, extra, spot, i):
        return block.at[spot, i] if i < pieces else extra.at[spot]

    def row_copy(spot, way, target, i):
        some = row_part(gathered, stat, spot, i)
        return mesh_copy(
            some,
            some,
            send_x.at[way, i // pieces, spot],
            recv_x.at[i, spot],
            "sp",
            target,
        )

    def rows_sent(spot, way):
        for some, kind in ((gathered.at[spot], 0), (stat.at[spot], 1)):
            mesh_copy(
                some, some, send_x.at[way, kind, spot], recv_x.at[0, spot], "sp", pair
            ).wait_send()

    def beside_own(way, target, i):
        return mesh_copy(
            row_part(gathered, stat, place, i),
            row_part(beside, stat_b, mine, i),
            send_b.at[way, i // pieces],
            recv_b.at[i // pieces, mine],
            "tp",
            target,
        )

    def beside_on(u, kind, way=2):
        some = (beside, stat_b)[kind].at[u]
        return mesh_copy(some, some, send_b.at[way, kind], recv_b.at[kind, u], "tp", partner)

    def raise_row(e, i):
        row_copy(place - e, 0, pair, i).wait_recv()
        row_copy(place - e, 0, me + 2, i).start()

    def lower_row(e, i):
        row_copy(place + e, 0, pair, i).wait_recv()
        row_copy(place + e, 1, me - 2, i).start()

    def rows_out(i):
        pl.when(above)(lambda: row_copy(place, 0, me + 2, i).start())
        pl.when(below)(lambda: row_copy(place, 1, me - 2, i).start())
        beside_own(1, across, i).start()
        beside_own(0, partner, i).start()

    fine = resid.shape[2]
    per = span // fine
    squares = jnp.zeros((rows, 1), jnp.float32)
    for i in range(pieces):
        cut = slice(i * span, (i + 1) * span)
        second[i].wait_recv()
        sums = kept[i] + in_two[i].astype(jnp.float32)
        sums = (stream[:, cut].astype(jnp.float32) + sums).astype(jnp.bfloat16)
        for j in range(per):
            resid[i * per + j] = sums[:, j * fine : (j + 1) * fine]
        sums = sums.astype(jnp.float32)
        squares = squares + jnp.sum(sums * sums, axis=-1, keepdims=True)
        gathered[place, i] = (sums * gain[:, cut]).astype(jnp.bfloat16)
        rows_out(i)
    shrink = lax.rsqrt(squares / width + 1e-06)
    square[0:rows, :] = jnp.broadcast_to(shrink, (rows, HEAD))
    stat[place] = square[...].T[0 : stat.shape[1], :]
    rows_out(pieces)
    ahead = pieces // 2
    for e in range(1, depth - 1):
        for i in range(pieces + 1 if e == 1 else ahead):
            pl.when(above & (place >= e))(lambda: raise_row(e, i))
        if e == 1:
            for i in range(pieces + 1):
                pl.when(above & below)(lambda: lower_row(1, i))
    def pass_down(e):
        def one(block, fresh):
            pl.when(fresh)(lambda: down_pair(block).wait_recv())
            down_pair(block).start()
            down_core(block, core).start()

        pl.when(place >= e)(lambda: one(me - 2 * e, jnp.logical_not(above)))
        pl.when(place + e < depth)(lambda: one(me + 2 * e, place >= 0))

    def collect(e):
        def one(block):
            down_pair(block).wait_recv()
            down_core(block, core).start()

        pl.when(place >= e)(lambda: one(pair - 2 * e))
        pl.when(place + e < depth)(lambda: one(pair + 2 * e))

    def factors(scales, spot):
        square[0 : scales.shape[1], :] = scales[spot]
        return square[...].T[0:rows, :1]

    def hidden_of(block, spot, factor, g, u):
        def project(m):
            parts = [
                jnp.dot(
                    block[spot, i],
                    m[i * span : (i + 1) * span, :],
                    preferred_element_type=jnp.float32,
                )
                for i in range(pieces)
            ]
            return sum(parts[1:], parts[0]) * factor

        gate_part, up_part = project(g), project(u)
        return (gate_part / (1.0 + jnp.exp(-gate_part)) * up_part).astype(jnp.bfloat16)

    for one, onward in zip(pair_weights(), pair_weights_on(share_at)):
        one.wait_recv()
        onward.start()
    for d in range(1, depth):
        pass_down(d)
    for e in range(2, depth - 1):
        for i in range(pieces + 1):
            pl.when(below & (place + e < depth))(lambda: lower_row(e, i))

    square[...] = jnp.zeros_like(square)
    for j in range(n):
        chosen = jnp.where(route_t[...] == j, share_t[...], 0.0)
        square[j : j + 1, 0:rows] = jnp.sum(chosen, axis=0, keepdims=True)
    turned = square[...].T
    for j in range(n):
        mix[j] = jnp.broadcast_to(turned[0:rows, j : j + 1], mix.shape[1:])
    for i in range(1, 5):
        loads[i].wait()

    def hid_copy(spot):
        return mesh_copy(
            out_hid.at[spot], in_hid.at[place], send_h.at[spot], recv_h.at[place], "sp",
            2 * spot + side,
        )

    def serve(spot):
        factor = factors(stat, spot)
        out_hid[spot, side] = hidden_of(gathered, spot, factor, gates.at[0], ups.at[0])
        out_hid[spot, 1 - side] = hidden_of(gathered, spot, factor, gates.at[1], ups.at[1])
        hid_copy(spot).start()

    def serve_last(spot):
        sums = None
        mats = (gates.at[0], ups.at[0], gates.at[1], ups.at[1])
        for i in range(pieces):
            row_copy(spot, 0, pair, i).wait_recv()
            parts = [
                jnp.dot(
                    gathered[spot, i],
                    m[i * span : (i + 1) * span, :],
                    preferred_element_type=jnp.float32,
                )
                for m in mats
            ]
            sums = parts if sums is None else [a + b for a, b in zip(sums, parts)]
        row_copy(spot, 0, pair, pieces).wait_recv()
        factor = factors(stat, spot)
        g_one, u_one, g_two, u_two = [v * factor for v in sums]
        for which, g, u in ((side, g_one, u_one), (1 - side, g_two, u_two)):
            out_hid[spot, which] = (g / (1.0 + jnp.exp(-g)) * u).astype(jnp.bfloat16)
        hid_copy(spot).start()

    def sh_copy(u):
        return mesh_copy(
            out_sh.at[u], in_sh.at[mine], send_s.at[u], recv_s.at[mine], "tp", u
        )

    def answer(u):
        out_sh[u] = hidden_of(beside, u, factors(stat_b, u), s_gate, s_up)
        sh_copy(u).start()

    def turn(e, carry):
        low, high = place >= e, place + e < depth

        @pl.when(low & jnp.logical_not(above))
        def _():
            for i in range(pieces + 1):
                row_copy(place - e, 0, pair, i).wait_recv()

        @pl.when(high & jnp.logical_not(below))
        def _():
            for i in range(pieces + 1):
                row_copy(place + e, 0, pair, i).wait_recv()

        @pl.when(e == 1)
        def _():
            factor = factors(stat, place)
            in_sh[mine] = hidden_of(gathered, place, factor, s_gate, s_up)
            in_hid[place, side] = hidden_of(gathered, place, factor, gates.at[0], ups.at[0])
            for one in pair_weights_on(other_at):
                one.wait_recv()

        @pl.when(low)
        def _():
            serve(place - e)

        @pl.when(high)
        def _():
            serve(place + e)

        @pl.when(e == 1)
        def _():
            for d in range(2, depth - 1):
                for i in range(ahead, pieces + 1):
                    pl.when(above & (place >= d))(lambda: raise_row(d, i))

        @pl.when(e == 2)
        def _():
            down_pair(pair).wait_recv()
            down_core(pair, core).start()
            in_hid[place, 1 - side] = hidden_of(
                gathered, place, factors(stat, place), gates.at[1], ups.at[1]
            )
            u = across
            for kind in range(2):
                beside_on(u, kind).wait_recv()
                beside_on(u, kind).start()
            answer(u)
            sd_on(u).wait_recv()
            sd_on(u).start()
            for o in range(2):
                u = 2 * ((far + o) % 2) + 1 - core
                for kind in range(2):
                    beside_on(u, kind).wait_recv()
                answer(u)

        return carry

    @pl.when(place == 0)
    def _():
        extra_pair(side).wait_recv()
        extra_pair(side).start()
        extra_core(side, core).start()

    lax.fori_loop(1, depth - 1, turn, 0)
    last = depth - 1

    @pl.when(place == 0)
    def _():
        serve_last(last)

    segments = units.shape[1]

    def unit_copy(s):
        return mesh_copy(
            units.at[0, s], units.at[1, s], send_u.at[s], recv_u.at[s], "tp", across
        )

    for o in range(1, nt):
        u = (mine + o) % nt
        mesh_copy(
            out_sh.at[u], in_sh.at[u], send_s.at[u], recv_s.at[u], "tp", u
        ).wait_recv()
    seg = units.shape[3]
    for j in range(nt):
        at = j * wide
        units[0, depth + at // seg, :, at % seg : at % seg + wide] = in_sh[j]
    for s in range(depth, segments):
        unit_copy(s).start()

    for e in range(1, depth - 1):
        collect(e)

    def place_unit(spot):
        @pl.when(place != spot)
        def _():
            mesh_copy(
                out_hid.at[spot], in_hid.at[spot], send_h.at[spot], recv_h.at[spot], "sp",
                2 * spot + side,
            ).wait_recv()

        for k in range(2):
            j = 2 * spot + k
            units[0, spot, :, k * hid : (k + 1) * hid] = (
                in_hid[spot, k].astype(jnp.float32) * mix[j][:, :1]
            ).astype(jnp.bfloat16)

    for spot in range(last - 1, -1, -1):
        place_unit(spot)
        unit_copy(spot).start()

    @pl.when(place != 0)
    def _():
        place_unit(last)
        unit_copy(last).start()

    @pl.when(top_place)
    def _():
        serve_last(0)

    @pl.when(place == 0)
    def _():
        extra_pair(1 - side).wait_recv()
        extra_core(1 - side, core).start()

    collect(last)

    loads[5].wait()
    loads[6].wait()
    for o in range(2):
        sd_on(2 * ((far + o) % 2) + 1 - core).wait_recv()

    taken = wall.at[pl.ds(0, (n - 1) * part)]
    cores = mesh_copy(taken, taken, send_d.at[3 * depth], recv_d.at[n], "tp", partner)
    cores.wait_recv()
    early = [s for s in range(segments) if s != last]
    for s in early:
        unit_copy(s).wait_recv()
    pl.when(place != 0)(lambda: unit_copy(last).wait_recv())

    def fin_copy(i):
        return mesh_copy(out_fin.at[i], in_fin.at[i], send_f.at[0], recv_f.at[i], "tp", across)

    def put(spot):
        return pltpu.make_async_copy(
            result.at[spot],
            out.at[:, pl.ds(pl.multiple_of(spot * fine, fine), fine)],
            save.at[0],
        )

    def close(spot, terms):
        result[spot] = (resid[spot].astype(jnp.float32) + terms).astype(jnp.bfloat16)
        put(spot).start()

    count = half // fine
    mine_at, other_of = far * count, (1 - far) * count
    for i in range(count):
        cut = slice(i * fine, (i + 1) * fine)
        terms = [
            jnp.dot(
                units[:, s].reshape(2 * rows, seg),
                wall[s * seg : (s + 1) * seg, cut],
                preferred_element_type=jnp.float32,
            )
            for s in early
        ]
        both = sum(terms[1:], terms[0])

        @pl.when(place == 0)
        def _():
            partial[i] = both[:rows]
            out_fin[i] = both[rows:].astype(jnp.bfloat16)
            fin_copy(i).start()

        @pl.when(place != 0)
        def _():
            full = both + jnp.dot(
                units[:, last].reshape(2 * rows, seg),
                wall[last * seg : (last + 1) * seg, cut],
                preferred_element_type=jnp.float32,
            )
            out_fin[i] = full[rows:].astype(jnp.bfloat16)
            fin_copy(i).start()
            close(mine_at + i, full[:rows])

    @pl.when(place == 0)
    def _():
        extra_core(0, 1 - core).wait_recv()
        extra_core(1, 1 - core).wait_recv()
        for i in range(count):
            fin_copy(i).wait_recv()
        place_unit(last)
        rest = units[0, last]
        for i in range(count):
            cut = slice(i * fine, (i + 1) * fine)
            terms = jnp.dot(
                rest, wall[last * seg : (last + 1) * seg, cut], preferred_element_type=jnp.float32
            )
            close(mine_at + i, partial[i] + terms)
            terms = jnp.dot(rest, extra[:, cut], preferred_element_type=jnp.float32)
            close(other_of + i, in_fin[i].astype(jnp.float32) + terms)

    @pl.when(place != 0)
    def _():
        for i in range(count):
            fin_copy(i).wait_recv()
            close(other_of + i, in_fin[i].astype(jnp.float32))

    def settle(e, carry):
        @pl.when(place >= e)
        def _():
            block = me - 2 * e

            @pl.when(above)
            def _():
                for one in copies(block, 0, me + 2, False):
                    one.wait_send()

                @pl.when(e > 0)
                def _():
                    down_up(block).wait_send()

            @pl.when((e > 0) | (side == 0))
            def _():
                for one in copies(block, 1, pair, False):
                    one.wait_send()

        pl.when((place + e < depth) & below)(lambda: rows_sent(place + e, 1))
        pl.when((place >= e) & above)(lambda: rows_sent(place - e, 0))

        @pl.when(e != place)
        def _():
            hid_copy(e).wait_send()
            down_pair(2 * e + side).wait_send()

        return carry

    lax.fori_loop(0, depth, settle, 0)

    cores.wait_send()
    for one in pair_weights() + pair_weights_on(share_at):
        one.wait_send()
    for some, sem, rec in (
        (out_one, send_one.at[0], recv_one.at[0]),
        (out_two, send_two.at[0], recv_two.at[0]),
        (out_fin, send_f.at[0], recv_f.at[0]),
    ):
        mesh_copy(some, some, sem, rec, "tp", partner).wait_send()
    for o in range(1, depth):
        pl.when((place + o >= depth) | (o == 1))(lambda: down_own(o, column(o)).wait_send())
    down_own(0, pair).wait_send()
    sd_own(0, far, partner).wait_send()
    sd_own(1, 1 - far, across).wait_send()
    sd_on(across).wait_send()
    for kind in range(2):
        for way in range(3):
            beside_on(across, kind, way).wait_send()
    for o in range(1, nt):
        sh_copy((mine + o) % nt).wait_send()
    for s in early:
        unit_copy(s).wait_send()
    pl.when(place != 0)(lambda: unit_copy(last).wait_send())
    pl.when(top_place)(lambda: extra_own().wait_send())

    @pl.when(place == 0)
    def _():
        extra_pair(side).wait_send()
        extra_core(0, core).wait_send()
        extra_core(1, core).wait_send()

    pltpu.make_async_copy(stream_h, stream, save.at[0]).wait()


def near(
    stream_in,
    q_first,
    q_second,
    k_first,
    k_second,
    values,
    head_lambda,
    w_out,
    norm_gain,
    routes,
    route_w,
    w_gate,
    w_up,
    w_down,
    s_gate,
    s_up,
    s_down,
):
    n, nt = lax.axis_size("sp"), lax.axis_size("tp")
    depth = n // 2
    seq, rows, width = q_first.shape[0], stream_in.shape[0], stream_in.shape[1]
    group, value_dim = q_first.shape[1] // HEAD, values.shape[1]
    hid, wide = w_down.shape[1], s_down.shape[0]
    tall, features = group * seq, group * value_dim
    pieces = 4
    span = width // pieces
    half, fine = width // 2, width // 8
    seg = 2 * hid
    segments = depth + nt * wide // seg
    topk = routes.shape[1]
    smem = pl.BlockSpec(memory_space=pltpu.SMEM)
    hbm = pl.BlockSpec(memory_space=pl.ANY)
    low, high = jnp.bfloat16, jnp.float32
    dma = pltpu.SemaphoreType.DMA
    return pl.pallas_call(
        functools.partial(near_kernel, n, nt, group, pieces),
        out_shape=jax.ShapeDtypeStruct((rows, width), low),
        in_specs=[hbm] * 5 + [smem] + [hbm] * 11,
        out_specs=hbm,
        scratch_shapes=[
            pltpu.VMEM((seq, group * HEAD), low),
            pltpu.VMEM((seq, group * HEAD), low),
            pltpu.VMEM((2, seq, HEAD), low),
            pltpu.VMEM((seq, value_dim), low),
            pltpu.VMEM((rows, width), low),
            pltpu.VMEM((1, width), high),
            pltpu.VMEM((topk, rows), jnp.int32),
            pltpu.VMEM((topk, rows), high),
            pltpu.VMEM((2, tall, HEAD), low),
            pltpu.VMEM((n, 2, seq, HEAD), low),
            pltpu.VMEM((n, seq, value_dim), low),
            pltpu.VMEM((2, tall, 1), high),
            pltpu.VMEM((2, tall, 1), high),
            pltpu.VMEM((2, tall, value_dim), high),
            pltpu.VMEM((seq, features), low),
            pltpu.VMEM((features, width), low),
            pltpu.VMEM((2, 2 * rows, features), low),
            pltpu.VMEM((pieces, 2 * rows, span), low),
            pltpu.VMEM((pieces, 2 * rows, span), low),
            pltpu.VMEM((pieces, rows, span), low),
            pltpu.VMEM((pieces, rows, span), low),
            pltpu.VMEM((width // fine, rows, fine), low),
            pltpu.VMEM((2, width, hid), low),
            pltpu.VMEM((2, width, hid), low),
            pltpu.VMEM((width, wide), low),
            pltpu.VMEM((width, wide), low),
            pltpu.VMEM((n * hid + nt * wide, half), low),
            pltpu.VMEM((depth, pieces, rows, span), low),
            pltpu.VMEM((nt, pieces, rows, span), low),
            pltpu.VMEM((depth, 8, HEAD), high),
            pltpu.VMEM((nt, 8, HEAD), high),
            pltpu.VMEM((depth, 2, rows, hid), low),
            pltpu.VMEM((depth, 2, rows, hid), low),
            pltpu.VMEM((nt, rows, wide), low),
            pltpu.VMEM((nt, rows, wide), low),
            pltpu.VMEM((2, segments, rows, seg), low),
            pltpu.VMEM((half // fine, rows, fine), low),
            pltpu.VMEM((half // fine, rows, fine), low),
            pltpu.VMEM((width // fine, rows, fine), low),
            pltpu.VMEM((n, rows, HEAD), high),
            pltpu.VMEM((HEAD, HEAD), high),
            pltpu.VMEM((2 * hid, half), low),
            pltpu.VMEM((half // fine, rows, fine), high),
            dma((16,)),
            dma((2, 3, depth)),
            dma((3, n)),
            dma((1,)),
            dma((pieces,)),
            dma((1,)),
            dma((pieces,)),
            dma((2, 2)),
            dma((2, 2)),
            dma((3 * depth + 1,)),
            dma((n + 1,)),
            dma((3,)),
            dma((nt,)),
            dma((2, 2, depth)),
            dma((pieces + 1, depth)),
            dma((3, 2)),
            dma((2, nt)),
            dma((depth,)),
            dma((depth,)),
            dma((nt,)),
            dma((nt,)),
            dma((segments,)),
            dma((segments,)),
            dma((1,)),
            dma((half // fine,)),
            dma((1,)),
            dma((4,)),
            dma((2, 2)),
        ],
        compiler_params=pltpu.CompilerParams(
            collective_id=0, has_side_effects=True, vmem_limit_bytes=60 << 20
        ),
        name="layer",
    )(
        q_first, q_second, k_first, k_second, values, head_lambda, w_out, stream_in,
        norm_gain.reshape(1, width), routes.T, route_w.T, w_gate[0], w_up[0], s_gate, s_up, w_down[0], s_down,
    )


def layer(*arrays):
    n, nt = lax.axis_size("sp"), lax.axis_size("tp")
    k_first, values, w_gate, w_down, s_down = (arrays[i] for i in (3, 5, 11, 13, 16))
    fits = (
        4 <= n <= 16
        and n % 2 == 0
        and nt == 4
        and k_first.shape[1] == HEAD
        and arrays[0].shape[0] <= HEAD
        and w_gate.shape[0] == 1
        and w_down.shape[1] % (16 * nt) == 0
        and s_down.shape[0] % (16 * n) == 0
        and w_down.shape[1] % HEAD == 0
        and (2 * w_down.shape[1]) % s_down.shape[0] == 0
        and (nt * s_down.shape[0]) % (2 * w_down.shape[1]) == 0
        and w_down.shape[2] % (16 * HEAD) == 0
    )
    return near(*arrays) if fits else local(*arrays)


def solution(mesh):
    return jax.shard_map(
        layer,
        mesh=mesh,
        in_specs=(
            P(("sp", "tp"), None),
            P("sp", "tp"),
            P("sp", "tp"),
            P("sp", "tp"),
            P("sp", "tp"),
            P("sp", "tp"),
            P("tp"),
            P("tp", None),
            P(),
            P(("sp", "tp"), None),
            P(("sp", "tp"), None),
            P("sp", None, None),
            P("sp", None, None),
            P("sp", None, None),
            P(None, "tp"),
            P(None, "tp"),
            P("tp", None),
        ),
        out_specs=P(("sp", "tp"), None),
        check_vma=False,
    )
```

```python
import functools
import math

import jax
import jax.numpy as jnp
from jax import lax
from jax.experimental import pallas as pl
from jax.experimental.pallas import tpu as pltpu
from jax.sharding import PartitionSpec as P

HEAD = 128


FLOOR = -1e30


def absorb(state, first_q, second_q, first_k, second_k, value_rows, query_pos, key_pos):
    allowed = key_pos[None, :] <= query_pos[:, None]
    scale = first_q.shape[-1] ** (-0.5)
    result = []
    pairs = ((first_q, first_k), (second_q, second_k))
    for index in range(2):
        query_rows, key_rows = pairs[index]
        peak, total, accum = (state[3 * index], state[3 * index + 1], state[3 * index + 2])
        scores = (
            jnp.einsum("qagd,kad->agqk", query_rows, key_rows, preferred_element_type=jnp.float32)
            * scale
        )
        scores = jnp.where(allowed, scores, FLOOR)
        raised = jnp.maximum(peak, scores.max(-1))
        weights = jnp.where(allowed, jnp.exp(scores - raised[..., None]), 0.0)
        fade = jnp.exp(peak - raised)
        total = total * fade + weights.sum(-1)
        accum = accum * fade[..., None] + jnp.einsum(
            "agqk,kad->agqd",
            weights.astype(jnp.bfloat16),
            value_rows,
            preferred_element_type=jnp.float32,
        )
        result += [raised, total, accum]
    return tuple(result)


def empty_state(kv_local, group, count, value_dim):
    peaks = jnp.full((kv_local, group, count), FLOOR, jnp.float32)
    sums = jnp.zeros((kv_local, group, count), jnp.float32)
    accums = jnp.zeros((kv_local, group, count, value_dim), jnp.float32)
    return (peaks, sums, accums, peaks, sums, accums)


def fold_rows(state, first_q, second_q, query_pos, last_row, pieces, start):
    first_k, second_k, value_rows = pieces
    length = first_k.shape[0]
    kv_local = first_q.shape[1]
    value_dim = value_rows.shape[1] // kv_local
    span = math.gcd(length, 2048)

    def sweep(current):

        def visit(block, inner):
            begin = block * span
            key_one = lax.dynamic_slice_in_dim(first_k, begin, span, 0).reshape(
                span, kv_local, HEAD
            )
            key_two = lax.dynamic_slice_in_dim(second_k, begin, span, 0).reshape(
                span, kv_local, HEAD
            )
            value_part = lax.dynamic_slice_in_dim(value_rows, begin, span, 0).reshape(
                span, kv_local, value_dim
            )
            key_pos = begin + jnp.arange(span, dtype=jnp.int32)
            return absorb(
                inner, first_q, second_q, key_one, key_two, value_part, query_pos, key_pos
            )

        return lax.fori_loop(0, length // span, visit, current)

    def unchanged(current):
        return current

    return lax.cond(start <= last_row, sweep, unchanged, state)


def finish_heads(final, head_lambda):
    kv_local, group, count, value_dim = final[2].shape
    weight = head_lambda.reshape(kv_local, group, 1, 1)
    head_out = final[2] / final[1][..., None] - weight * final[5] / final[4][..., None]
    head_out = head_out * lax.rsqrt(jnp.mean(head_out * head_out, axis=-1, keepdims=True) + 1e-05)
    return (
        head_out.transpose(2, 0, 1, 3)
        .reshape(count, kv_local * group * value_dim)
        .astype(jnp.bfloat16)
    )


def shared_part(normed, s_gate, s_up, s_down):
    piece = lax.all_gather(normed, "tp", axis=0, tiled=True)
    gate_part = jnp.dot(piece, s_gate, preferred_element_type=jnp.float32)
    up_part = jnp.dot(piece, s_up, preferred_element_type=jnp.float32)
    hidden = (jax.nn.silu(gate_part) * up_part).astype(jnp.bfloat16)
    terms = jnp.dot(hidden, s_down, preferred_element_type=jnp.float32)
    return lax.psum_scatter(
        terms.astype(jnp.bfloat16), "tp", scatter_dimension=0, tiled=True
    ).astype(jnp.float32)


def routed_part(normed, routes, route_w, w_gate, w_up, w_down):
    rows, topk = routes.shape
    local_experts = w_gate.shape[0]
    experts = local_experts * lax.axis_size("sp")
    slots = max(2, 3 * rows * topk // (2 * experts))
    flat_ids = routes.reshape(-1)
    hits = (flat_ids[:, None] == jnp.arange(experts, dtype=jnp.int32)[None, :]).astype(jnp.int32)
    slot_of = jnp.sum(jnp.cumsum(hits, axis=0) * hits, axis=1) - 1
    target = flat_ids * slots + slot_of
    placing = jnp.any(
        jnp.arange(experts * slots, dtype=jnp.int32)[:, None, None]
        == target.reshape(rows, topk)[None, :, :],
        axis=-1,
    ).astype(jnp.bfloat16)
    outgoing = (
        jnp.dot(placing, normed, preferred_element_type=jnp.float32)
        .astype(jnp.bfloat16)
        .reshape(experts, slots, normed.shape[1])
    )
    arrived = lax.all_to_all(outgoing, "sp", split_axis=0, concat_axis=0, tiled=True)
    sources = arrived.shape[0] // local_experts
    grouped = arrived.reshape(sources, local_experts, arrived.shape[1], arrived.shape[2])
    gate_part = jnp.einsum("sjcd,jdf->sjcf", grouped, w_gate, preferred_element_type=jnp.float32)
    up_part = jnp.einsum("sjcd,jdf->sjcf", grouped, w_up, preferred_element_type=jnp.float32)
    hidden = (jax.nn.silu(gate_part) * up_part).astype(jnp.bfloat16)
    result = jnp.einsum(
        "sjcf,jfd->sjcd", hidden, w_down, preferred_element_type=jnp.float32
    ).astype(jnp.bfloat16)
    returned = lax.all_to_all(
        result.reshape(arrived.shape), "sp", split_axis=0, concat_axis=0, tiled=True
    )
    picked = (
        returned.reshape(experts * slots, normed.shape[1])[target]
        .reshape(rows, topk, normed.shape[1])
        .astype(jnp.float32)
    )
    return jnp.sum(picked * route_w[..., None], axis=1)


def local(
    stream_in,
    q_first,
    q_second,
    k_first,
    k_second,
    values,
    head_lambda,
    w_out,
    norm_gain,
    routes,
    route_w,
    w_gate,
    w_up,
    w_down,
    s_gate,
    s_up,
    s_down,
):
    seq_rows = q_first.shape[0]
    kv_local = k_first.shape[1] // HEAD
    heads_local = q_first.shape[1] // HEAD
    group = heads_local // kv_local
    value_dim = values.shape[1] // kv_local
    offset = lax.axis_index("sp") * seq_rows
    query_pos = offset + jnp.arange(seq_rows, dtype=jnp.int32)
    last_row = offset + seq_rows - 1
    first_q = q_first.reshape(seq_rows, kv_local, group, HEAD)
    second_q = q_second.reshape(seq_rows, kv_local, group, HEAD)
    start_state = empty_state(kv_local, group, seq_rows, value_dim)
    folded_state = fold_rows(
        start_state,
        first_q,
        second_q,
        query_pos,
        last_row,
        (
            lax.all_gather(k_first, "sp", axis=0, tiled=True),
            lax.all_gather(k_second, "sp", axis=0, tiled=True),
            lax.all_gather(values, "sp", axis=0, tiled=True),
        ),
        jnp.int32(0),
    )
    attn_rows = finish_heads(folded_state, head_lambda)
    attn = lax.psum_scatter(
        jnp.dot(attn_rows, w_out, preferred_element_type=jnp.float32).astype(jnp.bfloat16),
        "tp",
        scatter_dimension=0,
        tiled=True,
    ).astype(jnp.float32)
    resid = (stream_in.astype(jnp.float32) + attn).astype(jnp.bfloat16)
    stream = lax.optimization_barrier(resid).astype(jnp.float32)
    normed = (
        stream * lax.rsqrt(jnp.mean(stream * stream, axis=-1, keepdims=True) + 1e-06) * norm_gain
    ).astype(jnp.bfloat16)
    routed = routed_part(normed, routes, route_w, w_gate, w_up, w_down)
    shared = shared_part(normed, s_gate, s_up, s_down)
    return (stream + routed + shared).astype(jnp.bfloat16)


def mesh_copy(src, dst, send_sem, recv_sem, axis, target):
    return pltpu.make_async_remote_copy(
        src_ref=src,
        dst_ref=dst,
        send_sem=send_sem,
        recv_sem=recv_sem,
        device_id={axis: target},
        device_id_type=pl.DeviceIdType.MESH,
    )


def greet(axis, target):
    pl.semaphore_signal(
        pltpu.get_barrier_semaphore(),
        inc=1,
        device_id={axis: target},
        device_id_type=pl.DeviceIdType.MESH,
    )


def near_kernel(
    n, nt, group, pieces,
    q_one_h, q_two_h, k_one_h, k_two_h, val_h, lam, w_out_h, stream_h, gain_h, route_h, share_h,
    gate_h, up_h, s_gate_h, s_up_h, down_h, s_down_h,
    out,
    q_one, q_two, k_own, val, stream, gain, route_t, share_t,
    stacked, keys, vals, peak, total, accum, rows_in,
    w, order, out_one, in_one, out_two, in_two, resid,
    gates, ups, s_gate, s_up, wall, gathered, beside, stat, stat_b,
    out_hid, in_hid, out_sh, in_sh, units, out_fin, in_fin, result, mix, square, extra, partial,
    load, send_kv, recv_kv, send_one, recv_one, send_two, recv_two,
    send_g, recv_g, send_d, recv_d, send_sd, recv_sd,
    send_x, recv_x, send_b, recv_b, send_h, recv_h, send_s, recv_s,
    send_u, recv_u, send_f, recv_f, save, send_e, recv_e,
):
    me, mine = lax.axis_index("sp"), lax.axis_index("tp")
    place, side = me // 2, me % 2
    far, core = mine // 2, mine % 2
    depth = n // 2
    pair, partner, across = me + 1 - 2 * side, mine + 1 - 2 * core, 2 * (1 - far) + core
    above, below = place < depth - 1, place > 0
    seq = q_one.shape[0]
    rows, width = stream.shape
    hid, wide = down_h.shape[0], s_down_h.shape[0]
    scale = HEAD ** (-0.5)
    half = width // 2

    def column(o):
        return 2 * ((place + o) % depth) + side

    def cols_of(f):
        return pl.ds(pl.multiple_of(f * half, half), half)

    loads = [
        pltpu.make_async_copy(source, target, load.at[i])
        for i, (source, target) in enumerate(
            (
                (w_out_h, w),
                (gate_h, gates.at[0]),
                (up_h, ups.at[0]),
                (s_gate_h, s_gate),
                (s_up_h, s_up),
                (
                    down_h.at[:, cols_of(far)],
                    wall.at[pl.ds(pl.multiple_of(me * hid, hid), hid)],
                ),
                (
                    s_down_h.at[:, cols_of(far)],
                    wall.at[pl.ds(pl.multiple_of(n * hid + mine * wide, wide), wide)],
                ),
            )
        )
    ]
    for o in range(1, depth):
        greet("sp", column(o))
    greet("sp", pair)
    greet("tp", across)
    greet("tp", partner)
    inputs = [
        pltpu.make_async_copy(source, target, load.at[7 + i])
        for i, (source, target) in enumerate(
            (
                (k_one_h, k_own.at[0]),
                (k_two_h, k_own.at[1]),
                (val_h, val),
                (q_one_h, q_one),
                (q_two_h, q_two),
                (stream_h, stream),
                (gain_h, gain),
                (route_h, route_t),
                (share_h, share_t),
            )
        )
    ]
    for one in inputs:
        one.start()
    for one in inputs[:3]:
        one.wait()
    pl.semaphore_wait(pltpu.get_barrier_semaphore(), depth + 2)

    mid = seq // 2

    def stuff(block):
        return keys.at[block], vals.at[block, :mid], vals.at[block, mid:]

    def copies(block, way, target, own):
        return [
            mesh_copy(
                (k_own, val.at[:mid], val.at[mid:])[a] if own else stuff(block)[a],
                stuff(block)[a],
                send_kv.at[way, a, block // 2],
                recv_kv.at[a, block],
                "sp",
                target,
            )
            for a in range(3)
        ]

    def start(block, way, target, own=False):
        for one in copies(block, way, target, own):
            one.start()

    def arrive(block):
        for one in copies(block, 0, pair, False):
            one.wait_recv()

    share = width // 2
    share_at = pl.ds(pl.multiple_of(core * share, share), share)
    other_at = pl.ds(pl.multiple_of((1 - core) * share, share), share)

    def pair_weights():
        return [
            mesh_copy(
                h.at[share_at], v.at[1, share_at], send_g.at[0, i], recv_g.at[0, i], "sp", pair
            )
            for i, (h, v) in enumerate(((gate_h, gates), (up_h, ups)))
        ]

    def pair_weights_on(at):
        return [
            mesh_copy(
                v.at[1, at], v.at[1, at], send_g.at[1, i], recv_g.at[1, i], "tp", partner
            )
            for i, v in enumerate((gates, ups))
        ]

    part = hid // 2

    def down_at(block, c):
        return wall.at[pl.ds(pl.multiple_of(block * hid + c * part, part), part)]

    def down_own(way, target):
        return mesh_copy(
            down_h.at[pl.ds(pl.multiple_of(core * part, part), part), cols_of(far)],
            down_at(me, core),
            send_d.at[way],
            recv_d.at[me],
            "sp",
            target,
        )

    def down_pair(block):
        return mesh_copy(
            down_at(block, core),
            down_at(block, core),
            send_d.at[depth + block // 2],
            recv_d.at[block],
            "sp",
            pair,
        )

    def down_core(block, c):
        return mesh_copy(
            down_at(block, c),
            down_at(block, c),
            send_d.at[3 * depth],
            recv_d.at[n],
            "tp",
            partner,
        )

    def extra_at(s, c):
        return extra.at[pl.ds(pl.multiple_of(s * hid + c * part, part), part)]

    def extra_own():
        return mesh_copy(
            down_h.at[pl.ds(pl.multiple_of(core * part, part), part), cols_of(1 - far)],
            extra_at(side, core),
            send_e.at[0],
            recv_e.at[0, side],
            "sp",
            side,
        )

    def extra_pair(s):
        return mesh_copy(
            extra_at(s, core), extra_at(s, core), send_e.at[1], recv_e.at[0, s], "sp", pair
        )

    def extra_core(s, c):
        return mesh_copy(
            extra_at(s, c), extra_at(s, c), send_e.at[2 + s], recv_e.at[1, s], "tp", partner
        )

    def sd_at(u):
        return wall.at[pl.ds(pl.multiple_of(n * hid + u * wide, wide), wide)]

    def sd_own(way, f, target):
        return mesh_copy(
            s_down_h.at[:, cols_of(f)], sd_at(mine), send_sd.at[way], recv_sd.at[mine], "tp", target
        )

    def sd_on(u):
        return mesh_copy(sd_at(u), sd_at(u), send_sd.at[2], recv_sd.at[u], "tp", partner)

    @pl.when(above)
    def _():
        start(me, 0, me + 2, True)

    @pl.when(side == 0)
    def _():
        start(me, 1, pair, True)

    for one in loads:
        one.start()
    late = place >= depth // 2

    @pl.when(late)
    def _():
        sd_own(1, 1 - far, across).start()

    sd_own(0, far, partner).start()
    for o in range(1, depth):

        @pl.when(place + o >= depth)
        def _():
            down_own(o, column(o)).start()

    top_place = place == depth - 1
    pl.when(top_place)(lambda: extra_own().start())

    for one in inputs[3:]:
        one.wait()
    for index, q in enumerate((q_one, q_two)):
        for h in range(group):
            stacked[index, h * seq : (h + 1) * seq, :] = q[:, h * HEAD : (h + 1) * HEAD]

    def scores_of(index, some):
        return (
            lax.dot_general(
                stacked[index], some, (((1,), (1,)), ((), ())), preferred_element_type=jnp.float32
            )
            * scale
        )

    spread = (group * seq, seq)
    row_of = lax.broadcasted_iota(jnp.int32, spread, 0) % seq
    allowed = lax.broadcasted_iota(jnp.int32, spread, 1) <= row_of
    for index in range(2):
        scores = jnp.where(allowed, scores_of(index, k_own[index]), FLOOR)
        top = jnp.max(scores, axis=-1, keepdims=True)
        weights = jnp.exp(scores - top)
        peak[index] = top
        total[index] = jnp.sum(weights, axis=-1, keepdims=True)
        accum[index] = jnp.dot(
            weights.astype(jnp.bfloat16), val[...], preferred_element_type=jnp.float32
        )

    def fold(block):
        for index in range(2):
            scores = scores_of(index, keys[block, index])
            old = peak[index]
            top = jnp.maximum(old, jnp.max(scores, axis=-1, keepdims=True))
            weights = jnp.exp(scores - top)
            fade = jnp.exp(old - top)
            peak[index] = top
            total[index] = total[index] * fade + jnp.sum(weights, axis=-1, keepdims=True)
            accum[index] = accum[index] * fade + jnp.dot(
                weights.astype(jnp.bfloat16), vals[block], preferred_element_type=jnp.float32
            )

    def down_up(block):
        return mesh_copy(
            down_at(block, core),
            down_at(block, core),
            send_d.at[2 * depth + block // 2],
            recv_d.at[block],
            "sp",
            me + 2,
        )

    def lift(d):
        @pl.when((place >= d) & above)
        def _():
            down_up(me - 2 * d).wait_recv()
            down_up(me - 2 * d).start()

    def weights_out():
        pl.when(above)(lambda: down_own(1, me + 2).start())
        for one in pair_weights():
            one.start()
        down_own(0, pair).start()
        lift(1)

    pl.when(place == 0)(weights_out)

    def visit(e, carry):
        @pl.when(place >= e)
        def _():
            block = me - 2 * e
            for up, over in zip(copies(block, 0, me + 2, False), copies(block, 1, pair, False)):
                over.wait_recv()
                pl.when(above)(up.start)
                over.start()
            pl.when(e == place)(weights_out)
            fold(block)

        @pl.when((place >= e - 1) & ((e > 1) | (side == 1)))
        def _():
            block = pair - 2 * (e - 1)
            arrive(block)
            fold(block)

        return carry

    lax.fori_loop(1, depth + 1, visit, 0)

    for d in range(2, depth):
        lift(d)

    for h in range(group):
        cut = slice(h * seq, (h + 1) * seq)
        head = accum[0, cut, :] / total[0, cut, :] - lam[h] * (
            accum[1, cut, :] / total[1, cut, :]
        )
        head = head * lax.rsqrt(jnp.mean(head * head, axis=-1, keepdims=True) + 1e-05)
        size = head.shape[1]
        rows_in[:, h * size : (h + 1) * size] = head.astype(jnp.bfloat16)

    for o in range(2):
        base = 2 * ((far + o) % 2)
        for which, parity in enumerate((1 - core, core)):
            begin = pl.multiple_of((base + parity) * rows, rows)
            order[which, o * rows : (o + 1) * rows, :] = rows_in[pl.ds(begin, rows), :]

    first = [
        mesh_copy(out_one.at[i], in_one.at[i], send_one.at[0], recv_one.at[i], "tp", partner)
        for i in range(pieces)
    ]
    second = [
        mesh_copy(out_two.at[i], in_two.at[i], send_two.at[0], recv_two.at[i], "tp", across)
        for i in range(pieces)
    ]
    span = width // pieces
    loads[0].wait()
    for i in range(pieces):
        out_one[i] = jnp.dot(
            order[0], w[:, i * span : (i + 1) * span], preferred_element_type=jnp.float32
        ).astype(jnp.bfloat16)
        first[i].start()
    kept = []
    for i in range(pieces):
        sums = jnp.dot(
            order[1], w[:, i * span : (i + 1) * span], preferred_element_type=jnp.float32
        )
        first[i].wait_recv()
        sums = sums + in_one[i].astype(jnp.float32)
        out_two[i] = sums[rows:].astype(jnp.bfloat16)
        second[i].start()
        kept.append(sums[:rows])

    @pl.when(jnp.logical_not(late))
    def _():
        sd_own(1, 1 - far, across).start()

    def row_part(block, extra, spot, i):
        return block.at[spot, i] if i < pieces else extra.at[spot]

    def row_copy(spot, way, target, i):
        some = row_part(gathered, stat, spot, i)
        return mesh_copy(
            some,
            some,
            send_x.at[way, i // pieces, spot],
            recv_x.at[i, spot],
            "sp",
            target,
        )

    def rows_sent(spot, way):
        for some, kind in ((gathered.at[spot], 0), (stat.at[spot], 1)):
            mesh_copy(
                some, some, send_x.at[way, kind, spot], recv_x.at[0, spot], "sp", pair
            ).wait_send()

    def beside_own(way, target, i):
        return mesh_copy(
            row_part(gathered, stat, place, i),
            row_part(beside, stat_b, mine, i),
            send_b.at[way, i // pieces],
            recv_b.at[i // pieces, mine],
            "tp",
            target,
        )

    def beside_on(u, kind, way=2):
        some = (beside, stat_b)[kind].at[u]
        return mesh_copy(some, some, send_b.at[way, kind], recv_b.at[kind, u], "tp", partner)

    def raise_row(e, i):
        row_copy(place - e, 0, pair, i).wait_recv()
        row_copy(place - e, 0, me + 2, i).start()

    def lower_row(e, i):
        row_copy(place + e, 0, pair, i).wait_recv()
        row_copy(place + e, 1, me - 2, i).start()

    def rows_out(i):
        pl.when(above)(lambda: row_copy(place, 0, me + 2, i).start())
        pl.when(below)(lambda: row_copy(place, 1, me - 2, i).start())
        beside_own(1, across, i).start()
        beside_own(0, partner, i).start()

    fine = resid.shape[2]
    per = span // fine
    squares = jnp.zeros((rows, 1), jnp.float32)
    for i in range(pieces):
        cut = slice(i * span, (i + 1) * span)
        second[i].wait_recv()
        sums = kept[i] + in_two[i].astype(jnp.float32)
        sums = (stream[:, cut].astype(jnp.float32) + sums).astype(jnp.bfloat16)
        for j in range(per):
            resid[i * per + j] = sums[:, j * fine : (j + 1) * fine]
        sums = sums.astype(jnp.float32)
        squares = squares + jnp.sum(sums * sums, axis=-1, keepdims=True)
        gathered[place, i] = (sums * gain[:, cut]).astype(jnp.bfloat16)
        rows_out(i)
    shrink = lax.rsqrt(squares / width + 1e-06)
    square[0:rows, :] = jnp.broadcast_to(shrink, (rows, HEAD))
    stat[place] = square[...].T[0 : stat.shape[1], :]
    rows_out(pieces)
    ahead = pieces // 2
    for e in range(1, depth - 1):
        for i in range(pieces + 1 if e == 1 else ahead):
            pl.when(above & (place >= e))(lambda: raise_row(e, i))
        if e == 1:
            for i in range(pieces + 1):
                pl.when(above & below)(lambda: lower_row(1, i))
    def pass_down(e):
        def one(block, fresh):
            pl.when(fresh)(lambda: down_pair(block).wait_recv())
            down_pair(block).start()
            down_core(block, core).start()

        pl.when(place >= e)(lambda: one(me - 2 * e, jnp.logical_not(above)))
        pl.when(place + e < depth)(lambda: one(me + 2 * e, place >= 0))

    def collect(e):
        def one(block):
            down_pair(block).wait_recv()
            down_core(block, core).start()

        pl.when(place >= e)(lambda: one(pair - 2 * e))
        pl.when(place + e < depth)(lambda: one(pair + 2 * e))

    def factors(scales, spot):
        square[0 : scales.shape[1], :] = scales[spot]
        return square[...].T[0:rows, :1]

    def hidden_of(block, spot, factor, g, u):
        def project(m):
            parts = [
                jnp.dot(
                    block[spot, i],
                    m[i * span : (i + 1) * span, :],
                    preferred_element_type=jnp.float32,
                )
                for i in range(pieces)
            ]
            return sum(parts[1:], parts[0]) * factor

        gate_part, up_part = project(g), project(u)
        return (gate_part / (1.0 + jnp.exp(-gate_part)) * up_part).astype(jnp.bfloat16)

    for one, onward in zip(pair_weights(), pair_weights_on(share_at)):
        one.wait_recv()
        onward.start()
    for d in range(1, depth):
        pass_down(d)
    for e in range(2, depth - 1):
        for i in range(ahead):
            pl.when(below & (place + e < depth))(lambda: lower_row(e, i))

    square[...] = jnp.zeros_like(square)
    for j in range(n):
        chosen = jnp.where(route_t[...] == j, share_t[...], 0.0)
        square[j : j + 1, 0:rows] = jnp.sum(chosen, axis=0, keepdims=True)
    turned = square[...].T
    for j in range(n):
        mix[j] = jnp.broadcast_to(turned[0:rows, j : j + 1], mix.shape[1:])
    for i in range(1, 5):
        loads[i].wait()

    def hid_copy(spot):
        return mesh_copy(
            out_hid.at[spot], in_hid.at[place], send_h.at[spot], recv_h.at[place], "sp",
            2 * spot + side,
        )

    def serve(spot):
        factor = factors(stat, spot)
        out_hid[spot, side] = hidden_of(gathered, spot, factor, gates.at[0], ups.at[0])
        out_hid[spot, 1 - side] = hidden_of(gathered, spot, factor, gates.at[1], ups.at[1])
        hid_copy(spot).start()

    def serve_last(spot):
        sums = None
        mats = (gates.at[0], ups.at[0], gates.at[1], ups.at[1])
        for i in range(pieces):
            row_copy(spot, 0, pair, i).wait_recv()
            parts = [
                jnp.dot(
                    gathered[spot, i],
                    m[i * span : (i + 1) * span, :],
                    preferred_element_type=jnp.float32,
                )
                for m in mats
            ]
            sums = parts if sums is None else [a + b for a, b in zip(sums, parts)]
        row_copy(spot, 0, pair, pieces).wait_recv()
        factor = factors(stat, spot)
        g_one, u_one, g_two, u_two = [v * factor for v in sums]
        for which, g, u in ((side, g_one, u_one), (1 - side, g_two, u_two)):
            out_hid[spot, which] = (g / (1.0 + jnp.exp(-g)) * u).astype(jnp.bfloat16)
        hid_copy(spot).start()

    def sh_copy(u):
        return mesh_copy(
            out_sh.at[u], in_sh.at[mine], send_s.at[u], recv_s.at[mine], "tp", u
        )

    def answer(u):
        out_sh[u] = hidden_of(beside, u, factors(stat_b, u), s_gate, s_up)
        sh_copy(u).start()

    def turn(e, carry):
        low, high = place >= e, place + e < depth

        @pl.when(low & jnp.logical_not(above))
        def _():
            for i in range(pieces + 1):
                row_copy(place - e, 0, pair, i).wait_recv()

        @pl.when(high & jnp.logical_not(below))
        def _():
            for i in range(pieces + 1):
                row_copy(place + e, 0, pair, i).wait_recv()

        @pl.when(e == 1)
        def _():
            factor = factors(stat, place)
            in_sh[mine] = hidden_of(gathered, place, factor, s_gate, s_up)
            in_hid[place, side] = hidden_of(gathered, place, factor, gates.at[0], ups.at[0])
            for one in pair_weights_on(other_at):
                one.wait_recv()

        @pl.when(low)
        def _():
            serve(place - e)

        @pl.when(high)
        def _():
            serve(place + e)

        @pl.when(e == 1)
        def _():
            for d in range(2, depth - 1):
                for i in range(ahead, pieces + 1):
                    pl.when(above & (place >= d))(lambda: raise_row(d, i))
                    pl.when(below & (place + d < depth))(lambda: lower_row(d, i))

        @pl.when(e == 2)
        def _():
            down_pair(pair).wait_recv()
            down_core(pair, core).start()
            in_hid[place, 1 - side] = hidden_of(
                gathered, place, factors(stat, place), gates.at[1], ups.at[1]
            )
            u = across
            for kind in range(2):
                beside_on(u, kind).wait_recv()
                beside_on(u, kind).start()
            answer(u)
            sd_on(u).wait_recv()
            sd_on(u).start()
            for o in range(2):
                u = 2 * ((far + o) % 2) + 1 - core
                for kind in range(2):
                    beside_on(u, kind).wait_recv()
                answer(u)

        return carry

    @pl.when(place == 0)
    def _():
        extra_pair(side).wait_recv()
        extra_pair(side).start()
        extra_core(side, core).start()

    lax.fori_loop(1, depth - 1, turn, 0)
    last = depth - 1

    @pl.when(place == 0)
    def _():
        serve_last(last)

    segments = units.shape[1]

    def unit_copy(s):
        return mesh_copy(
            units.at[0, s], units.at[1, s], send_u.at[s], recv_u.at[s], "tp", across
        )

    seg = units.shape[3]

    def share_units():
        for o in range(1, nt):
            u = (mine + o) % nt
            mesh_copy(
                out_sh.at[u], in_sh.at[u], send_s.at[u], recv_s.at[u], "tp", u
            ).wait_recv()
        for j in range(nt):
            at = j * wide
            units[0, depth + at // seg, :, at % seg : at % seg + wide] = in_sh[j]
        for s in range(depth, segments):
            unit_copy(s).start()

    pl.when(top_place)(share_units)

    def place_unit(spot):
        @pl.when(place != spot)
        def _():
            mesh_copy(
                out_hid.at[spot], in_hid.at[spot], send_h.at[spot], recv_h.at[spot], "sp",
                2 * spot + side,
            ).wait_recv()

        for k in range(2):
            j = 2 * spot + k
            units[0, spot, :, k * hid : (k + 1) * hid] = (
                in_hid[spot, k].astype(jnp.float32) * mix[j][:, :1]
            ).astype(jnp.bfloat16)

    @pl.when(place != 0)
    def _():
        place_unit(last)
        unit_copy(last).start()

    for spot in range(last - 1, -1, -1):
        place_unit(spot)
        unit_copy(spot).start()

    pl.when(jnp.logical_not(top_place))(share_units)
    for e in range(1, depth - 1):
        collect(e)

    collect(last)

    @pl.when(top_place)
    def _():
        serve_last(0)

    @pl.when(place == 0)
    def _():
        extra_pair(1 - side).wait_recv()
        extra_core(1 - side, core).start()


    loads[5].wait()
    loads[6].wait()
    for o in range(2):
        sd_on(2 * ((far + o) % 2) + 1 - core).wait_recv()

    taken = wall.at[pl.ds(0, (n - 1) * part)]
    cores = mesh_copy(taken, taken, send_d.at[3 * depth], recv_d.at[n], "tp", partner)
    cores.wait_recv()
    early = [s for s in range(segments) if s != last]
    for s in early:
        unit_copy(s).wait_recv()
    pl.when(place != 0)(lambda: unit_copy(last).wait_recv())

    def fin_copy(i):
        return mesh_copy(out_fin.at[i], in_fin.at[i], send_f.at[0], recv_f.at[i], "tp", across)

    def put(spot):
        return pltpu.make_async_copy(
            result.at[spot],
            out.at[:, pl.ds(pl.multiple_of(spot * fine, fine), fine)],
            save.at[0],
        )

    def close(spot, terms):
        result[spot] = (resid[spot].astype(jnp.float32) + terms).astype(jnp.bfloat16)
        put(spot).start()

    count = half // fine
    mine_at, other_of = far * count, (1 - far) * count
    for i in range(count):
        cut = slice(i * fine, (i + 1) * fine)
        terms = [
            jnp.dot(
                units[:, s].reshape(2 * rows, seg),
                wall[s * seg : (s + 1) * seg, cut],
                preferred_element_type=jnp.float32,
            )
            for s in early
        ]
        both = sum(terms[1:], terms[0])

        @pl.when(place == 0)
        def _():
            partial[i] = both[:rows]
            out_fin[i] = both[rows:].astype(jnp.bfloat16)
            fin_copy(i).start()

        @pl.when(place != 0)
        def _():
            full = both + jnp.dot(
                units[:, last].reshape(2 * rows, seg),
                wall[last * seg : (last + 1) * seg, cut],
                preferred_element_type=jnp.float32,
            )
            out_fin[i] = full[rows:].astype(jnp.bfloat16)
            fin_copy(i).start()
            close(mine_at + i, full[:rows])

    @pl.when(place == 0)
    def _():
        extra_core(0, 1 - core).wait_recv()
        extra_core(1, 1 - core).wait_recv()
        for i in range(count):
            fin_copy(i).wait_recv()
        place_unit(last)
        rest = units[0, last]
        for i in range(count):
            cut = slice(i * fine, (i + 1) * fine)
            terms = jnp.dot(
                rest, wall[last * seg : (last + 1) * seg, cut], preferred_element_type=jnp.float32
            )
            close(mine_at + i, partial[i] + terms)
            terms = jnp.dot(rest, extra[:, cut], preferred_element_type=jnp.float32)
            close(other_of + i, in_fin[i].astype(jnp.float32) + terms)

    @pl.when(place != 0)
    def _():
        for i in range(count):
            fin_copy(i).wait_recv()
            close(other_of + i, in_fin[i].astype(jnp.float32))

    def settle(e, carry):
        @pl.when(place >= e)
        def _():
            block = me - 2 * e

            @pl.when(above)
            def _():
                for one in copies(block, 0, me + 2, False):
                    one.wait_send()

                @pl.when(e > 0)
                def _():
                    down_up(block).wait_send()

            @pl.when((e > 0) | (side == 0))
            def _():
                for one in copies(block, 1, pair, False):
                    one.wait_send()

        pl.when((place + e < depth) & below)(lambda: rows_sent(place + e, 1))
        pl.when((place >= e) & above)(lambda: rows_sent(place - e, 0))

        @pl.when(e != place)
        def _():
            hid_copy(e).wait_send()
            down_pair(2 * e + side).wait_send()

        return carry

    lax.fori_loop(0, depth, settle, 0)

    cores.wait_send()
    for one in pair_weights() + pair_weights_on(share_at):
        one.wait_send()
    for some, sem, rec in (
        (out_one, send_one.at[0], recv_one.at[0]),
        (out_two, send_two.at[0], recv_two.at[0]),
        (out_fin, send_f.at[0], recv_f.at[0]),
    ):
        mesh_copy(some, some, sem, rec, "tp", partner).wait_send()
    for o in range(1, depth):
        pl.when((place + o >= depth) | (o == 1))(lambda: down_own(o, column(o)).wait_send())
    down_own(0, pair).wait_send()
    sd_own(0, far, partner).wait_send()
    sd_own(1, 1 - far, across).wait_send()
    sd_on(across).wait_send()
    for kind in range(2):
        for way in range(3):
            beside_on(across, kind, way).wait_send()
    for o in range(1, nt):
        sh_copy((mine + o) % nt).wait_send()
    for s in early:
        unit_copy(s).wait_send()
    pl.when(place != 0)(lambda: unit_copy(last).wait_send())
    pl.when(top_place)(lambda: extra_own().wait_send())

    @pl.when(place == 0)
    def _():
        extra_pair(side).wait_send()
        extra_core(0, core).wait_send()
        extra_core(1, core).wait_send()

    pltpu.make_async_copy(stream_h, stream, save.at[0]).wait()


def near(
    stream_in,
    q_first,
    q_second,
    k_first,
    k_second,
    values,
    head_lambda,
    w_out,
    norm_gain,
    routes,
    route_w,
    w_gate,
    w_up,
    w_down,
    s_gate,
    s_up,
    s_down,
):
    n, nt = lax.axis_size("sp"), lax.axis_size("tp")
    depth = n // 2
    seq, rows, width = q_first.shape[0], stream_in.shape[0], stream_in.shape[1]
    group, value_dim = q_first.shape[1] // HEAD, values.shape[1]
    hid, wide = w_down.shape[1], s_down.shape[0]
    tall, features = group * seq, group * value_dim
    pieces = 4
    span = width // pieces
    half, fine = width // 2, width // 8
    seg = 2 * hid
    segments = depth + nt * wide // seg
    topk = routes.shape[1]
    smem = pl.BlockSpec(memory_space=pltpu.SMEM)
    hbm = pl.BlockSpec(memory_space=pl.ANY)
    low, high = jnp.bfloat16, jnp.float32
    dma = pltpu.SemaphoreType.DMA
    return pl.pallas_call(
        functools.partial(near_kernel, n, nt, group, pieces),
        out_shape=jax.ShapeDtypeStruct((rows, width), low),
        in_specs=[hbm] * 5 + [smem] + [hbm] * 11,
        out_specs=hbm,
        scratch_shapes=[
            pltpu.VMEM((seq, group * HEAD), low),
            pltpu.VMEM((seq, group * HEAD), low),
            pltpu.VMEM((2, seq, HEAD), low),
            pltpu.VMEM((seq, value_dim), low),
            pltpu.VMEM((rows, width), low),
            pltpu.VMEM((1, width), high),
            pltpu.VMEM((topk, rows), jnp.int32),
            pltpu.VMEM((topk, rows), high),
            pltpu.VMEM((2, tall, HEAD), low),
            pltpu.VMEM((n, 2, seq, HEAD), low),
            pltpu.VMEM((n, seq, value_dim), low),
            pltpu.VMEM((2, tall, 1), high),
            pltpu.VMEM((2, tall, 1), high),
            pltpu.VMEM((2, tall, value_dim), high),
            pltpu.VMEM((seq, features), low),
            pltpu.VMEM((features, width), low),
            pltpu.VMEM((2, 2 * rows, features), low),
            pltpu.VMEM((pieces, 2 * rows, span), low),
            pltpu.VMEM((pieces, 2 * rows, span), low),
            pltpu.VMEM((pieces, rows, span), low),
            pltpu.VMEM((pieces, rows, span), low),
            pltpu.VMEM((width // fine, rows, fine), low),
            pltpu.VMEM((2, width, hid), low),
            pltpu.VMEM((2, width, hid), low),
            pltpu.VMEM((width, wide), low),
            pltpu.VMEM((width, wide), low),
            pltpu.VMEM((n * hid + nt * wide, half), low),
            pltpu.VMEM((depth, pieces, rows, span), low),
            pltpu.VMEM((nt, pieces, rows, span), low),
            pltpu.VMEM((depth, 8, HEAD), high),
            pltpu.VMEM((nt, 8, HEAD), high),
            pltpu.VMEM((depth, 2, rows, hid), low),
            pltpu.VMEM((depth, 2, rows, hid), low),
            pltpu.VMEM((nt, rows, wide), low),
            pltpu.VMEM((nt, rows, wide), low),
            pltpu.VMEM((2, segments, rows, seg), low),
            pltpu.VMEM((half // fine, rows, fine), low),
            pltpu.VMEM((half // fine, rows, fine), low),
            pltpu.VMEM((width // fine, rows, fine), low),
            pltpu.VMEM((n, rows, HEAD), high),
            pltpu.VMEM((HEAD, HEAD), high),
            pltpu.VMEM((2 * hid, half), low),
            pltpu.VMEM((half // fine, rows, fine), high),
            dma((16,)),
            dma((2, 3, depth)),
            dma((3, n)),
            dma((1,)),
            dma((pieces,)),
            dma((1,)),
            dma((pieces,)),
            dma((2, 2)),
            dma((2, 2)),
            dma((3 * depth + 1,)),
            dma((n + 1,)),
            dma((3,)),
            dma((nt,)),
            dma((2, 2, depth)),
            dma((pieces + 1, depth)),
            dma((3, 2)),
            dma((2, nt)),
            dma((depth,)),
            dma((depth,)),
            dma((nt,)),
            dma((nt,)),
            dma((segments,)),
            dma((segments,)),
            dma((1,)),
            dma((half // fine,)),
            dma((1,)),
            dma((4,)),
            dma((2, 2)),
        ],
        compiler_params=pltpu.CompilerParams(
            collective_id=0, has_side_effects=True, vmem_limit_bytes=60 << 20
        ),
        name="layer",
    )(
        q_first, q_second, k_first, k_second, values, head_lambda, w_out, stream_in,
        norm_gain.reshape(1, width), routes.T, route_w.T, w_gate[0], w_up[0], s_gate, s_up, w_down[0], s_down,
    )


def layer(*arrays):
    n, nt = lax.axis_size("sp"), lax.axis_size("tp")
    k_first, values, w_gate, w_down, s_down = (arrays[i] for i in (3, 5, 11, 13, 16))
    fits = (
        4 <= n <= 16
        and n % 2 == 0
        and nt == 4
        and k_first.shape[1] == HEAD
        and arrays[0].shape[0] <= HEAD
        and w_gate.shape[0] == 1
        and w_down.shape[1] % (16 * nt) == 0
        and s_down.shape[0] % (16 * n) == 0
        and w_down.shape[1] % HEAD == 0
        and (2 * w_down.shape[1]) % s_down.shape[0] == 0
        and (nt * s_down.shape[0]) % (2 * w_down.shape[1]) == 0
        and w_down.shape[2] % (16 * HEAD) == 0
    )
    return near(*arrays) if fits else local(*arrays)


def solution(mesh):
    return jax.shard_map(
        layer,
        mesh=mesh,
        in_specs=(
            P(("sp", "tp"), None),
            P("sp", "tp"),
            P("sp", "tp"),
            P("sp", "tp"),
            P("sp", "tp"),
            P("sp", "tp"),
            P("tp"),
            P("tp", None),
            P(),
            P(("sp", "tp"), None),
            P(("sp", "tp"), None),
            P("sp", None, None),
            P("sp", None, None),
            P("sp", None, None),
            P(None, "tp"),
            P(None, "tp"),
            P("tp", None),
        ),
        out_specs=P(("sp", "tp"), None),
        check_vma=False,
    )
```

```python
import functools
import math

import jax
import jax.numpy as jnp
from jax import lax
from jax.experimental import pallas as pl
from jax.experimental.pallas import tpu as pltpu
from jax.sharding import PartitionSpec as P

HEAD = 128


FLOOR = -1e30


def absorb(state, first_q, second_q, first_k, second_k, value_rows, query_pos, key_pos):
    allowed = key_pos[None, :] <= query_pos[:, None]
    scale = first_q.shape[-1] ** (-0.5)
    result = []
    pairs = ((first_q, first_k), (second_q, second_k))
    for index in range(2):
        query_rows, key_rows = pairs[index]
        peak, total, accum = (state[3 * index], state[3 * index + 1], state[3 * index + 2])
        scores = (
            jnp.einsum("qagd,kad->agqk", query_rows, key_rows, preferred_element_type=jnp.float32)
            * scale
        )
        scores = jnp.where(allowed, scores, FLOOR)
        raised = jnp.maximum(peak, scores.max(-1))
        weights = jnp.where(allowed, jnp.exp(scores - raised[..., None]), 0.0)
        fade = jnp.exp(peak - raised)
        total = total * fade + weights.sum(-1)
        accum = accum * fade[..., None] + jnp.einsum(
            "agqk,kad->agqd",
            weights.astype(jnp.bfloat16),
            value_rows,
            preferred_element_type=jnp.float32,
        )
        result += [raised, total, accum]
    return tuple(result)


def empty_state(kv_local, group, count, value_dim):
    peaks = jnp.full((kv_local, group, count), FLOOR, jnp.float32)
    sums = jnp.zeros((kv_local, group, count), jnp.float32)
    accums = jnp.zeros((kv_local, group, count, value_dim), jnp.float32)
    return (peaks, sums, accums, peaks, sums, accums)


def fold_rows(state, first_q, second_q, query_pos, last_row, pieces, start):
    first_k, second_k, value_rows = pieces
    length = first_k.shape[0]
    kv_local = first_q.shape[1]
    value_dim = value_rows.shape[1] // kv_local
    span = math.gcd(length, 2048)

    def sweep(current):

        def visit(block, inner):
            begin = block * span
            key_one = lax.dynamic_slice_in_dim(first_k, begin, span, 0).reshape(
                span, kv_local, HEAD
            )
            key_two = lax.dynamic_slice_in_dim(second_k, begin, span, 0).reshape(
                span, kv_local, HEAD
            )
            value_part = lax.dynamic_slice_in_dim(value_rows, begin, span, 0).reshape(
                span, kv_local, value_dim
            )
            key_pos = begin + jnp.arange(span, dtype=jnp.int32)
            return absorb(
                inner, first_q, second_q, key_one, key_two, value_part, query_pos, key_pos
            )

        return lax.fori_loop(0, length // span, visit, current)

    def unchanged(current):
        return current

    return lax.cond(start <= last_row, sweep, unchanged, state)


def finish_heads(final, head_lambda):
    kv_local, group, count, value_dim = final[2].shape
    weight = head_lambda.reshape(kv_local, group, 1, 1)
    head_out = final[2] / final[1][..., None] - weight * final[5] / final[4][..., None]
    head_out = head_out * lax.rsqrt(jnp.mean(head_out * head_out, axis=-1, keepdims=True) + 1e-05)
    return (
        head_out.transpose(2, 0, 1, 3)
        .reshape(count, kv_local * group * value_dim)
        .astype(jnp.bfloat16)
    )


def shared_part(normed, s_gate, s_up, s_down):
    piece = lax.all_gather(normed, "tp", axis=0, tiled=True)
    gate_part = jnp.dot(piece, s_gate, preferred_element_type=jnp.float32)
    up_part = jnp.dot(piece, s_up, preferred_element_type=jnp.float32)
    hidden = (jax.nn.silu(gate_part) * up_part).astype(jnp.bfloat16)
    terms = jnp.dot(hidden, s_down, preferred_element_type=jnp.float32)
    return lax.psum_scatter(
        terms.astype(jnp.bfloat16), "tp", scatter_dimension=0, tiled=True
    ).astype(jnp.float32)


def routed_part(normed, routes, route_w, w_gate, w_up, w_down):
    rows, topk = routes.shape
    local_experts = w_gate.shape[0]
    experts = local_experts * lax.axis_size("sp")
    slots = max(2, 3 * rows * topk // (2 * experts))
    flat_ids = routes.reshape(-1)
    hits = (flat_ids[:, None] == jnp.arange(experts, dtype=jnp.int32)[None, :]).astype(jnp.int32)
    slot_of = jnp.sum(jnp.cumsum(hits, axis=0) * hits, axis=1) - 1
    target = flat_ids * slots + slot_of
    placing = jnp.any(
        jnp.arange(experts * slots, dtype=jnp.int32)[:, None, None]
        == target.reshape(rows, topk)[None, :, :],
        axis=-1,
    ).astype(jnp.bfloat16)
    outgoing = (
        jnp.dot(placing, normed, preferred_element_type=jnp.float32)
        .astype(jnp.bfloat16)
        .reshape(experts, slots, normed.shape[1])
    )
    arrived = lax.all_to_all(outgoing, "sp", split_axis=0, concat_axis=0, tiled=True)
    sources = arrived.shape[0] // local_experts
    grouped = arrived.reshape(sources, local_experts, arrived.shape[1], arrived.shape[2])
    gate_part = jnp.einsum("sjcd,jdf->sjcf", grouped, w_gate, preferred_element_type=jnp.float32)
    up_part = jnp.einsum("sjcd,jdf->sjcf", grouped, w_up, preferred_element_type=jnp.float32)
    hidden = (jax.nn.silu(gate_part) * up_part).astype(jnp.bfloat16)
    result = jnp.einsum(
        "sjcf,jfd->sjcd", hidden, w_down, preferred_element_type=jnp.float32
    ).astype(jnp.bfloat16)
    returned = lax.all_to_all(
        result.reshape(arrived.shape), "sp", split_axis=0, concat_axis=0, tiled=True
    )
    picked = (
        returned.reshape(experts * slots, normed.shape[1])[target]
        .reshape(rows, topk, normed.shape[1])
        .astype(jnp.float32)
    )
    return jnp.sum(picked * route_w[..., None], axis=1)


def local(
    stream_in,
    q_first,
    q_second,
    k_first,
    k_second,
    values,
    head_lambda,
    w_out,
    norm_gain,
    routes,
    route_w,
    w_gate,
    w_up,
    w_down,
    s_gate,
    s_up,
    s_down,
):
    seq_rows = q_first.shape[0]
    kv_local = k_first.shape[1] // HEAD
    heads_local = q_first.shape[1] // HEAD
    group = heads_local // kv_local
    value_dim = values.shape[1] // kv_local
    offset = lax.axis_index("sp") * seq_rows
    query_pos = offset + jnp.arange(seq_rows, dtype=jnp.int32)
    last_row = offset + seq_rows - 1
    first_q = q_first.reshape(seq_rows, kv_local, group, HEAD)
    second_q = q_second.reshape(seq_rows, kv_local, group, HEAD)
    start_state = empty_state(kv_local, group, seq_rows, value_dim)
    folded_state = fold_rows(
        start_state,
        first_q,
        second_q,
        query_pos,
        last_row,
        (
            lax.all_gather(k_first, "sp", axis=0, tiled=True),
            lax.all_gather(k_second, "sp", axis=0, tiled=True),
            lax.all_gather(values, "sp", axis=0, tiled=True),
        ),
        jnp.int32(0),
    )
    attn_rows = finish_heads(folded_state, head_lambda)
    attn = lax.psum_scatter(
        jnp.dot(attn_rows, w_out, preferred_element_type=jnp.float32).astype(jnp.bfloat16),
        "tp",
        scatter_dimension=0,
        tiled=True,
    ).astype(jnp.float32)
    resid = (stream_in.astype(jnp.float32) + attn).astype(jnp.bfloat16)
    stream = lax.optimization_barrier(resid).astype(jnp.float32)
    normed = (
        stream * lax.rsqrt(jnp.mean(stream * stream, axis=-1, keepdims=True) + 1e-06) * norm_gain
    ).astype(jnp.bfloat16)
    routed = routed_part(normed, routes, route_w, w_gate, w_up, w_down)
    shared = shared_part(normed, s_gate, s_up, s_down)
    return (stream + routed + shared).astype(jnp.bfloat16)


def mesh_copy(src, dst, send_sem, recv_sem, axis, target):
    return pltpu.make_async_remote_copy(
        src_ref=src,
        dst_ref=dst,
        send_sem=send_sem,
        recv_sem=recv_sem,
        device_id={axis: target},
        device_id_type=pl.DeviceIdType.MESH,
    )


def greet(axis, target):
    pl.semaphore_signal(
        pltpu.get_barrier_semaphore(),
        inc=1,
        device_id={axis: target},
        device_id_type=pl.DeviceIdType.MESH,
    )


def near_kernel(
    n, nt, group, pieces,
    q_one_h, q_two_h, k_one_h, k_two_h, val_h, lam, w_out_h, stream_h, gain_h, route_h, share_h,
    gate_h, up_h, s_gate_h, s_up_h, down_h, s_down_h,
    out,
    q_one, q_two, k_own, val, stream, gain, route_t, share_t,
    stacked, keys, vals, peak, total, accum, rows_in,
    w, order, out_one, in_one, out_two, in_two, resid,
    gates, ups, s_gate, s_up, wall, gathered, beside, stat, stat_b,
    out_hid, in_hid, out_sh, in_sh, units, out_fin, in_fin, result, mix, square, extra, partial,
    load, send_kv, recv_kv, send_one, recv_one, send_two, recv_two,
    send_g, recv_g, send_d, recv_d, send_sd, recv_sd,
    send_x, recv_x, send_b, recv_b, send_h, recv_h, send_s, recv_s,
    send_u, recv_u, send_f, recv_f, save, send_e, recv_e,
):
    me, mine = lax.axis_index("sp"), lax.axis_index("tp")
    place, side = me // 2, me % 2
    far, core = mine // 2, mine % 2
    depth = n // 2
    pair, partner, across = me + 1 - 2 * side, mine + 1 - 2 * core, 2 * (1 - far) + core
    above, below = place < depth - 1, place > 0
    seq = q_one.shape[0]
    rows, width = stream.shape
    hid, wide = down_h.shape[0], s_down_h.shape[0]
    scale = HEAD ** (-0.5)
    half = width // 2

    def column(o):
        return 2 * ((place + o) % depth) + side

    def cols_of(f):
        return pl.ds(pl.multiple_of(f * half, half), half)

    loads = [
        pltpu.make_async_copy(source, target, load.at[i])
        for i, (source, target) in enumerate(
            (
                (w_out_h, w),
                (gate_h, gates.at[0]),
                (up_h, ups.at[0]),
                (s_gate_h, s_gate),
                (s_up_h, s_up),
                (
                    down_h.at[:, cols_of(far)],
                    wall.at[pl.ds(pl.multiple_of(me * hid, hid), hid)],
                ),
                (
                    s_down_h.at[:, cols_of(far)],
                    wall.at[pl.ds(pl.multiple_of(n * hid + mine * wide, wide), wide)],
                ),
            )
        )
    ]
    for o in range(1, depth):
        greet("sp", column(o))
    greet("sp", pair)
    greet("tp", across)
    greet("tp", partner)
    inputs = [
        pltpu.make_async_copy(source, target, load.at[7 + i])
        for i, (source, target) in enumerate(
            (
                (k_one_h, k_own.at[0]),
                (k_two_h, k_own.at[1]),
                (val_h, val),
                (q_one_h, q_one),
                (q_two_h, q_two),
                (stream_h, stream),
                (gain_h, gain),
                (route_h, route_t),
                (share_h, share_t),
            )
        )
    ]
    for one in inputs:
        one.start()
    for one in inputs[:3]:
        one.wait()
    pl.semaphore_wait(pltpu.get_barrier_semaphore(), depth + 2)

    mid = seq // 2

    def stuff(block):
        return keys.at[block], vals.at[block, :mid], vals.at[block, mid:]

    def copies(block, way, target, own):
        return [
            mesh_copy(
                (k_own, val.at[:mid], val.at[mid:])[a] if own else stuff(block)[a],
                stuff(block)[a],
                send_kv.at[way, a, block // 2],
                recv_kv.at[a, block],
                "sp",
                target,
            )
            for a in range(3)
        ]

    def start(block, way, target, own=False):
        for one in copies(block, way, target, own):
            one.start()

    def arrive(block):
        for one in copies(block, 0, pair, False):
            one.wait_recv()

    share = width // 2
    share_at = pl.ds(pl.multiple_of(core * share, share), share)
    other_at = pl.ds(pl.multiple_of((1 - core) * share, share), share)

    def pair_weights():
        return [
            mesh_copy(
                h.at[share_at], v.at[1, share_at], send_g.at[0, i], recv_g.at[0, i], "sp", pair
            )
            for i, (h, v) in enumerate(((gate_h, gates), (up_h, ups)))
        ]

    def pair_weights_on(at):
        return [
            mesh_copy(
                v.at[1, at], v.at[1, at], send_g.at[1, i], recv_g.at[1, i], "tp", partner
            )
            for i, v in enumerate((gates, ups))
        ]

    part = hid // 2

    def down_at(block, c):
        return wall.at[pl.ds(pl.multiple_of(block * hid + c * part, part), part)]

    def down_own(way, target):
        return mesh_copy(
            down_h.at[pl.ds(pl.multiple_of(core * part, part), part), cols_of(far)],
            down_at(me, core),
            send_d.at[way],
            recv_d.at[me],
            "sp",
            target,
        )

    def down_pair(block):
        return mesh_copy(
            down_at(block, core),
            down_at(block, core),
            send_d.at[depth + block // 2],
            recv_d.at[block],
            "sp",
            pair,
        )

    def down_core(block, c):
        return mesh_copy(
            down_at(block, c),
            down_at(block, c),
            send_d.at[3 * depth],
            recv_d.at[n],
            "tp",
            partner,
        )

    def extra_at(s, c):
        return extra.at[pl.ds(pl.multiple_of(s * hid + c * part, part), part)]

    def extra_own():
        return mesh_copy(
            down_h.at[pl.ds(pl.multiple_of(core * part, part), part), cols_of(1 - far)],
            extra_at(side, core),
            send_e.at[0],
            recv_e.at[0, side],
            "sp",
            side,
        )

    def extra_pair(s):
        return mesh_copy(
            extra_at(s, core), extra_at(s, core), send_e.at[1], recv_e.at[0, s], "sp", pair
        )

    def extra_core(s, c):
        return mesh_copy(
            extra_at(s, c), extra_at(s, c), send_e.at[2 + s], recv_e.at[1, s], "tp", partner
        )

    def sd_at(u):
        return wall.at[pl.ds(pl.multiple_of(n * hid + u * wide, wide), wide)]

    def sd_own(way, f, target):
        return mesh_copy(
            s_down_h.at[:, cols_of(f)], sd_at(mine), send_sd.at[way], recv_sd.at[mine], "tp", target
        )

    def sd_on(u):
        return mesh_copy(sd_at(u), sd_at(u), send_sd.at[2], recv_sd.at[u], "tp", partner)

    @pl.when(above)
    def _():
        start(me, 0, me + 2, True)

    @pl.when(side == 0)
    def _():
        start(me, 1, pair, True)

    for one in loads:
        one.start()
    late = place >= depth // 2

    @pl.when(late)
    def _():
        sd_own(1, 1 - far, across).start()

    sd_own(0, far, partner).start()
    for o in range(1, depth):

        @pl.when(place + o >= depth)
        def _():
            down_own(o, column(o)).start()

    top_place = place == depth - 1
    pl.when(top_place)(lambda: extra_own().start())

    for one in inputs[3:]:
        one.wait()
    for index, q in enumerate((q_one, q_two)):
        for h in range(group):
            stacked[index, h * seq : (h + 1) * seq, :] = q[:, h * HEAD : (h + 1) * HEAD]

    def scores_of(index, some):
        return (
            lax.dot_general(
                stacked[index], some, (((1,), (1,)), ((), ())), preferred_element_type=jnp.float32
            )
            * scale
        )

    spread = (group * seq, seq)
    row_of = lax.broadcasted_iota(jnp.int32, spread, 0) % seq
    allowed = lax.broadcasted_iota(jnp.int32, spread, 1) <= row_of
    for index in range(2):
        scores = jnp.where(allowed, scores_of(index, k_own[index]), FLOOR)
        top = jnp.max(scores, axis=-1, keepdims=True)
        weights = jnp.exp(scores - top)
        peak[index] = top
        total[index] = jnp.sum(weights, axis=-1, keepdims=True)
        accum[index] = jnp.dot(
            weights.astype(jnp.bfloat16), val[...], preferred_element_type=jnp.float32
        )

    def fold(block):
        for index in range(2):
            scores = scores_of(index, keys[block, index])
            old = peak[index]
            top = jnp.maximum(old, jnp.max(scores, axis=-1, keepdims=True))
            weights = jnp.exp(scores - top)
            fade = jnp.exp(old - top)
            peak[index] = top
            total[index] = total[index] * fade + jnp.sum(weights, axis=-1, keepdims=True)
            accum[index] = accum[index] * fade + jnp.dot(
                weights.astype(jnp.bfloat16), vals[block], preferred_element_type=jnp.float32
            )

    def down_up(block):
        return mesh_copy(
            down_at(block, core),
            down_at(block, core),
            send_d.at[2 * depth + block // 2],
            recv_d.at[block],
            "sp",
            me + 2,
        )

    def lift(d):
        @pl.when((place >= d) & above)
        def _():
            down_up(me - 2 * d).wait_recv()
            down_up(me - 2 * d).start()

    def weights_out():
        pl.when(above)(lambda: down_own(1, me + 2).start())
        for one in pair_weights():
            one.start()
        down_own(0, pair).start()
        lift(1)

    pl.when(place == 0)(weights_out)

    def visit(e, carry):
        @pl.when(place >= e)
        def _():
            block = me - 2 * e
            for up, over in zip(copies(block, 0, me + 2, False), copies(block, 1, pair, False)):
                over.wait_recv()
                pl.when(above)(up.start)
                over.start()
            pl.when(e == place)(weights_out)
            fold(block)

        @pl.when((place >= e - 1) & ((e > 1) | (side == 1)))
        def _():
            block = pair - 2 * (e - 1)
            arrive(block)
            fold(block)

        return carry

    lax.fori_loop(1, depth + 1, visit, 0)

    for d in range(2, depth):
        lift(d)

    for h in range(group):
        cut = slice(h * seq, (h + 1) * seq)
        head = accum[0, cut, :] / total[0, cut, :] - lam[h] * (
            accum[1, cut, :] / total[1, cut, :]
        )
        head = head * lax.rsqrt(jnp.mean(head * head, axis=-1, keepdims=True) + 1e-05)
        size = head.shape[1]
        rows_in[:, h * size : (h + 1) * size] = head.astype(jnp.bfloat16)

    for o in range(2):
        base = 2 * ((far + o) % 2)
        for which, parity in enumerate((1 - core, core)):
            begin = pl.multiple_of((base + parity) * rows, rows)
            order[which, o * rows : (o + 1) * rows, :] = rows_in[pl.ds(begin, rows), :]

    first = [
        mesh_copy(out_one.at[i], in_one.at[i], send_one.at[0], recv_one.at[i], "tp", partner)
        for i in range(pieces)
    ]
    second = [
        mesh_copy(out_two.at[i], in_two.at[i], send_two.at[0], recv_two.at[i], "tp", across)
        for i in range(pieces)
    ]
    span = width // pieces
    loads[0].wait()
    for i in range(pieces):
        out_one[i] = jnp.dot(
            order[0], w[:, i * span : (i + 1) * span], preferred_element_type=jnp.float32
        ).astype(jnp.bfloat16)
        first[i].start()
    kept = []
    for i in range(pieces):
        sums = jnp.dot(
            order[1], w[:, i * span : (i + 1) * span], preferred_element_type=jnp.float32
        )
        first[i].wait_recv()
        sums = sums + in_one[i].astype(jnp.float32)
        out_two[i] = sums[rows:].astype(jnp.bfloat16)
        second[i].start()
        kept.append(sums[:rows])

    @pl.when(jnp.logical_not(late))
    def _():
        sd_own(1, 1 - far, across).start()

    def row_part(block, extra, spot, i):
        return block.at[spot, i] if i < pieces else extra.at[spot]

    def row_copy(spot, way, target, i):
        some = row_part(gathered, stat, spot, i)
        return mesh_copy(
            some,
            some,
            send_x.at[way, i // pieces, spot],
            recv_x.at[i, spot],
            "sp",
            target,
        )

    def rows_sent(spot, way):
        for some, kind in ((gathered.at[spot], 0), (stat.at[spot], 1)):
            mesh_copy(
                some, some, send_x.at[way, kind, spot], recv_x.at[0, spot], "sp", pair
            ).wait_send()

    def beside_own(way, target, i):
        return mesh_copy(
            row_part(gathered, stat, place, i),
            row_part(beside, stat_b, mine, i),
            send_b.at[way, i // pieces],
            recv_b.at[i // pieces, mine],
            "tp",
            target,
        )

    def beside_on(u, kind, way=2):
        some = (beside, stat_b)[kind].at[u]
        return mesh_copy(some, some, send_b.at[way, kind], recv_b.at[kind, u], "tp", partner)

    def raise_row(e, i):
        row_copy(place - e, 0, pair, i).wait_recv()
        row_copy(place - e, 0, me + 2, i).start()

    def lower_row(e, i):
        row_copy(place + e, 0, pair, i).wait_recv()
        row_copy(place + e, 1, me - 2, i).start()

    def rows_out(i):
        pl.when(above)(lambda: row_copy(place, 0, me + 2, i).start())
        pl.when(below)(lambda: row_copy(place, 1, me - 2, i).start())
        beside_own(1, across, i).start()
        beside_own(0, partner, i).start()

    fine = resid.shape[2]
    per = span // fine
    squares = jnp.zeros((rows, 1), jnp.float32)
    for i in range(pieces):
        cut = slice(i * span, (i + 1) * span)
        second[i].wait_recv()
        sums = kept[i] + in_two[i].astype(jnp.float32)
        sums = (stream[:, cut].astype(jnp.float32) + sums).astype(jnp.bfloat16)
        for j in range(per):
            resid[i * per + j] = sums[:, j * fine : (j + 1) * fine]
        sums = sums.astype(jnp.float32)
        squares = squares + jnp.sum(sums * sums, axis=-1, keepdims=True)
        gathered[place, i] = (sums * gain[:, cut]).astype(jnp.bfloat16)
        rows_out(i)
    shrink = lax.rsqrt(squares / width + 1e-06)
    square[0:rows, :] = jnp.broadcast_to(shrink, (rows, HEAD))
    stat[place] = square[...].T[0 : stat.shape[1], :]
    rows_out(pieces)
    ahead = pieces // 4
    for e in range(1, depth - 1):
        for i in range(pieces + 1 if e == 1 else ahead):
            pl.when(above & (place >= e))(lambda: raise_row(e, i))
        if e == 1:
            for i in range(pieces + 1):
                pl.when(above & below)(lambda: lower_row(1, i))
    def pass_down(e):
        def one(block, fresh):
            pl.when(fresh)(lambda: down_pair(block).wait_recv())
            down_pair(block).start()
            down_core(block, core).start()

        pl.when(place >= e)(lambda: one(me - 2 * e, jnp.logical_not(above)))
        pl.when(place + e < depth)(lambda: one(me + 2 * e, place >= 0))

    def collect(e):
        def one(block):
            down_pair(block).wait_recv()
            down_core(block, core).start()

        pl.when(place >= e)(lambda: one(pair - 2 * e))
        pl.when(place + e < depth)(lambda: one(pair + 2 * e))

    def factors(scales, spot):
        square[0 : scales.shape[1], :] = scales[spot]
        return square[...].T[0:rows, :1]

    def hidden_of(block, spot, factor, g, u):
        def project(m):
            parts = [
                jnp.dot(
                    block[spot, i],
                    m[i * span : (i + 1) * span, :],
                    preferred_element_type=jnp.float32,
                )
                for i in range(pieces)
            ]
            return sum(parts[1:], parts[0]) * factor

        gate_part, up_part = project(g), project(u)
        return (gate_part / (1.0 + jnp.exp(-gate_part)) * up_part).astype(jnp.bfloat16)

    for one, onward in zip(pair_weights(), pair_weights_on(share_at)):
        one.wait_recv()
        onward.start()
    for d in range(1, depth):
        pass_down(d)
    for e in range(2, depth - 1):
        for i in range(ahead):
            pl.when(below & (place + e < depth))(lambda: lower_row(e, i))

    square[...] = jnp.zeros_like(square)
    for j in range(n):
        chosen = jnp.where(route_t[...] == j, share_t[...], 0.0)
        square[j : j + 1, 0:rows] = jnp.sum(chosen, axis=0, keepdims=True)
    turned = square[...].T
    for j in range(n):
        mix[j] = jnp.broadcast_to(turned[0:rows, j : j + 1], mix.shape[1:])
    for i in range(1, 5):
        loads[i].wait()

    def hid_copy(spot):
        return mesh_copy(
            out_hid.at[spot], in_hid.at[place], send_h.at[spot], recv_h.at[place], "sp",
            2 * spot + side,
        )

    def serve(spot):
        factor = factors(stat, spot)
        out_hid[spot, side] = hidden_of(gathered, spot, factor, gates.at[0], ups.at[0])
        out_hid[spot, 1 - side] = hidden_of(gathered, spot, factor, gates.at[1], ups.at[1])
        hid_copy(spot).start()

    def serve_last(spot):
        sums = None
        mats = (gates.at[0], ups.at[0], gates.at[1], ups.at[1])
        for i in range(pieces):
            row_copy(spot, 0, pair, i).wait_recv()
            parts = [
                jnp.dot(
                    gathered[spot, i],
                    m[i * span : (i + 1) * span, :],
                    preferred_element_type=jnp.float32,
                )
                for m in mats
            ]
            sums = parts if sums is None else [a + b for a, b in zip(sums, parts)]
        row_copy(spot, 0, pair, pieces).wait_recv()
        factor = factors(stat, spot)
        g_one, u_one, g_two, u_two = [v * factor for v in sums]
        for which, g, u in ((side, g_one, u_one), (1 - side, g_two, u_two)):
            out_hid[spot, which] = (g / (1.0 + jnp.exp(-g)) * u).astype(jnp.bfloat16)
        hid_copy(spot).start()

    def sh_copy(u):
        return mesh_copy(
            out_sh.at[u], in_sh.at[mine], send_s.at[u], recv_s.at[mine], "tp", u
        )

    def answer(u):
        out_sh[u] = hidden_of(beside, u, factors(stat_b, u), s_gate, s_up)
        sh_copy(u).start()

    def turn(e, carry):
        low, high = place >= e, place + e < depth

        @pl.when(low & jnp.logical_not(above))
        def _():
            for i in range(pieces + 1):
                row_copy(place - e, 0, pair, i).wait_recv()

        @pl.when(high & jnp.logical_not(below))
        def _():
            for i in range(pieces + 1):
                row_copy(place + e, 0, pair, i).wait_recv()

        @pl.when(e == 1)
        def _():
            factor = factors(stat, place)
            in_sh[mine] = hidden_of(gathered, place, factor, s_gate, s_up)
            in_hid[place, side] = hidden_of(gathered, place, factor, gates.at[0], ups.at[0])
            for one in pair_weights_on(other_at):
                one.wait_recv()

        @pl.when(low)
        def _():
            serve(place - e)

        @pl.when(high)
        def _():
            serve(place + e)

        @pl.when(e == 1)
        def _():
            for d in range(2, depth - 1):
                for i in range(ahead, pieces + 1):
                    pl.when(above & (place >= d))(lambda: raise_row(d, i))
                    pl.when(below & (place + d < depth))(lambda: lower_row(d, i))

        @pl.when(e == 2)
        def _():
            down_pair(pair).wait_recv()
            down_core(pair, core).start()
            in_hid[place, 1 - side] = hidden_of(
                gathered, place, factors(stat, place), gates.at[1], ups.at[1]
            )
            u = across
            for kind in range(2):
                beside_on(u, kind).wait_recv()
                beside_on(u, kind).start()
            answer(u)
            sd_on(u).wait_recv()
            sd_on(u).start()
            for o in range(2):
                u = 2 * ((far + o) % 2) + 1 - core
                for kind in range(2):
                    beside_on(u, kind).wait_recv()
                answer(u)

        return carry

    @pl.when(place == 0)
    def _():
        extra_pair(side).wait_recv()
        extra_pair(side).start()
        extra_core(side, core).start()

    lax.fori_loop(1, depth - 1, turn, 0)
    last = depth - 1

    @pl.when(place == 0)
    def _():
        serve_last(last)

    segments = units.shape[1]

    def unit_copy(s):
        return mesh_copy(
            units.at[0, s], units.at[1, s], send_u.at[s], recv_u.at[s], "tp", across
        )

    seg = units.shape[3]

    def share_units():
        for o in range(1, nt):
            u = (mine + o) % nt
            mesh_copy(
                out_sh.at[u], in_sh.at[u], send_s.at[u], recv_s.at[u], "tp", u
            ).wait_recv()
        for j in range(nt):
            at = j * wide
            units[0, depth + at // seg, :, at % seg : at % seg + wide] = in_sh[j]
        for s in range(depth, segments):
            unit_copy(s).start()

    pl.when(top_place)(share_units)

    def place_unit(spot):
        @pl.when(place != spot)
        def _():
            mesh_copy(
                out_hid.at[spot], in_hid.at[spot], send_h.at[spot], recv_h.at[spot], "sp",
                2 * spot + side,
            ).wait_recv()

        for k in range(2):
            j = 2 * spot + k
            units[0, spot, :, k * hid : (k + 1) * hid] = (
                in_hid[spot, k].astype(jnp.float32) * mix[j][:, :1]
            ).astype(jnp.bfloat16)

    @pl.when(place != 0)
    def _():
        place_unit(last)
        unit_copy(last).start()

    for spot in range(last - 1, -1, -1):
        place_unit(spot)
        unit_copy(spot).start()

    pl.when(jnp.logical_not(top_place))(share_units)
    for e in range(1, depth - 1):
        collect(e)

    collect(last)

    @pl.when(top_place)
    def _():
        serve_last(0)

    @pl.when(place == 0)
    def _():
        extra_pair(1 - side).wait_recv()
        extra_core(1 - side, core).start()


    loads[5].wait()
    loads[6].wait()
    for o in range(2):
        sd_on(2 * ((far + o) % 2) + 1 - core).wait_recv()

    taken = wall.at[pl.ds(0, (n - 1) * part)]
    cores = mesh_copy(taken, taken, send_d.at[3 * depth], recv_d.at[n], "tp", partner)
    cores.wait_recv()
    early = [s for s in range(segments) if s != last]
    for s in early:
        unit_copy(s).wait_recv()
    pl.when(place != 0)(lambda: unit_copy(last).wait_recv())

    def fin_copy(i):
        return mesh_copy(out_fin.at[i], in_fin.at[i], send_f.at[0], recv_f.at[i], "tp", across)

    def put(spot):
        return pltpu.make_async_copy(
            result.at[spot],
            out.at[:, pl.ds(pl.multiple_of(spot * fine, fine), fine)],
            save.at[0],
        )

    def close(spot, terms):
        result[spot] = (resid[spot].astype(jnp.float32) + terms).astype(jnp.bfloat16)
        put(spot).start()

    count = half // fine
    mine_at, other_of = far * count, (1 - far) * count
    for i in range(count):
        cut = slice(i * fine, (i + 1) * fine)
        terms = [
            jnp.dot(
                units[:, s].reshape(2 * rows, seg),
                wall[s * seg : (s + 1) * seg, cut],
                preferred_element_type=jnp.float32,
            )
            for s in early
        ]
        both = sum(terms[1:], terms[0])

        @pl.when(place == 0)
        def _():
            partial[i] = both[:rows]
            out_fin[i] = both[rows:].astype(jnp.bfloat16)
            fin_copy(i).start()

        @pl.when(place != 0)
        def _():
            full = both + jnp.dot(
                units[:, last].reshape(2 * rows, seg),
                wall[last * seg : (last + 1) * seg, cut],
                preferred_element_type=jnp.float32,
            )
            out_fin[i] = full[rows:].astype(jnp.bfloat16)
            fin_copy(i).start()
            close(mine_at + i, full[:rows])

    @pl.when(place == 0)
    def _():
        extra_core(0, 1 - core).wait_recv()
        extra_core(1, 1 - core).wait_recv()
        for i in range(count):
            fin_copy(i).wait_recv()
        place_unit(last)
        rest = units[0, last]
        for i in range(count):
            cut = slice(i * fine, (i + 1) * fine)
            terms = jnp.dot(
                rest, wall[last * seg : (last + 1) * seg, cut], preferred_element_type=jnp.float32
            )
            close(mine_at + i, partial[i] + terms)
            terms = jnp.dot(rest, extra[:, cut], preferred_element_type=jnp.float32)
            close(other_of + i, in_fin[i].astype(jnp.float32) + terms)

    @pl.when(place != 0)
    def _():
        for i in range(count):
            fin_copy(i).wait_recv()
            close(other_of + i, in_fin[i].astype(jnp.float32))

    def settle(e, carry):
        @pl.when(place >= e)
        def _():
            block = me - 2 * e

            @pl.when(above)
            def _():
                for one in copies(block, 0, me + 2, False):
                    one.wait_send()

                @pl.when(e > 0)
                def _():
                    down_up(block).wait_send()

            @pl.when((e > 0) | (side == 0))
            def _():
                for one in copies(block, 1, pair, False):
                    one.wait_send()

        pl.when((place + e < depth) & below)(lambda: rows_sent(place + e, 1))
        pl.when((place >= e) & above)(lambda: rows_sent(place - e, 0))

        @pl.when(e != place)
        def _():
            hid_copy(e).wait_send()
            down_pair(2 * e + side).wait_send()

        return carry

    lax.fori_loop(0, depth, settle, 0)

    cores.wait_send()
    for one in pair_weights() + pair_weights_on(share_at):
        one.wait_send()
    for some, sem, rec in (
        (out_one, send_one.at[0], recv_one.at[0]),
        (out_two, send_two.at[0], recv_two.at[0]),
        (out_fin, send_f.at[0], recv_f.at[0]),
    ):
        mesh_copy(some, some, sem, rec, "tp", partner).wait_send()
    for o in range(1, depth):
        pl.when((place + o >= depth) | (o == 1))(lambda: down_own(o, column(o)).wait_send())
    down_own(0, pair).wait_send()
    sd_own(0, far, partner).wait_send()
    sd_own(1, 1 - far, across).wait_send()
    sd_on(across).wait_send()
    for kind in range(2):
        for way in range(3):
            beside_on(across, kind, way).wait_send()
    for o in range(1, nt):
        sh_copy((mine + o) % nt).wait_send()
    for s in early:
        unit_copy(s).wait_send()
    pl.when(place != 0)(lambda: unit_copy(last).wait_send())
    pl.when(top_place)(lambda: extra_own().wait_send())

    @pl.when(place == 0)
    def _():
        extra_pair(side).wait_send()
        extra_core(0, core).wait_send()
        extra_core(1, core).wait_send()

    pltpu.make_async_copy(stream_h, stream, save.at[0]).wait()


def near(
    stream_in,
    q_first,
    q_second,
    k_first,
    k_second,
    values,
    head_lambda,
    w_out,
    norm_gain,
    routes,
    route_w,
    w_gate,
    w_up,
    w_down,
    s_gate,
    s_up,
    s_down,
):
    n, nt = lax.axis_size("sp"), lax.axis_size("tp")
    depth = n // 2
    seq, rows, width = q_first.shape[0], stream_in.shape[0], stream_in.shape[1]
    group, value_dim = q_first.shape[1] // HEAD, values.shape[1]
    hid, wide = w_down.shape[1], s_down.shape[0]
    tall, features = group * seq, group * value_dim
    pieces = 8
    span = width // pieces
    half, fine = width // 2, width // 8
    seg = 2 * hid
    segments = depth + nt * wide // seg
    topk = routes.shape[1]
    smem = pl.BlockSpec(memory_space=pltpu.SMEM)
    hbm = pl.BlockSpec(memory_space=pl.ANY)
    low, high = jnp.bfloat16, jnp.float32
    dma = pltpu.SemaphoreType.DMA
    return pl.pallas_call(
        functools.partial(near_kernel, n, nt, group, pieces),
        out_shape=jax.ShapeDtypeStruct((rows, width), low),
        in_specs=[hbm] * 5 + [smem] + [hbm] * 11,
        out_specs=hbm,
        scratch_shapes=[
            pltpu.VMEM((seq, group * HEAD), low),
            pltpu.VMEM((seq, group * HEAD), low),
            pltpu.VMEM((2, seq, HEAD), low),
            pltpu.VMEM((seq, value_dim), low),
            pltpu.VMEM((rows, width), low),
            pltpu.VMEM((1, width), high),
            pltpu.VMEM((topk, rows), jnp.int32),
            pltpu.VMEM((topk, rows), high),
            pltpu.VMEM((2, tall, HEAD), low),
            pltpu.VMEM((n, 2, seq, HEAD), low),
            pltpu.VMEM((n, seq, value_dim), low),
            pltpu.VMEM((2, tall, 1), high),
            pltpu.VMEM((2, tall, 1), high),
            pltpu.VMEM((2, tall, value_dim), high),
            pltpu.VMEM((seq, features), low),
            pltpu.VMEM((features, width), low),
            pltpu.VMEM((2, 2 * rows, features), low),
            pltpu.VMEM((pieces, 2 * rows, span), low),
            pltpu.VMEM((pieces, 2 * rows, span), low),
            pltpu.VMEM((pieces, rows, span), low),
            pltpu.VMEM((pieces, rows, span), low),
            pltpu.VMEM((width // fine, rows, fine), low),
            pltpu.VMEM((2, width, hid), low),
            pltpu.VMEM((2, width, hid), low),
            pltpu.VMEM((width, wide), low),
            pltpu.VMEM((width, wide), low),
            pltpu.VMEM((n * hid + nt * wide, half), low),
            pltpu.VMEM((depth, pieces, rows, span), low),
            pltpu.VMEM((nt, pieces, rows, span), low),
            pltpu.VMEM((depth, 8, HEAD), high),
            pltpu.VMEM((nt, 8, HEAD), high),
            pltpu.VMEM((depth, 2, rows, hid), low),
            pltpu.VMEM((depth, 2, rows, hid), low),
            pltpu.VMEM((nt, rows, wide), low),
            pltpu.VMEM((nt, rows, wide), low),
            pltpu.VMEM((2, segments, rows, seg), low),
            pltpu.VMEM((half // fine, rows, fine), low),
            pltpu.VMEM((half // fine, rows, fine), low),
            pltpu.VMEM((width // fine, rows, fine), low),
            pltpu.VMEM((n, rows, HEAD), high),
            pltpu.VMEM((HEAD, HEAD), high),
            pltpu.VMEM((2 * hid, half), low),
            pltpu.VMEM((half // fine, rows, fine), high),
            dma((16,)),
            dma((2, 3, depth)),
            dma((3, n)),
            dma((1,)),
            dma((pieces,)),
            dma((1,)),
            dma((pieces,)),
            dma((2, 2)),
            dma((2, 2)),
            dma((3 * depth + 1,)),
            dma((n + 1,)),
            dma((3,)),
            dma((nt,)),
            dma((2, 2, depth)),
            dma((pieces + 1, depth)),
            dma((3, 2)),
            dma((2, nt)),
            dma((depth,)),
            dma((depth,)),
            dma((nt,)),
            dma((nt,)),
            dma((segments,)),
            dma((segments,)),
            dma((1,)),
            dma((half // fine,)),
            dma((1,)),
            dma((4,)),
            dma((2, 2)),
        ],
        compiler_params=pltpu.CompilerParams(
            collective_id=0, has_side_effects=True, vmem_limit_bytes=60 << 20
        ),
        name="layer",
    )(
        q_first, q_second, k_first, k_second, values, head_lambda, w_out, stream_in,
        norm_gain.reshape(1, width), routes.T, route_w.T, w_gate[0], w_up[0], s_gate, s_up, w_down[0], s_down,
    )


def layer(*arrays):
    n, nt = lax.axis_size("sp"), lax.axis_size("tp")
    k_first, values, w_gate, w_down, s_down = (arrays[i] for i in (3, 5, 11, 13, 16))
    fits = (
        4 <= n <= 16
        and n % 2 == 0
        and nt == 4
        and k_first.shape[1] == HEAD
        and arrays[0].shape[0] <= HEAD
        and w_gate.shape[0] == 1
        and w_down.shape[1] % (16 * nt) == 0
        and s_down.shape[0] % (16 * n) == 0
        and w_down.shape[1] % HEAD == 0
        and (2 * w_down.shape[1]) % s_down.shape[0] == 0
        and (nt * s_down.shape[0]) % (2 * w_down.shape[1]) == 0
        and w_down.shape[2] % (16 * HEAD) == 0
    )
    return near(*arrays) if fits else local(*arrays)


def solution(mesh):
    return jax.shard_map(
        layer,
        mesh=mesh,
        in_specs=(
            P(("sp", "tp"), None),
            P("sp", "tp"),
            P("sp", "tp"),
            P("sp", "tp"),
            P("sp", "tp"),
            P("sp", "tp"),
            P("tp"),
            P("tp", None),
            P(),
            P(("sp", "tp"), None),
            P(("sp", "tp"), None),
            P("sp", None, None),
            P("sp", None, None),
            P("sp", None, None),
            P(None, "tp"),
            P(None, "tp"),
            P("tp", None),
        ),
        out_specs=P(("sp", "tp"), None),
        check_vma=False,
    )
```
